32 devices in a mesh: sp: 16 (over z, y, x), tp: 2 (over core).
Axes of the slice: x: 2, y: 2, z: 4, core: 2. Of those that a mesh axis runs over, the one named last changes fastest.
Arguments:
- tokens: bfloat16 [2048, 2048], P('sp'), may hold values from -6 to 6
- in_gain: bfloat16 [2048], replicated, may hold values from 0.099609375 to 1.8984375
- w_value: bfloat16 [2048, 4096], P('sp', 'tp'), may hold values from -0.125 to 0.125
- w_gate: bfloat16 [2048, 4096], P('sp', 'tp'), may hold values from -0.125 to 0.125
- w_in_key: bfloat16 [2048, 1024], P('sp', 'tp'), may hold values from -0.125 to 0.125
- w_read: bfloat16 [2048, 1024], P('sp', 'tp'), may hold values from -0.125 to 0.125
- w_step_fwd: bfloat16 [2048, 64], P('sp', 'tp'), may hold values from -0.25 to 0.25
- w_step_bwd: bfloat16 [2048, 64], P('sp', 'tp'), may hold values from -0.25 to 0.25
- conv_value: bfloat16 [5, 4096], P(None, 'tp'), may hold values from -2.5 to 2.5
- conv_key: bfloat16 [5, 1024], P(None, 'tp'), may hold values from -2.5 to 2.5
- conv_read: bfloat16 [5, 1024], P(None, 'tp'), may hold values from -2.5 to 2.5
- step_bias: float32 [2, 64], P(None, 'tp'), may hold values from -4 to -2
- rate: float32 [2, 64], P(None, 'tp'), may hold values from 0 to 1, as said below
- norm_gain: bfloat16 [4096], P('tp'), may hold values from 0.099609375 to 1.8984375
- w_out: bfloat16 [4096, 2048], P('tp', 'sp'), may hold values from -0.09375 to 0.09375
Outputs:
- mixed: bfloat16 [2048, 2048], P('sp')
The draws below stay inside these ranges and needn't reach their ends.
Inputs may be any that keep to these rules, and one draw needn't show every extreme that they name: `rate`: positive decay rates, one per head and direction.
All inputs are finite; a program needn't handle non-finite values.
Results may differ from the reference program's by a relative error of at most 0.018.
Values may be sent and summed in bfloat16 or wider, within the bound.
A program may use at most 128 MiB of HBM per device.

```python
import math
import jax
import jax.numpy as jnp
from jax import lax

D = 2048
HEADS = 64
HEAD_DIM = 64
GROUPS = 8
STATE = 128
KERNEL = 5
BLOCK = 128
INNER = 4096
SEQ = 2048
N_TP = 2


def draw_rate(key, part):
    chooser, fast_key, slow_key = jax.random.split(jax.random.fold_in(key, 7), 3)
    fast_share = 0.5
    picked = jax.random.uniform(chooser, (2, HEADS), jnp.float32) < fast_share
    fast_rates = jnp.exp(jax.random.uniform(fast_key, (2, HEADS), jnp.float32, math.log(0.01), math.log(1.0 / 30.0))) / 0.4
    slow_rates = jnp.exp(jax.random.uniform(slow_key, (2, HEADS), jnp.float32, math.log(0.5), math.log(2.0))) / (0.4 * SEQ)
    return jnp.where(picked, fast_rates, slow_rates).astype(jnp.float32)


def steps_of(own_key, extent, pieces, smallest, largest):
    loudness = 1.0
    for position, blocks in pieces:
        steps = jax.random.uniform(jax.random.fold_in(jax.random.fold_in(own_key, 6), position), (blocks,), jnp.float32, smallest / len(pieces), largest / len(pieces))
        loudness = loudness * jnp.repeat(jnp.exp(steps), extent[position] // blocks).reshape((-1,) + (1,) * (len(extent) - 1 - position))
    return loudness


def bell_draw(own_key, dims, deviation, limit, cuts=(), dtype=jnp.bfloat16):
    entries = deviation * jax.random.normal(own_key, dims, jnp.float32)
    if cuts:
        entries = entries * steps_of(own_key, dims, cuts, -0.22, 0.18)
    return jnp.clip(entries, -limit, limit).astype(dtype)


def setup_inputs(seed: int = 0) -> dict:
    seeds = jax.random.split(jax.random.key(seed), 16)
    return {
        "tokens": bell_draw(seeds[0], (SEQ, D), 1.0, 6.0, ((0, 16),)),
        "in_gain": jnp.clip(1.0 + 0.18 * jax.random.normal(seeds[1], (D,), jnp.float32), 0.099609375, 1.8984375).astype(jnp.bfloat16),
        "w_value": bell_draw(seeds[2], (D, INNER), D ** -0.5, 0.125, ((0, 16), (1, 2))),
        "w_gate": bell_draw(seeds[3], (D, INNER), D ** -0.5, 0.125, ((0, 16), (1, 2))),
        "w_in_key": bell_draw(seeds[4], (D, GROUPS * STATE), D ** -0.5, 0.125, ((0, 16), (1, 2))),
        "w_read": bell_draw(seeds[5], (D, GROUPS * STATE), D ** -0.5, 0.125, ((0, 16), (1, 2))),
        "w_step_fwd": bell_draw(seeds[6], (D, HEADS), (D // 4) ** -0.5, 0.25, ((0, 16), (1, 2))),
        "w_step_bwd": bell_draw(seeds[7], (D, HEADS), (D // 4) ** -0.5, 0.25, ((0, 16), (1, 2))),
        "conv_value": bell_draw(seeds[8], (KERNEL, INNER), KERNEL ** -0.5, 2.5, ((1, 2),)),
        "conv_key": bell_draw(seeds[9], (KERNEL, GROUPS * STATE), KERNEL ** -0.5, 2.5, ((1, 2),)),
        "conv_read": bell_draw(seeds[10], (KERNEL, GROUPS * STATE), KERNEL ** -0.5, 2.5, ((1, 2),)),
        "step_bias": jnp.clip(-4.0 + 2.0 * jax.random.uniform(seeds[11], (2, HEADS), jnp.float32) ** steps_of(seeds[11], (2, HEADS), ((1, 2),), -0.2, 0.2), -4.0, -2.0),
        "rate": draw_rate(jax.random.fold_in(seeds[15], 71), 0),
        "norm_gain": jnp.clip(1.0 + 0.18 * jax.random.normal(seeds[13], (INNER,), jnp.float32), 0.099609375, 1.8984375).astype(jnp.bfloat16),
        "w_out": bell_draw(seeds[14], (INNER, D), INNER ** -0.5, 0.09375, ((0, 2), (1, 16))),
    }


EPSILON = 1e-05
FULL_PRECISION = lax.Precision.HIGHEST

def normalize(tensor, gain):
    return tensor * lax.rsqrt(lax.optimization_barrier(jnp.mean(tensor * tensor, -1, keepdims=True)) + EPSILON) * gain

def centred(projected, kernel_taps):
    tap_count = kernel_taps.shape[0]
    half_reach = (tap_count - 1) // 2
    length = projected.shape[0]
    padded = jnp.pad(projected.astype(jnp.float32), ((half_reach, half_reach), (0, 0)))
    summed = jnp.zeros(projected.shape, jnp.float32)
    for offset in range(tap_count):
        summed = summed + padded[offset:offset + length] * kernel_taps[offset].astype(jnp.float32)
    return jax.nn.silu(summed).astype(jnp.bfloat16)

def block_parts(values, step_size, log_decay, in_keys):
    per_group = values.shape[1] // in_keys.shape[1]
    cumulative = jnp.cumsum(log_decay, axis=0)
    log_total = cumulative[-1]
    weighting = jnp.exp(log_total[None, :] - cumulative) * step_size
    key_heads = jnp.repeat(in_keys.astype(jnp.float32), per_group, axis=1)
    scaled = (values.astype(jnp.float32) * weighting[:, :, None]).astype(jnp.bfloat16).astype(jnp.float32)
    injected = jnp.einsum('jhn,jhp->hpn', key_heads, scaled, precision=FULL_PRECISION)
    return (cumulative, jnp.exp(log_total), injected)

def block_step(memory, inputs):
    values, step_size, log_decay, in_keys, read_in = inputs
    per_group = values.shape[1] // in_keys.shape[1]
    cumulative, damping, injected = block_parts(values, step_size, log_decay, in_keys)
    scores = jnp.einsum('ign,jgn->ijg', read_in.astype(jnp.float32), in_keys.astype(jnp.float32), precision=FULL_PRECISION)
    scores = jnp.repeat(scores, per_group, axis=2)
    length = values.shape[0]
    below_mask = (jnp.arange(length)[:, None] >= jnp.arange(length)[None, :])[:, :, None]
    gaps = jnp.where(below_mask, cumulative[:, None, :] - cumulative[None, :, :], -jnp.inf)
    weights = (scores * jnp.exp(gaps) * step_size[None, :, :]).astype(jnp.bfloat16).astype(jnp.float32)
    within = jnp.einsum('ijh,jhp->ihp', weights, values.astype(jnp.float32), precision=FULL_PRECISION)
    read_heads = jnp.repeat(read_in.astype(jnp.float32), per_group, axis=1)
    carried = jnp.einsum('ihn,hpn->ihp', read_heads, memory, precision=FULL_PRECISION) * jnp.exp(cumulative)[:, :, None]
    memory = damping[:, None, None] * memory + injected
    return (memory, within + carried)

def sweep(values, step_size, log_decay, in_keys, read_in, memory):
    blocks = values.shape[0] // BLOCK

    def blocked(tensor):
        return tensor.reshape((blocks, BLOCK) + tensor.shape[1:])
    memory, swept = lax.scan(block_step, memory, (blocked(values), blocked(step_size), blocked(log_decay), blocked(in_keys), blocked(read_in)))
    return (swept.reshape((blocks * BLOCK,) + swept.shape[2:]), memory)

def reference(tokens, in_gain, w_value, w_gate, w_in_key, w_read, w_step_fwd, w_step_bwd, conv_value, conv_key, conv_read, step_bias, rate, norm_gain, w_out):
    normed = normalize(tokens.astype(jnp.float32), in_gain.astype(jnp.float32)).astype(jnp.bfloat16)

    def project(weight):
        return jnp.dot(normed, weight, preferred_element_type=jnp.float32).astype(jnp.bfloat16)
    length = tokens.shape[0]
    values = centred(project(w_value), conv_value).reshape(length, HEADS, HEAD_DIM)
    gate_raw = project(w_gate)
    in_keys = centred(project(w_in_key), conv_key).reshape(length, GROUPS, STATE)
    read_in = centred(project(w_read), conv_read).reshape(length, GROUPS, STATE)
    blank = jnp.zeros((HEADS, HEAD_DIM, STATE), jnp.float32)
    summed_heads = jnp.zeros((length, HEADS, HEAD_DIM), jnp.float32)
    for direction, weight in ((0, w_step_fwd), (1, w_step_bwd)):
        step_pre = project(weight).astype(jnp.float32)
        step_size = jax.nn.softplus(step_pre + step_bias[direction].astype(jnp.float32))
        log_decay = -rate[direction].astype(jnp.float32) * step_size
        if direction == 0:
            swept, final_state = sweep(values, step_size, log_decay, in_keys, read_in, blank)
        else:
            swept, final_state = sweep(values[::-1], step_size[::-1], log_decay[::-1], in_keys[::-1], read_in[::-1], blank)
            swept = swept[::-1]
        summed_heads = summed_heads + swept
    gated_out = summed_heads * jax.nn.silu(gate_raw.astype(jnp.float32)).reshape(length, HEADS, HEAD_DIM)
    head_gain = norm_gain.astype(jnp.float32).reshape(HEADS, HEAD_DIM)
    normed_heads = normalize(gated_out, head_gain).astype(jnp.bfloat16).reshape(length, INNER)
    part_width = INNER // N_TP
    result = jnp.zeros((length, D), jnp.float32)
    for tp_part in range(N_TP):
        portion = jnp.dot(normed_heads[:, tp_part * part_width:(tp_part + 1) * part_width], w_out[tp_part * part_width:(tp_part + 1) * part_width], preferred_element_type=jnp.float32)
        result = result + lax.optimization_barrier(portion.astype(jnp.bfloat16)).astype(jnp.float32)
    return result.astype(jnp.bfloat16)
```

```python
import functools
import math

import jax
import jax.numpy as jnp
from jax import lax
from jax.experimental import pallas as pl
from jax.experimental.pallas import tpu as pltpu
from jax.sharding import PartitionSpec as P

HEAD_DIM = 64
STATE = 128
KERNEL = 5
BLOCK = 128


EPSILON = 1e-05
FULL_PRECISION = lax.Precision.HIGHEST


def entering_2(x, axis, combine, identity, reverse):
    length, place = (lax.axis_size(axis), lax.axis_index(axis))
    everything = jax.tree.map(lambda part: lax.all_gather(part, axis), x)
    start = jax.tree.map(
        lambda part, zero: jnp.broadcast_to(jnp.asarray(zero, part.dtype), part.shape), x, identity
    )

    def step(k, before):
        at = length - 1 - k if reverse else k
        reached = at > place if reverse else at < place
        new = combine(before, jax.tree.map(lambda part: part[at], everything))
        return jax.tree.map(lambda a, b: jnp.where(reached, a, b), new, before)

    return lax.fori_loop(0, length, step, start)


def with_halo(cells, sides, width):
    for axis, dim in sides:
        count = lax.axis_size(axis)
        ends = count - 1
        head = lax.slice_in_dim(cells, 0, width, axis=dim)
        tail = lax.slice_in_dim(cells, cells.shape[dim] - width, cells.shape[dim], axis=dim)
        cells = jnp.concatenate(
            [
                lax.ppermute(tail, axis, [(i, (i + 1) % count) for i in range(ends)]),
                cells,
                lax.ppermute(head, axis, [((i + 1) % count, i) for i in range(ends)]),
            ],
            axis=dim,
        )
    return cells


def normalize(tensor, gain):
    return tensor * lax.rsqrt(jnp.mean(tensor * tensor, -1, keepdims=True) + EPSILON) * gain


def block_parts(values, step_size, log_decay, in_keys):
    per_group = values.shape[1] // in_keys.shape[1]
    cumulative = jnp.cumsum(log_decay, axis=0)
    log_total = cumulative[-1]
    weighting = jnp.exp(log_total[None, :] - cumulative) * step_size
    key_heads = jnp.repeat(in_keys, per_group, axis=1)
    scaled = (values.astype(jnp.float32) * weighting[:, :, None]).astype(jnp.bfloat16)
    injected = jnp.einsum("jhn,jhp->hpn", key_heads, scaled, preferred_element_type=jnp.float32)
    return (cumulative, jnp.exp(log_total), injected)


def block_step(memory, inputs):
    values, step_size, cumulative, damping, injected, in_keys, read_in = inputs
    per_group = values.shape[1] // in_keys.shape[1]
    scores = jnp.einsum("ign,jgn->ijg", read_in, in_keys, preferred_element_type=jnp.float32)
    scores = jnp.repeat(scores, per_group, axis=2)
    length = values.shape[0]
    below_mask = (jnp.arange(length)[:, None] >= jnp.arange(length)[None, :])[:, :, None]
    gaps = jnp.where(below_mask, cumulative[:, None, :] - cumulative[None, :, :], -jnp.inf)
    weights = (scores * jnp.exp(gaps) * step_size[None, :, :]).astype(jnp.bfloat16)
    within = jnp.einsum("ijh,jhp->ihp", weights, values, preferred_element_type=jnp.float32)
    read_heads = jnp.repeat(read_in.astype(jnp.float32), per_group, axis=1)
    carried = (
        jnp.einsum("ihn,hpn->ihp", read_heads, memory, precision=FULL_PRECISION)
        * jnp.exp(cumulative)[:, :, None]
    )
    memory = damping[:, None, None] * memory + injected
    return (memory, within + carried)


def blocked(tensor):
    blocks = tensor.shape[0] // BLOCK
    return tensor.reshape((blocks, BLOCK) + tensor.shape[1:])


def sweep(block_inputs, memory):
    memory, swept = lax.scan(block_step, memory, block_inputs)
    return (swept.reshape((swept.shape[0] * swept.shape[1],) + swept.shape[2:]), memory)


def settle(damping_blocks, injected_blocks, memory):

    def advance(memory, inputs):
        return (inputs[0][:, None, None] * memory + inputs[1], None)

    memory, unused = lax.scan(advance, memory, (damping_blocks, injected_blocks))
    return memory


def chain(before_pair, after_pair):
    return (
        before_pair[0] * after_pair[0],
        after_pair[0][:, None, None] * before_pair[1] + after_pair[1],
    )


def entering(damping, final_state, backward):
    identity_pair = (jnp.ones_like(damping), jnp.zeros_like(final_state))
    if backward:
        arrived = entering_2((damping, final_state), "sp", chain, identity_pair, True)
    else:
        arrived = entering_2((damping, final_state), "sp", chain, identity_pair, False)
    return arrived[1]


def body(
    tokens,
    in_gain,
    w_value,
    w_gate,
    w_in_key,
    w_read,
    w_step_fwd,
    w_step_bwd,
    conv_value,
    conv_key,
    conv_read,
    step_bias,
    rate,
    norm_gain,
    w_out,
):
    normed = normalize(tokens.astype(jnp.float32), in_gain.astype(jnp.float32)).astype(jnp.bfloat16)
    weights = (
        lax.all_gather(w_value, "sp", axis=0, tiled=True),
        lax.all_gather(w_gate, "sp", axis=0, tiled=True),
        lax.all_gather(w_in_key, "sp", axis=0, tiled=True),
        lax.all_gather(w_read, "sp", axis=0, tiled=True),
        lax.all_gather(w_step_fwd, "sp", axis=0, tiled=True),
        lax.all_gather(w_step_bwd, "sp", axis=0, tiled=True),
    )
    projected = [
        jnp.dot(normed, weight, preferred_element_type=jnp.float32).astype(jnp.bfloat16)
        for weight in weights
    ]
    value_raw, gate_raw, key_raw, read_raw, pre_fwd, pre_bwd = projected
    value_cols = value_raw.shape[1]
    key_cols = key_raw.shape[1]
    joined = jnp.concatenate([value_raw, key_raw, read_raw], axis=1)
    padded = with_halo(joined, (("sp", 0),), (KERNEL - 1) // 2)
    kernel_taps = jnp.concatenate([conv_value, conv_key, conv_read], axis=1).astype(jnp.float32)
    length = joined.shape[0]
    summed = jnp.zeros(joined.shape, jnp.float32)
    for offset in range(KERNEL):
        summed = summed + padded[offset : offset + length].astype(jnp.float32) * kernel_taps[offset]
    mixed_in = jax.nn.silu(summed).astype(jnp.bfloat16)
    head_count = value_cols // HEAD_DIM
    group_count = key_cols // STATE
    values = mixed_in[:, :value_cols].reshape(length, head_count, HEAD_DIM)
    in_keys = mixed_in[:, value_cols : value_cols + key_cols].reshape(length, group_count, STATE)
    read_in = mixed_in[:, value_cols + key_cols :].reshape(length, group_count, STATE)
    blank = jnp.zeros((head_count, HEAD_DIM, STATE), jnp.float32)
    summed_heads = jnp.zeros(values.shape, jnp.float32)
    for direction, step_pre in ((0, pre_fwd), (1, pre_bwd)):
        step_size = jax.nn.softplus(step_pre.astype(jnp.float32) + step_bias[direction])
        log_decay = -rate[direction] * step_size
        ordered = (values, step_size, log_decay, in_keys, read_in)
        if direction == 1:
            ordered = tuple((tensor[::-1] for tensor in ordered))
        value_blocks, step_blocks, decay_blocks, key_blocks, read_blocks = [
            blocked(tensor) for tensor in ordered
        ]
        cumulative_blocks, damping_blocks, injected_blocks = jax.vmap(block_parts)(
            value_blocks, step_blocks, decay_blocks, key_blocks
        )
        block_inputs = (
            value_blocks,
            step_blocks,
            cumulative_blocks,
            damping_blocks,
            injected_blocks,
            key_blocks,
            read_blocks,
        )
        damping = jnp.exp(jnp.sum(ordered[2], axis=0))
        final_state = settle(damping_blocks, injected_blocks, blank)
        arriving = entering(damping, final_state, direction == 1)
        swept, final_state = sweep(block_inputs, arriving)
        if direction == 1:
            swept = swept[::-1]
        summed_heads = summed_heads + swept
    gated_out = summed_heads * jax.nn.silu(gate_raw.astype(jnp.float32)).reshape(values.shape)
    head_gain = norm_gain.astype(jnp.float32).reshape(head_count, HEAD_DIM)
    normed_heads = normalize(gated_out, head_gain).astype(jnp.bfloat16).reshape(length, value_cols)
    out_whole = lax.all_gather(w_out, "sp", axis=1, tiled=True)
    own_rows = lax.psum_scatter(
        jnp.dot(normed_heads, out_whole, preferred_element_type=jnp.float32).astype(jnp.bfloat16),
        "tp",
        scatter_dimension=0,
        tiled=True,
    )
    return lax.all_gather(own_rows, "tp", axis=0, tiled=True)


F32 = jnp.float32
BF16 = jnp.bfloat16
LANES = 128
VMEM_SPEC = pl.BlockSpec(memory_space=pltpu.VMEM)


def push(src, dst, send, recv, peer):
    copy = pltpu.make_async_remote_copy(
        src_ref=src,
        dst_ref=dst,
        send_sem=send,
        recv_sem=recv,
        device_id=peer,
        device_id_type=pl.DeviceIdType.MESH,
    )
    copy.start()
    return copy


def silu(x):
    return x * jax.nn.sigmoid(x)


def whole_kernel(
    n, q, tin, ing, wv, wg, wk, wr, wsf, wsb, wo, cv, ck, cr, bias, rate, ngain, out,
    nrm, ws, taps, gains, tok, wts, wst, wout, raw, gate, pre, vals, keys, reads, cums, yy, injf, injb, carf, carb,
    nh, full, part, both,
    tzs, tzr, tps, tpr, tss, tsr, kzs, kzr, kps, kpr, vs, vr, ss, sr, os, orr,
    as_, ar, bs, br, es, er, fs, fr, ls,
):
    s, t = lax.axis_index("sp"), lax.axis_index("tp")
    z, p = s // q, s % q
    sibling = (s, 1 - t)
    half = tok.shape[2]
    depth = wv.shape[0]
    blocks = tok.shape[0] * 2 * half // BLOCK

    def at(dz, dp):
        return lax.rem(z + dz, q) * q + lax.rem(p + dp, q)

    def span(i, size):
        return pl.ds(pl.multiple_of(i * size, size), size)

    px = p + 1 - 2 * lax.rem(p, 2)
    py = lax.rem(p + 2, q)
    pd = lax.rem(px + 2, q)
    side = {"x": (z * q + px, t), "y": (z * q + py, t)}
    turns = (("x", "y"), ("y", "x"))

    def chip(dz, where):
        return lax.rem(z + q - dz, q) * q + where

    with jax.named_scope("greet"):
        barrier = pltpu.get_barrier_semaphore()
        peers = [(lax.rem(s + k, n), t) for k in range(1, n)] + [sibling]
        for peer in peers:
            pl.semaphore_signal(barrier, inc=1, device_id=peer, device_id_type=pl.DeviceIdType.MESH)

    def local(src, dst, i):
        copy = pltpu.make_async_copy(src, dst, ls.at[i])
        copy.start()
        return copy

    mine = span(s, depth)
    rows = span(t, half)
    kcol, rcol = pl.ds(2 * LANES, LANES), pl.ds(3 * LANES, LANES)
    krcol = pl.ds(2 * LANES, 2 * LANES)

    with jax.named_scope("prep"):
        locals_ = [
            local(wk.at[:, span(z, LANES)], wts.at[mine, kcol], 2),
            local(wr.at[:, span(z, LANES)], wts.at[mine, rcol], 3),
            local(wv.at[:, mine], wts.at[mine, pl.ds(0, LANES)], 4),
            local(wg.at[:, mine], wts.at[mine, pl.ds(LANES, LANES)], 5),
        ]
        wide_in = tin[...].astype(F32)
        nrm[...] = normalize(wide_in, ing[...].astype(F32).reshape(1, ing.shape[0])).astype(BF16)
        heads = wsf.shape[0]
        slot = ws.shape[0] // n
        row_i = lax.broadcasted_iota(jnp.int32, (n * slot, heads), 0)
        col_i = lax.broadcasted_iota(jnp.int32, (n * slot, heads), 1)
        place = lax.rem(row_i, slot)
        head_of = 2 * (row_i // slot)
        pick_f = jnp.where((place < 2) & (col_i == head_of + place), 1.0, 0.0).astype(BF16)
        pick_b = jnp.where((place >= 2) & (col_i == head_of + place - 2), 1.0, 0.0).astype(BF16)
        ws[...] = (
            jnp.dot(pick_f, wsf[...], preferred_element_type=F32)
            + jnp.dot(pick_b, wsb[...], preferred_element_type=F32)
        ).astype(BF16)
        own = span(s, LANES)
        taps[0:KERNEL, 0:LANES] = cv[:, own].astype(F32)
        taps[0:KERNEL, LANES : 2 * LANES] = ck[:, span(z, LANES)].astype(F32)
        taps[0:KERNEL, 2 * LANES : 3 * LANES] = cr[:, span(z, LANES)].astype(F32)
        gains[...] = ngain[...].astype(F32).reshape(n, LANES)
        hk = lax.broadcasted_iota(jnp.int32, (heads, LANES), 0)
        hl = lax.broadcasted_iota(jnp.int32, (heads, LANES), 1)
        spread = jnp.where((hl < 4) & (hk == 2 * s + lax.rem(hl, 2)), 1.0, 0.0).astype(F32)
        first_two = lax.broadcasted_iota(jnp.int32, (1, LANES), 1) < 2

        def own_lanes(both_dirs):
            got = jnp.dot(both_dirs, spread, precision=FULL_PRECISION, preferred_element_type=F32)
            return jnp.where(first_two, got[0:1], got[1:2])

        offsets = own_lanes(bias[...])
        rates = own_lanes(rate[...])
        wst[slot:, :] = jnp.zeros((LANES - slot, wst.shape[1]), BF16)
        seq = blocks * BLOCK
        wide = 3 * LANES
        raw[0:8, :] = jnp.zeros((8, wide), F32)
        raw[seq + 8 : seq + 16, :] = jnp.zeros((8, wide), F32)
        for copy in locals_:
            copy.wait()
    with jax.named_scope("greeted"):
        pl.semaphore_wait(barrier, len(peers))

    one, last = q - 1, q
    rising, sinking = z < q - 1, z > 0
    unit = nrm.at[rows]

    def arrival(e):
        later = [[1, 2, 3], [0, 2, 3], [3, 1, 0], [2, 1, 0]]
        picked = later[q - 1][e]
        for k in range(q - 1):
            picked = jnp.where(z == k, later[k][e], picked)
        return picked

    sources = [z] + [arrival(e) for e in range(q - 1)]

    def chain(src_ref, dst_ref, sends, recvs):
        @pl.when(rising)
        def _():
            push(src_ref, dst_ref, sends.at[z], recvs.at[z], (s + q, t))

        @pl.when(sinking)
        def _():
            push(src_ref, dst_ref, sends.at[q], recvs.at[z], (s - q, t))

    def remote(src, dst, send, recv, peer):
        return pltpu.make_async_remote_copy(
            src_ref=src, dst_ref=dst, send_sem=send, recv_sem=recv,
            device_id=peer, device_id_type=pl.DeviceIdType.MESH,
        )

    def onward(zs):
        to = z + jnp.where(zs < z, 1, -1)
        return to, (to >= 0) & (to < q)

    def settle_chain(src_ref, sends, recvs, ref_of):
        @pl.when(rising)
        def _():
            remote(src_ref, ref_of(z), sends.at[z], recvs.at[z], (s + q, t)).wait_send()

        @pl.when(sinking)
        def _():
            remote(src_ref, ref_of(z), sends.at[q], recvs.at[z], (s - q, t)).wait_send()

        for zs in sources[1:]:
            to, ok = onward(zs)

            @pl.when(ok)
            def _():
                ref = ref_of(zs)
                remote(ref, ref, sends.at[zs], recvs.at[zs], (to * q + p, t)).wait_send()

    def tok_of(zs):
        return tok.at[zs * q + p, t]

    def wout_of(zs):
        return wout.at[:, span(zs, LANES)]

    plane, keyz, keyp, weights, swaps = {}, [], {}, [], {}
    with jax.named_scope("issue"):
        chain(unit, tok_of(z), tzs, tzr)
        for i, to in enumerate("xy"):
            plane[0, to] = push(unit, tok.at[s, t], tps.at[0, i], tpr.at[0, i], side[to])
        for dz in range(1, q):
            grp = span(lax.rem(z + dz, q), LANES)
            keyz.append(
                [
                    push(w.at[:, grp], wts.at[mine, col], kzs.at[dz, i], kzr.at[dz, i], (at(dz, 0), t))
                    for i, (w, col) in enumerate(((wk, kcol), (wr, rcol)))
                ]
            )
        got = wts.at[mine, krcol]
        for i, to in enumerate("xy"):
            keyp[0, to] = push(got, got, kps.at[0, i], kpr.at[0, i], side[to])
        for k in range(1, n):
            j = lax.rem(s + k, n)
            cols = span(j, LANES)
            for i, w in enumerate((wv, wg)):
                weights.append(
                    push(w.at[:, cols], wts.at[mine, pl.ds(i * LANES, LANES)], vs.at[k, i], vr.at[k, i], (j, t))
                )
            weights.append(
                push(ws.at[span(j, slot)], wst.at[pl.ds(0, slot), mine], ss.at[k], sr.at[k], (j, t))
            )
        locals_ = [
            local(nrm.at[pl.ds(0, half)], tok.at[s, 0], 0),
            local(nrm.at[pl.ds(half, half)], tok.at[s, 1], 1),
            local(ws.at[span(s, slot)], wst.at[pl.ds(0, slot), mine], 6),
            local(wo, wout_of(z), 7),
        ]

    def swap(e, i):
        src = sources[e] * q + (p, px, py, pd)[i]
        swaps[e, i] = push(tok.at[src, t], tok.at[src, t], tss.at[e, i], tsr.at[e, i], sibling)

    def arrive(e):
        with jax.named_scope("arrive"):
            zs = sources[e]
            ref = tok_of(zs)
            remote(ref, ref, tzs.at[zs], tzr.at[zs], sibling).wait_recv()
            to, ok = onward(zs)

            @pl.when(ok)
            def _():
                push(ref, ref, tzs.at[zs], tzr.at[zs], (to * q + p, t))

            for i, way in enumerate("xy"):
                plane[e, way] = push(ref, ref, tps.at[e, i], tpr.at[e, i], side[way])
            swap(e, 0)

    quarter = half // 2

    def relay(e):
        with jax.named_scope("relay"):
            for i, (near_by, other) in enumerate(turns):
                plane[e, near_by].wait_recv()
                ref = tok.at[sources[e] * q + (px, py)[i], t, pl.ds(i * quarter, quarter)]
                plane[e, other + "d"] = push(ref, ref, tps.at[e, 2 + i], tpr.at[e, 2 + i], side[other])
                swap(e, 1 + i)

    def key_arrive(dz):
        with jax.named_scope("key_arrive"):
            for copy in keyz[dz - 1]:
                copy.wait_recv()
            ref = wts.at[span(at(q - dz, 0), depth), krcol]
            for i, to in enumerate("xy"):
                keyp[dz, to] = push(ref, ref, kps.at[dz, i], kpr.at[dz, i], side[to])

    def key_relay(dz):
        with jax.named_scope("key_relay"):
            for i, (near_by, other) in enumerate(turns):
                keyp[dz, near_by].wait_recv()
                ref = wts.at[span(chip(dz, (px, py)[i]), depth), (kcol, rcol)[i]]
                keyp[dz, other + "d"] = push(ref, ref, kps.at[dz, 2 + i], kpr.at[dz, 2 + i], side[other])

    def project(zs):
        @pl.loop(0, q // 2)
        def _(i):
            pair = zs * q + 2 * i
            r0 = pl.multiple_of(pair * BLOCK, 2 * BLOCK)
            at2 = pl.ds(r0, 2 * BLOCK)
            x = tok[pl.ds(pair, 2)].reshape(2 * BLOCK, tok.shape[3])
            got = jnp.dot(x, wts[...], preferred_element_type=F32).astype(BF16)
            for i_, b_ in ((0, 0), (2, 1), (3, 2)):
                raw[pl.ds(r0 + 8, 2 * BLOCK), b_ * LANES : (b_ + 1) * LANES] = got[
                    :, i_ * LANES : (i_ + 1) * LANES
                ].astype(F32)
            gate[at2, :] = got[:, LANES : 2 * LANES]
            u = lax.dot_general(x, wst[...], (((1,), (1,)), ((), ())), preferred_element_type=F32)
            u = u.astype(BF16).astype(F32) + offsets
            pre[at2, :] = jnp.maximum(u, 0.0) + jnp.log1p(jnp.exp(-jnp.abs(u)))

    def convolve(i):
        r0 = pl.multiple_of(i * BLOCK, BLOCK)
        for b, dst in enumerate((vals, keys, reads)):
            window = raw[pl.ds(r0, BLOCK + 16), b * LANES : (b + 1) * LANES]
            total = jnp.zeros((BLOCK, LANES), F32)
            for k in range(KERNEL):
                lo = 8 - (KERNEL - 1) // 2 + k
                total = total + window[lo : lo + BLOCK] * taps[k : k + 1, b * LANES : (b + 1) * LANES]
            dst[pl.ds(r0, BLOCK), :] = silu(total).astype(BF16)

    ri = lax.broadcasted_iota(jnp.int32, (BLOCK, BLOCK), 0)
    ci = lax.broadcasted_iota(jnp.int32, (BLOCK, BLOCK), 1)
    low = ri >= ci
    diag = ri == ci
    fwd = ci < 2
    left = ci < HEAD_DIM
    lower = jnp.where(low, 1.0, 0.0).astype(F32)
    upper = jnp.where(ri <= ci, 1.0, 0.0).astype(F32)

    def within(i):
        r0 = pl.multiple_of(i * BLOCK, BLOCK)
        here = pl.ds(r0, BLOCK)
        st = pre[here, :]
        ld = -rates * st
        c = jnp.where(
            fwd,
            jnp.dot(lower, ld, precision=FULL_PRECISION, preferred_element_type=F32),
            jnp.dot(upper, ld, precision=FULL_PRECISION, preferred_element_type=F32),
        )
        cums[here, :] = c
        ct = c.T
        stt = st.T
        key, read, val = keys[here, :], reads[here, :], vals[here, :]
        val32 = val.astype(F32)
        score = lax.dot_general(read, key, (((1,), (1,)), ((), ())), preferred_element_type=F32)
        total = jnp.zeros((BLOCK, LANES), F32)
        for h in range(2):
            gap = jnp.where(low, c[:, h : h + 1] - ct[h : h + 1, :], c[:, h + 2 : h + 3] - ct[h + 2 : h + 3, :])
            sb = stt[h + 2 : h + 3, :]
            e = jnp.exp(gap) * jnp.where(low, stt[h : h + 1, :], sb) + jnp.where(diag, sb, 0.0)
            mask = left if h == 0 else jnp.logical_not(left)
            own_val = jnp.where(mask, val32, 0.0).astype(BF16)
            total = total + jnp.dot((score * e).astype(BF16), own_val, preferred_element_type=F32)
        yy[here, :] = total
        c_end = jnp.where(fwd[0:1], c[BLOCK - 1 : BLOCK, :], c[0:1, :])
        weighting = jnp.exp(c_end - c) * st
        key_t = key.astype(F32).T.astype(BF16)
        for d, dst in ((0, injf), (1, injb)):
            w = jnp.where(left, weighting[:, 2 * d : 2 * d + 1], weighting[:, 2 * d + 1 : 2 * d + 2])
            scaled = (val32 * w).astype(BF16)
            dst[i] = jnp.dot(key_t, scaled, preferred_element_type=F32)

    def use(e):
        zs = sources[e]
        with jax.named_scope("usewait"):
            plane[e, "yd"].wait_recv()
            plane[e, "xd"].wait_recv()
            swap(e, 3)
            for i in range(q):
                if (e, i) != (0, 0):
                    swaps[e, i].wait_recv()
        with jax.named_scope("project"):
            project(zs)
        edge = jnp.where(zs == 0, 0, blocks - 1)
        if e == 0:
            start, count = zs * q + 1, q - 2
        else:
            start, count = zs * q + jnp.where(zs > z, -1, 1), q
        if e == q - 1:
            count = count + 1

        def which(i):
            return start + i if e < q - 1 else jnp.where(i < q, start + i, edge)

        with jax.named_scope("conv"):

            @pl.loop(0, count, unroll=count)
            def _(i):
                convolve(which(i))

        with jax.named_scope("intra"):

            @pl.loop(0, count, unroll=count)
            def _(i):
                within(which(i))

        if e < q - 1:

            @pl.when((zs == 0) | (zs == q - 1))
            def _():
                convolve(edge)
                within(edge)

    def wout_onward(e):
        zs = sources[e]
        to, ok = onward(zs)

        @pl.when(ok)
        def _():
            ref = wout_of(zs)
            remote(ref, ref, os.at[zs], orr.at[zs], sibling).wait_recv()
            push(ref, ref, os.at[zs], orr.at[zs], (to * q + p, t))

    def wout_arrive(e):
        zs = sources[e]
        to, ok = onward(zs)

        @pl.when(jnp.logical_not(ok))
        def _():
            ref = wout_of(zs)
            remote(ref, ref, os.at[zs], orr.at[zs], sibling).wait_recv()

    arrive(1)
    relay(0)
    for dz in range(1, q):
        key_arrive(dz)
    arrive(2)
    key_relay(0)
    key_relay(1)
    relay(1)
    key_relay(2)
    key_relay(3)
    arrive(3)
    chain(wo, wout_of(z), os, orr)
    relay(2)
    with jax.named_scope("weights"):
        for copy in locals_:
            copy.wait()
        for copy in weights + [keyp[dz, to] for dz in range(q) for to in ("xd", "yd")]:
            copy.wait_recv()
    use(0)
    use(1)
    relay(3)
    use(2)
    with jax.named_scope("wout1"):
        wout_onward(1)
        wout_onward(2)
    use(3)

    def carry(i, state, d, inj, kept):
        r0 = pl.multiple_of(i * BLOCK, BLOCK)
        here = pl.ds(r0, BLOCK)
        ec = jnp.exp(cums[here, :])
        grown = jnp.where(left, ec[:, 2 * d : 2 * d + 1], ec[:, 2 * d + 1 : 2 * d + 2])
        high = state.astype(BF16)
        rest = (state - high.astype(F32)).astype(BF16)
        read = reads[here, :]
        add = jnp.dot(read, high, preferred_element_type=F32) + jnp.dot(
            read, rest, preferred_element_type=F32
        )
        kept[here, :] = add * grown
        end = grown[BLOCK - 1 : BLOCK, :] if d == 0 else grown[0:1, :]
        return state * end + inj[i]

    def advance(i, states):
        return (
            carry(i, states[0], 0, injf, carf),
            carry(blocks - 1 - i, states[1], 1, injb, carb),
        )

    with jax.named_scope("carry"):
        zero = jnp.zeros((STATE, LANES), F32)
        lax.fori_loop(0, blocks, advance, (zero, zero), unroll=4)

    gain = gains[pl.ds(s, 1), :]

    def finish(i):
        r0 = pl.multiple_of(i * BLOCK, BLOCK)
        here = pl.ds(r0, BLOCK)
        g = (yy[here, :] + carf[here, :] + carb[here, :]) * silu(gate[here, :].astype(F32))
        sq = g * g
        m0 = jnp.sum(jnp.where(left, sq, 0.0), -1, keepdims=True) / HEAD_DIM
        m1 = jnp.sum(jnp.where(left, 0.0, sq), -1, keepdims=True) / HEAD_DIM
        scale = jnp.where(left, lax.rsqrt(m0 + EPSILON), lax.rsqrt(m1 + EPSILON))
        nh[here, :] = (g * scale * gain).astype(BF16)

    away = []
    for dz in range(1, q + 1):
        to = lax.rem(z + dz, q)

        with jax.named_scope("finish"):

            @pl.loop(0, q, unroll=4)
            def _(i):
                finish(to * q + i)

        if dz < q:
            away.append(
                push(nh.at[span(to, q * BLOCK)], full.at[:, mine], as_.at[dz], ar.at[dz], (at(dz, 0), t))
            )
    near = {}
    keep = local(nh.at[span(z, q * BLOCK)], full.at[:, mine], 8)
    for i, to in enumerate("xy"):
        near[0, to] = push(
            nh.at[span(z, q * BLOCK)], full.at[:, mine], bs.at[0, i], br.at[0, i], side[to]
        )
    with jax.named_scope("wout2"):
        wout_onward(3)
    rest_rows = q * BLOCK // 2

    def near_relay(dz):
        with jax.named_scope("nearwait"):
            for i, (near_by, other) in enumerate(turns):
                near[dz, near_by].wait_recv()
                got = full.at[pl.ds(i * rest_rows, rest_rows), span(chip(dz, (px, py)[i]), LANES)]
                near[dz, other + "d"] = push(got, got, bs.at[dz, 2 + i], br.at[dz, 2 + i], side[other])

    for dz in range(1, q):
        with jax.named_scope("awaywait"):
            away[dz - 1].wait_recv()
        got = full.at[:, span(at(q - dz, 0), LANES)]
        for i, to in enumerate("xy"):
            near[dz, to] = push(got, got, bs.at[dz, i], br.at[dz, i], side[to])
        near_relay(dz - 1)
    near_relay(q - 1)
    with jax.named_scope("outswait"):
        for e in range(1, q):
            wout_arrive(e)
    with jax.named_scope("fullwait"):
        keep.wait()
        for copy in [near[dz, to] for dz in range(q) for to in ("xd", "yd")]:
            copy.wait_recv()
    legs = []

    def leg(dp):
        to = lax.rem(p + dp, q)
        legs.append(push(part.at[to], both.at[t, p], es.at[dp], er.at[dp], (at(0, dp), t)))

    with jax.named_scope("outdot"):
        for dp in range(1, q + 1):
            to = lax.rem(p + dp, q)
            part[to] = jnp.dot(full[span(to, BLOCK), :], wout[...], preferred_element_type=F32).astype(BF16)
            if dp >= 2:
                leg(dp - 1)
    across = [push(part.at[p], both.at[t, p], fs.at[0], fr.at[0], sibling)]
    keep = local(part.at[p], both.at[t, p], 9)
    with jax.named_scope("legswait"):
        for dp in range(1, q):
            legs[dp - 1].wait_recv()
            got = both.at[t, lax.rem(p + q - dp, q)]
            across.append(push(got, got, fs.at[dp], fr.at[dp], sibling))
    with jax.named_scope("acrosswait"):
        keep.wait()
        for copy in across:
            copy.wait()
    with jax.named_scope("sum"):
        for a in range(q):
            for b in range(q):
                here = slice(a * LANES, (a + 1) * LANES)
                total = both[0, b, :, here].astype(F32) + both[1, b, :, here].astype(F32)
                out[:, (a * q + b) * LANES : (a * q + b + 1) * LANES] = total.astype(BF16)
    with jax.named_scope("sends"):
        settle_chain(unit, tzs, tzr, tok_of)
        settle_chain(wo, os, orr, wout_of)
        flat = [copy for pair in keyz for copy in pair]
        for copy in flat + list(plane.values()) + list(keyp.values()) + weights + list(swaps.values()):
            copy.wait_send()
        for copy in away + list(near.values()) + legs:
            copy.wait_send()


def whole(n, q, *args):
    dma = pltpu.SemaphoreType.DMA
    vm = pltpu.VMEM
    tokens, wo, wsf = args[0], args[8], args[6]
    depth, width = tokens.shape
    seq = n * depth
    slot = 16
    return pl.pallas_call(
        functools.partial(whole_kernel, n, q),
        out_shape=jax.ShapeDtypeStruct((BLOCK, n * LANES), BF16),
        in_specs=[VMEM_SPEC] * len(args),
        out_specs=VMEM_SPEC,
        scratch_shapes=[
            vm((depth, width), BF16),
            vm((n * slot, depth), BF16),
            vm((8, 3 * LANES), F32),
            vm((n, LANES), F32),
            vm((n, 2, depth // 2, width), BF16),
            vm((width, 4 * LANES), BF16),
            vm((LANES, width), BF16),
            vm((wo.shape[0], q * LANES), BF16),
            vm((seq + 16, 3 * LANES), F32),
            vm((seq, LANES), BF16),
            vm((seq, LANES), F32),
            vm((seq, LANES), BF16),
            vm((seq, LANES), BF16),
            vm((seq, LANES), BF16),
            vm((seq, LANES), F32),
            vm((seq, LANES), F32),
            vm((seq // BLOCK, STATE, LANES), F32),
            vm((seq // BLOCK, STATE, LANES), F32),
            vm((seq, LANES), F32),
            vm((seq, LANES), F32),
            vm((seq, LANES), BF16),
            vm((q * BLOCK, n * LANES), BF16),
            vm((q, BLOCK, q * LANES), BF16),
            vm((2, q, BLOCK, q * LANES), BF16),
            dma((q + 1,)), dma((q,)), dma((q, q)), dma((q, q)), dma((q, q)), dma((q, q)),
            dma((q, 2)), dma((q, 2)), dma((q, q)), dma((q, q)),
            dma((n, 2)), dma((n, 2)), dma((n,)), dma((n,)), dma((q + 1,)), dma((q,)),
            dma((q,)), dma((q,)), dma((q, q)), dma((q, q)), dma((q,)), dma((q,)),
            dma((q,)), dma((q,)), dma((10,)),
        ],
        compiler_params=pltpu.CompilerParams(
            collective_id=0, has_side_effects=True, vmem_limit_bytes=VMEM_LIMIT << 20
        ),
        name="whole",
    )(*args)


VMEM_LIMIT = 56


def headwise(
    n,
    q,
    tokens,
    in_gain,
    w_value,
    w_gate,
    w_in_key,
    w_read,
    w_step_fwd,
    w_step_bwd,
    conv_value,
    conv_key,
    conv_read,
    step_bias,
    rate,
    norm_gain,
    w_out,
):
    return whole(
        n, q, tokens, in_gain, w_value, w_gate, w_in_key, w_read, w_step_fwd.T, w_step_bwd.T, w_out,
        conv_value, conv_key, conv_read, step_bias, rate, norm_gain,
    )


def whole_heads(mesh):
    n, q = mesh.shape["sp"], math.isqrt(mesh.shape["sp"])

    def run(*args):
        cols, keys = args[2].shape[1], args[4].shape[1]
        ready = (
            q * q == n
            and mesh.shape["tp"] == 2
            and cols == n * LANES
            and args[14].shape[1] == LANES
            and keys == q * LANES
            and q == 4
            and args[0].shape[1] == n * LANES
            and args[0].shape[0] == BLOCK
        )
        return headwise(n, q, *args) if ready else body(*args)

    return run


def solution(mesh):
    in_specs = (
        P("sp", None),
        P(),
        P("sp", "tp"),
        P("sp", "tp"),
        P("sp", "tp"),
        P("sp", "tp"),
        P("sp", "tp"),
        P("sp", "tp"),
        P(None, "tp"),
        P(None, "tp"),
        P(None, "tp"),
        P(None, "tp"),
        P(None, "tp"),
        P("tp"),
        P("tp", "sp"),
    )
    out_specs = P("sp", None)
    return jax.shard_map(whole_heads(mesh), mesh=mesh, in_specs=in_specs, out_specs=out_specs, check_vma=False)
```

```python
import functools
import math

import jax
import jax.numpy as jnp
from jax import lax
from jax.experimental import pallas as pl
from jax.experimental.pallas import tpu as pltpu
from jax.sharding import PartitionSpec as P

HEAD_DIM = 64
STATE = 128
KERNEL = 5
BLOCK = 128


EPSILON = 1e-05
FULL_PRECISION = lax.Precision.HIGHEST


def entering_2(x, axis, combine, identity, reverse):
    length, place = (lax.axis_size(axis), lax.axis_index(axis))
    everything = jax.tree.map(lambda part: lax.all_gather(part, axis), x)
    start = jax.tree.map(
        lambda part, zero: jnp.broadcast_to(jnp.asarray(zero, part.dtype), part.shape), x, identity
    )

    def step(k, before):
        at = length - 1 - k if reverse else k
        reached = at > place if reverse else at < place
        new = combine(before, jax.tree.map(lambda part: part[at], everything))
        return jax.tree.map(lambda a, b: jnp.where(reached, a, b), new, before)

    return lax.fori_loop(0, length, step, start)


def with_halo(cells, sides, width):
    for axis, dim in sides:
        count = lax.axis_size(axis)
        ends = count - 1
        head = lax.slice_in_dim(cells, 0, width, axis=dim)
        tail = lax.slice_in_dim(cells, cells.shape[dim] - width, cells.shape[dim], axis=dim)
        cells = jnp.concatenate(
            [
                lax.ppermute(tail, axis, [(i, (i + 1) % count) for i in range(ends)]),
                cells,
                lax.ppermute(head, axis, [((i + 1) % count, i) for i in range(ends)]),
            ],
            axis=dim,
        )
    return cells


def normalize(tensor, gain):
    return tensor * lax.rsqrt(jnp.mean(tensor * tensor, -1, keepdims=True) + EPSILON) * gain


def block_parts(values, step_size, log_decay, in_keys):
    per_group = values.shape[1] // in_keys.shape[1]
    cumulative = jnp.cumsum(log_decay, axis=0)
    log_total = cumulative[-1]
    weighting = jnp.exp(log_total[None, :] - cumulative) * step_size
    key_heads = jnp.repeat(in_keys, per_group, axis=1)
    scaled = (values.astype(jnp.float32) * weighting[:, :, None]).astype(jnp.bfloat16)
    injected = jnp.einsum("jhn,jhp->hpn", key_heads, scaled, preferred_element_type=jnp.float32)
    return (cumulative, jnp.exp(log_total), injected)


def block_step(memory, inputs):
    values, step_size, cumulative, damping, injected, in_keys, read_in = inputs
    per_group = values.shape[1] // in_keys.shape[1]
    scores = jnp.einsum("ign,jgn->ijg", read_in, in_keys, preferred_element_type=jnp.float32)
    scores = jnp.repeat(scores, per_group, axis=2)
    length = values.shape[0]
    below_mask = (jnp.arange(length)[:, None] >= jnp.arange(length)[None, :])[:, :, None]
    gaps = jnp.where(below_mask, cumulative[:, None, :] - cumulative[None, :, :], -jnp.inf)
    weights = (scores * jnp.exp(gaps) * step_size[None, :, :]).astype(jnp.bfloat16)
    within = jnp.einsum("ijh,jhp->ihp", weights, values, preferred_element_type=jnp.float32)
    read_heads = jnp.repeat(read_in.astype(jnp.float32), per_group, axis=1)
    carried = (
        jnp.einsum("ihn,hpn->ihp", read_heads, memory, precision=FULL_PRECISION)
        * jnp.exp(cumulative)[:, :, None]
    )
    memory = damping[:, None, None] * memory + injected
    return (memory, within + carried)


def blocked(tensor):
    blocks = tensor.shape[0] // BLOCK
    return tensor.reshape((blocks, BLOCK) + tensor.shape[1:])


def sweep(block_inputs, memory):
    memory, swept = lax.scan(block_step, memory, block_inputs)
    return (swept.reshape((swept.shape[0] * swept.shape[1],) + swept.shape[2:]), memory)


def settle(damping_blocks, injected_blocks, memory):

    def advance(memory, inputs):
        return (inputs[0][:, None, None] * memory + inputs[1], None)

    memory, unused = lax.scan(advance, memory, (damping_blocks, injected_blocks))
    return memory


def chain(before_pair, after_pair):
    return (
        before_pair[0] * after_pair[0],
        after_pair[0][:, None, None] * before_pair[1] + after_pair[1],
    )


def entering(damping, final_state, backward):
    identity_pair = (jnp.ones_like(damping), jnp.zeros_like(final_state))
    if backward:
        arrived = entering_2((damping, final_state), "sp", chain, identity_pair, True)
    else:
        arrived = entering_2((damping, final_state), "sp", chain, identity_pair, False)
    return arrived[1]


def body(
    tokens,
    in_gain,
    w_value,
    w_gate,
    w_in_key,
    w_read,
    w_step_fwd,
    w_step_bwd,
    conv_value,
    conv_key,
    conv_read,
    step_bias,
    rate,
    norm_gain,
    w_out,
):
    normed = normalize(tokens.astype(jnp.float32), in_gain.astype(jnp.float32)).astype(jnp.bfloat16)
    weights = (
        lax.all_gather(w_value, "sp", axis=0, tiled=True),
        lax.all_gather(w_gate, "sp", axis=0, tiled=True),
        lax.all_gather(w_in_key, "sp", axis=0, tiled=True),
        lax.all_gather(w_read, "sp", axis=0, tiled=True),
        lax.all_gather(w_step_fwd, "sp", axis=0, tiled=True),
        lax.all_gather(w_step_bwd, "sp", axis=0, tiled=True),
    )
    projected = [
        jnp.dot(normed, weight, preferred_element_type=jnp.float32).astype(jnp.bfloat16)
        for weight in weights
    ]
    value_raw, gate_raw, key_raw, read_raw, pre_fwd, pre_bwd = projected
    value_cols = value_raw.shape[1]
    key_cols = key_raw.shape[1]
    joined = jnp.concatenate([value_raw, key_raw, read_raw], axis=1)
    padded = with_halo(joined, (("sp", 0),), (KERNEL - 1) // 2)
    kernel_taps = jnp.concatenate([conv_value, conv_key, conv_read], axis=1).astype(jnp.float32)
    length = joined.shape[0]
    summed = jnp.zeros(joined.shape, jnp.float32)
    for offset in range(KERNEL):
        summed = summed + padded[offset : offset + length].astype(jnp.float32) * kernel_taps[offset]
    mixed_in = jax.nn.silu(summed).astype(jnp.bfloat16)
    head_count = value_cols // HEAD_DIM
    group_count = key_cols // STATE
    values = mixed_in[:, :value_cols].reshape(length, head_count, HEAD_DIM)
    in_keys = mixed_in[:, value_cols : value_cols + key_cols].reshape(length, group_count, STATE)
    read_in = mixed_in[:, value_cols + key_cols :].reshape(length, group_count, STATE)
    blank = jnp.zeros((head_count, HEAD_DIM, STATE), jnp.float32)
    summed_heads = jnp.zeros(values.shape, jnp.float32)
    for direction, step_pre in ((0, pre_fwd), (1, pre_bwd)):
        step_size = jax.nn.softplus(step_pre.astype(jnp.float32) + step_bias[direction])
        log_decay = -rate[direction] * step_size
        ordered = (values, step_size, log_decay, in_keys, read_in)
        if direction == 1:
            ordered = tuple((tensor[::-1] for tensor in ordered))
        value_blocks, step_blocks, decay_blocks, key_blocks, read_blocks = [
            blocked(tensor) for tensor in ordered
        ]
        cumulative_blocks, damping_blocks, injected_blocks = jax.vmap(block_parts)(
            value_blocks, step_blocks, decay_blocks, key_blocks
        )
        block_inputs = (
            value_blocks,
            step_blocks,
            cumulative_blocks,
            damping_blocks,
            injected_blocks,
            key_blocks,
            read_blocks,
        )
        damping = jnp.exp(jnp.sum(ordered[2], axis=0))
        final_state = settle(damping_blocks, injected_blocks, blank)
        arriving = entering(damping, final_state, direction == 1)
        swept, final_state = sweep(block_inputs, arriving)
        if direction == 1:
            swept = swept[::-1]
        summed_heads = summed_heads + swept
    gated_out = summed_heads * jax.nn.silu(gate_raw.astype(jnp.float32)).reshape(values.shape)
    head_gain = norm_gain.astype(jnp.float32).reshape(head_count, HEAD_DIM)
    normed_heads = normalize(gated_out, head_gain).astype(jnp.bfloat16).reshape(length, value_cols)
    out_whole = lax.all_gather(w_out, "sp", axis=1, tiled=True)
    own_rows = lax.psum_scatter(
        jnp.dot(normed_heads, out_whole, preferred_element_type=jnp.float32).astype(jnp.bfloat16),
        "tp",
        scatter_dimension=0,
        tiled=True,
    )
    return lax.all_gather(own_rows, "tp", axis=0, tiled=True)


F32 = jnp.float32
BF16 = jnp.bfloat16
LANES = 128
VMEM_SPEC = pl.BlockSpec(memory_space=pltpu.VMEM)


def push(src, dst, send, recv, peer):
    copy = pltpu.make_async_remote_copy(
        src_ref=src,
        dst_ref=dst,
        send_sem=send,
        recv_sem=recv,
        device_id=peer,
        device_id_type=pl.DeviceIdType.MESH,
    )
    copy.start()
    return copy


def silu(x):
    return x * jax.nn.sigmoid(x)


def whole_kernel(
    n, q, tin_h, ing_h, wv, wg, wk, wr, wsf_h, wsb_h, wo, cv_h, ck_h, cr_h, bias_h, rate_h, ngain_h, out,
    tin, ing, wsf, wsb, cv, ck, cr, bias, rate, ngain,
    nrm, ws, taps, gains, tok, wts, wgt, wst, wout, raw, gate, pre, sums, vals, keys, reads, cums, yy, injf, injb, carf, carb,
    nh, full, part, both,
    tzs, tzr, tps, tpr, tss, tsr, kzs, kzr, kps, kpr, kdr, vs, vr, ss, sr, os, orr,
    as_, ar, bs, br, bdr, es, er, fs, fr, ls, ins,
):
    s, t = lax.axis_index("sp"), lax.axis_index("tp")
    z, p = s // q, s % q
    sibling = (s, 1 - t)
    half = tok.shape[2]
    depth = wv.shape[0]
    blocks = tok.shape[0] * 2 * half // BLOCK

    def at(dz, dp):
        return lax.rem(z + dz, q) * q + lax.rem(p + dp, q)

    def span(i, size):
        return pl.ds(pl.multiple_of(i * size, size), size)

    px = p + 1 - 2 * lax.rem(p, 2)
    py = lax.rem(p + 2, q)
    pd = lax.rem(px + 2, q)
    side = {"x": (z * q + px, t), "y": (z * q + py, t)}
    turns = (("x", "y"), ("y", "x"))

    def chip(dz, where):
        return lax.rem(z + q - dz, q) * q + where

    with jax.named_scope("greet"):
        barrier = pltpu.get_barrier_semaphore()
        peers = [(lax.rem(s + k, n), t) for k in range(1, n)] + [sibling]
        for peer in peers:
            pl.semaphore_signal(barrier, inc=1, device_id=peer, device_id_type=pl.DeviceIdType.MESH)

    def local(src, dst, i):
        copy = pltpu.make_async_copy(src, dst, ls.at[i])
        copy.start()
        return copy

    mine = span(s, depth)
    rows = span(t, half)
    kcol, rcol = pl.ds(LANES, LANES), pl.ds(2 * LANES, LANES)
    krcol = pl.ds(LANES, 2 * LANES)

    with jax.named_scope("load"):
        held = (
            (tin_h, tin), (ing_h, ing), (wsf_h, wsf), (wsb_h, wsb), (cv_h, cv), (ck_h, ck), (cr_h, cr),
            (bias_h, bias), (rate_h, rate), (ngain_h, ngain),
        )
        loads = [pltpu.make_async_copy(src, dst, ins.at[i]) for i, (src, dst) in enumerate(held)]
        for copy in loads:
            copy.start()
        locals_ = [
            local(wk.at[:, span(z, LANES)], wts.at[mine, kcol], 2),
            local(wr.at[:, span(z, LANES)], wts.at[mine, rcol], 3),
            local(wv.at[:, mine], wts.at[mine, pl.ds(0, LANES)], 4),
            local(wg.at[:, mine], wgt.at[mine], 5),
        ]
        for copy in loads:
            copy.wait()
    with jax.named_scope("prep"):
        wide_in = tin[...].astype(F32)
        nrm[...] = normalize(wide_in, ing[...].astype(F32).reshape(1, ing.shape[0])).astype(BF16)
        heads = wsf.shape[0]
        slot = ws.shape[0] // n
        row_i = lax.broadcasted_iota(jnp.int32, (n * slot, heads), 0)
        col_i = lax.broadcasted_iota(jnp.int32, (n * slot, heads), 1)
        place = lax.rem(row_i, slot)
        head_of = 2 * (row_i // slot)
        pick_f = jnp.where((place < 2) & (col_i == head_of + place), 1.0, 0.0).astype(BF16)
        pick_b = jnp.where((place >= 2) & (col_i == head_of + place - 2), 1.0, 0.0).astype(BF16)
        ws[...] = (
            jnp.dot(pick_f, wsf[...], preferred_element_type=F32)
            + jnp.dot(pick_b, wsb[...], preferred_element_type=F32)
        ).astype(BF16)
        own = span(s, LANES)
        taps[0:KERNEL, 0:LANES] = cv[:, own].astype(F32)
        taps[0:KERNEL, LANES : 2 * LANES] = ck[:, span(z, LANES)].astype(F32)
        taps[0:KERNEL, 2 * LANES : 3 * LANES] = cr[:, span(z, LANES)].astype(F32)
        gains[...] = ngain[...].astype(F32).reshape(n, LANES)
        lanes_of = lax.broadcasted_iota(jnp.int32, (8, heads), 1)
        rows_of = lax.broadcasted_iota(jnp.int32, (8, heads), 0)
        spread = jnp.where((rows_of < 4) & (lanes_of == 2 * s + lax.rem(rows_of, 2)), 1.0, 0.0).astype(F32)
        first_two = lax.broadcasted_iota(jnp.int32, (8, 1), 0) < 2
        across_lanes = (((1,), (1,)), ((), ()))

        def own_rows(both_dirs):
            got = lax.dot_general(
                spread, both_dirs, across_lanes, precision=FULL_PRECISION, preferred_element_type=F32
            )
            return jnp.where(first_two, got[:, 0:1], got[:, 1:2])

        offsets = own_rows(bias[...])
        rates = own_rows(rate[...])
        wst[slot:, :] = jnp.zeros((LANES - slot, wst.shape[1]), BF16)
        seq = blocks * BLOCK
        wide = 3 * LANES
        raw[0:8, :] = jnp.zeros((8, wide), F32)
        raw[seq + 8 : seq + 16, :] = jnp.zeros((8, wide), F32)
        for copy in locals_:
            copy.wait()
    with jax.named_scope("greeted"):
        pl.semaphore_wait(barrier, len(peers))

    one, last = q - 1, q
    rising, sinking = z < q - 1, z > 0
    unit = nrm.at[rows]

    def arrival(e):
        later = [[1, 2, 3], [0, 2, 3], [3, 1, 0], [2, 1, 0]]
        picked = later[q - 1][e]
        for k in range(q - 1):
            picked = jnp.where(z == k, later[k][e], picked)
        return picked

    sources = [z] + [arrival(e) for e in range(q - 1)]

    def chain(src_ref, dst_ref, sends, recvs):
        @pl.when(rising)
        def _():
            push(src_ref, dst_ref, sends.at[z], recvs.at[z], (s + q, t))

        @pl.when(sinking)
        def _():
            push(src_ref, dst_ref, sends.at[q], recvs.at[z], (s - q, t))

    def remote(src, dst, send, recv, peer):
        return pltpu.make_async_remote_copy(
            src_ref=src, dst_ref=dst, send_sem=send, recv_sem=recv,
            device_id=peer, device_id_type=pl.DeviceIdType.MESH,
        )

    def landed(ref, sem):
        remote(ref, ref, sem, sem, sibling).wait_recv()

    def left_here(ref, sem):
        remote(ref, ref, sem, sem, sibling).wait_send()

    def onward(zs):
        to = z + jnp.where(zs < z, 1, -1)
        return to, (to >= 0) & (to < q)

    def settle_chain(src_ref, sends, recvs, ref_of):
        @pl.when(rising)
        def _():
            remote(src_ref, ref_of(z), sends.at[z], recvs.at[z], (s + q, t)).wait_send()

        @pl.when(sinking)
        def _():
            remote(src_ref, ref_of(z), sends.at[q], recvs.at[z], (s - q, t)).wait_send()

        for zs in sources[1:]:
            to, ok = onward(zs)

            @pl.when(ok)
            def _():
                ref = ref_of(zs)
                remote(ref, ref, sends.at[zs], recvs.at[zs], (to * q + p, t)).wait_send()

    def tok_of(zs):
        return tok.at[zs * q + p, t]

    def wout_of(zs):
        return wout.at[:, span(zs, LANES)]

    plane, keyz, keyp, weights, swaps = {}, [], {}, [], {}
    with jax.named_scope("issue"):
        chain(unit, tok_of(z), tzs, tzr)
        for i, to in enumerate("xy"):
            plane[0, to] = push(unit, tok.at[s, t], tps.at[0], tpr.at[0, i], side[to])
        for dz in range(1, q):
            grp = span(lax.rem(z + dz, q), LANES)
            keyz.append(
                [
                    push(w.at[:, grp], wts.at[mine, col], kzs.at[0], kzr.at[dz], (at(dz, 0), t))
                    for i, (w, col) in enumerate(((wk, kcol), (wr, rcol)))
                ]
            )
        got = wts.at[mine, krcol]
        for i, to in enumerate("xy"):
            keyp[0, to] = push(got, got, kps.at[0], kpr.at[0, i], side[to])
        for k in range(1, n):
            j = lax.rem(s + k, n)
            weights.append(
                push(wv.at[:, span(j, LANES)], wts.at[mine, pl.ds(0, LANES)], vs.at[0], vr.at[0], (j, t))
            )
            weights.append(
                push(ws.at[span(j, slot)], wst.at[pl.ds(0, slot), mine], ss.at[0], sr.at[0], (j, t))
            )
        locals_ = [
            local(nrm.at[pl.ds(0, half)], tok.at[s, 0], 0),
            local(nrm.at[pl.ds(half, half)], tok.at[s, 1], 1),
            local(ws.at[span(s, slot)], wst.at[pl.ds(0, slot), mine], 6),
            local(wo, wout_of(z), 7),
        ]

    gates = []

    def send_gates():
        for k in range(1, n):
            j = lax.rem(s + k, n)
            gates.append(push(wg.at[:, span(j, LANES)], wgt.at[mine], vs.at[1], vr.at[1], (j, t)))

    def swap(e, i):
        src = sources[e] * q + (p, px, py, pd)[i]
        swaps[e, i] = push(tok.at[src, t], tok.at[src, t], tss.at[0], tsr.at[e], sibling)

    def arrive(e):
        with jax.named_scope("arrive"):
            zs = sources[e]
            ref = tok_of(zs)
            remote(ref, ref, tzs.at[zs], tzr.at[zs], sibling).wait_recv()
            to, ok = onward(zs)

            @pl.when(ok)
            def _():
                push(ref, ref, tzs.at[zs], tzr.at[zs], (to * q + p, t))

    def spread_plane(e):
        ref = tok_of(sources[e])
        for i, way in enumerate("xy"):
            plane[e, way] = push(ref, ref, tps.at[0], tpr.at[e, i], side[way])
        swap(e, 0)

    quarter = half // 2

    def relay(e):
        with jax.named_scope("relay"):
            for i, (near_by, other) in enumerate(turns):
                plane[e, near_by].wait_recv()
                ref = tok.at[sources[e] * q + (px, py)[i], t, pl.ds(i * quarter, quarter)]
                plane[e, other + "d"] = push(ref, ref, tps.at[0], tpr.at[e, 2], side[other])
                swap(e, 1 + i)

    def key_arrive(dz):
        with jax.named_scope("key_arrive"):
            landed(wgt.at[pl.ds(0, 2 * depth)], kzr.at[dz])
            ref = wts.at[span(at(q - dz, 0), depth), krcol]
            for i, to in enumerate("xy"):
                keyp[dz, to] = push(ref, ref, kps.at[0], kpr.at[dz, i], side[to])

    def key_relay(dz):
        with jax.named_scope("key_relay"):
            for i, (near_by, other) in enumerate(turns):
                keyp[dz, near_by].wait_recv()
                ref = wts.at[span(chip(dz, (px, py)[i]), depth), (kcol, rcol)[i]]
                keyp[dz, other + "d"] = push(ref, ref, kps.at[0], kdr.at[0], side[other])

    ri = lax.broadcasted_iota(jnp.int32, (BLOCK, BLOCK), 0)
    ci = lax.broadcasted_iota(jnp.int32, (BLOCK, BLOCK), 1)
    low = ri >= ci
    diag = ri == ci
    left = ci < HEAD_DIM
    until = jnp.where(ri <= ci, 1.0, 0.0).astype(BF16)
    since = jnp.where(low, 1.0, 0.0).astype(BF16)
    sums_of = jnp.concatenate([until, since], axis=1)
    pick = jnp.where(ri[0:8] == ci[0:8], 1.0, 0.0).astype(BF16)

    def project(zs):
        r0 = pl.multiple_of(zs * q * BLOCK, q * BLOCK)
        whole_plane = pl.ds(r0, q * BLOCK)
        x = tok[pl.ds(zs * q, q)].reshape(q * BLOCK, tok.shape[3])
        got = jnp.dot(x, wts[...], preferred_element_type=F32).astype(BF16)
        raw[pl.ds(r0 + 8, q * BLOCK), :] = got[:, 0 : 3 * LANES].astype(F32)
        u = lax.dot_general(pick, got[:, 3 * LANES :], across_lanes, preferred_element_type=F32) + offsets
        steps = jnp.maximum(u, 0.0) + jnp.log1p(jnp.exp(-jnp.abs(u)))
        pre[:, whole_plane] = steps
        decay = -rates * steps
        parts = []
        for b in range(q):
            rest = decay[:, b * BLOCK : (b + 1) * BLOCK]
            for _ in range(3):
                piece = rest.astype(BF16).astype(F32)
                parts.append(piece)
                rest = rest - piece
        summed = jnp.dot(jnp.concatenate(parts, axis=0).astype(BF16), sums_of, preferred_element_type=F32)
        for b in range(q):
            at_b = pl.ds(pl.multiple_of((zs * q + b) * BLOCK, BLOCK), BLOCK)
            got = [summed[24 * b + 8 * k : 24 * b + 8 * k + 8] for k in range(3)]
            both_sums = got[0] + (got[1] + got[2])
            c = jnp.where(first_two, both_sums[:, 0:BLOCK], both_sums[:, BLOCK:])
            c_end = jnp.where(first_two, c[:, BLOCK - 1 : BLOCK], c[:, 0:1])
            sums[:, at_b] = c
            weighting = jnp.exp(c_end - c) * steps[:, b * BLOCK : (b + 1) * BLOCK]
            stacked = jnp.concatenate([c, weighting, jnp.exp(c), jnp.zeros((LANES - 24, BLOCK), F32)], axis=0)
            cums[at_b, :] = stacked.T

    def open_gate(zs):
        with jax.named_scope("gate"):
            x = tok[pl.ds(zs * q, q)].reshape(q * BLOCK, tok.shape[3])
            here = pl.ds(pl.multiple_of(zs * q * BLOCK, q * BLOCK), q * BLOCK)
            gate[here, :] = jnp.dot(x, wgt[...], preferred_element_type=F32).astype(BF16)

    def convolve(i):
        r0 = pl.multiple_of(i * BLOCK, BLOCK)
        for b, dst in enumerate((vals, keys, reads)):
            window = raw[pl.ds(r0, BLOCK + 16), b * LANES : (b + 1) * LANES]
            total = jnp.zeros((BLOCK, LANES), F32)
            for k in range(KERNEL):
                lo = 8 - (KERNEL - 1) // 2 + k
                total = total + window[lo : lo + BLOCK] * taps[k : k + 1, b * LANES : (b + 1) * LANES]
            dst[pl.ds(r0, BLOCK), :] = silu(total).astype(BF16)

    def within(i):
        r0 = pl.multiple_of(i * BLOCK, BLOCK)
        here = pl.ds(r0, BLOCK)
        c, ct, stt = cums[here, :], sums[:, here], pre[:, here]
        key, read, val = keys[here, :], reads[here, :], vals[here, :]
        val32 = val.astype(F32)
        score = lax.dot_general(read, key, across_lanes, preferred_element_type=F32)
        total = jnp.zeros((BLOCK, LANES), F32)
        for h in range(2):
            gap = jnp.where(low, c[:, h : h + 1] - ct[h : h + 1, :], c[:, h + 2 : h + 3] - ct[h + 2 : h + 3, :])
            sb = stt[h + 2 : h + 3, :]
            e = jnp.exp(gap) * jnp.where(low, stt[h : h + 1, :], sb) + jnp.where(diag, sb, 0.0)
            mask = left if h == 0 else jnp.logical_not(left)
            own_val = jnp.where(mask, val32, 0.0).astype(BF16)
            total = total + jnp.dot((score * e).astype(BF16), own_val, preferred_element_type=F32)
        yy[here, :] = total
        key_t = key.astype(F32).T.astype(BF16)
        for d, dst in ((0, injf), (1, injb)):
            w = jnp.where(left, c[:, 8 + 2 * d : 9 + 2 * d], c[:, 9 + 2 * d : 10 + 2 * d])
            scaled = (val32 * w).astype(BF16)
            dst[i] = jnp.dot(key_t, scaled, preferred_element_type=F32)

    def use(e):
        zs = sources[e]
        with jax.named_scope("usewait"):
            landed(tok.at[0, 0], tpr.at[e, 2])
            swap(e, 3)
            landed(tok.at[pl.ds(0, q if e else q - 1), 0], tsr.at[e])
        with jax.named_scope("project"):
            project(zs)
        edge = jnp.where(zs == 0, 0, blocks - 1)
        if e == 0:
            start, count = zs * q + 1, q - 2
        else:
            start, count = zs * q + jnp.where(zs > z, -1, 1), q
        if e == q - 1:
            count = count + 1

        def which(i):
            return start + i if e < q - 1 else jnp.where(i < q, start + i, edge)

        if e == q - 1:
            open_gate(zs)
        with jax.named_scope("conv"):

            @pl.loop(0, count, unroll=count)
            def _(i):
                convolve(which(i))

        with jax.named_scope("intra"):

            @pl.loop(0, count, unroll=count)
            def _(i):
                within(which(i))

        if e < q - 1:

            @pl.when((zs == 0) | (zs == q - 1))
            def _():
                convolve(edge)
                within(edge)

    def wout_onward(e):
        zs = sources[e]
        to, ok = onward(zs)

        @pl.when(ok)
        def _():
            ref = wout_of(zs)
            remote(ref, ref, os.at[zs], orr.at[zs], sibling).wait_recv()
            push(ref, ref, os.at[zs], orr.at[zs], (to * q + p, t))

    def wout_arrive(e):
        zs = sources[e]
        to, ok = onward(zs)

        @pl.when(jnp.logical_not(ok))
        def _():
            ref = wout_of(zs)
            remote(ref, ref, os.at[zs], orr.at[zs], sibling).wait_recv()

    arrive(1)
    relay(0)
    for dz in range(1, q):
        key_arrive(dz)
    key_relay(0)
    spread_plane(1)
    for dz in range(1, q):
        key_relay(dz)
    arrive(2)
    spread_plane(2)
    relay(1)
    send_gates()
    with jax.named_scope("weights"):
        for copy in locals_:
            copy.wait()
        landed(wgt.at[pl.ds(0, (n - 1) * depth)], vr.at[0])
        landed(ws.at[pl.ds(0, (n - 1) * slot)], sr.at[0])
        landed(wgt.at[pl.ds(0, 2 * q * depth)], kdr.at[0])
    with jax.named_scope("turn"):
        for k in range(wst.shape[1] // LANES):
            chunk = slice(k * LANES, (k + 1) * LANES)
            wts[chunk, 3 * LANES :] = wst[:, chunk].astype(F32).T.astype(BF16)
    use(0)
    arrive(3)
    spread_plane(3)
    chain(wo, wout_of(z), os, orr)
    relay(2)
    use(1)
    relay(3)
    use(2)
    with jax.named_scope("gates"):
        landed(wgt.at[pl.ds(0, (n - 1) * depth)], vr.at[1])
    for e in range(q - 1):
        open_gate(sources[e])
    with jax.named_scope("wout1"):
        wout_onward(1)
        wout_onward(2)
    use(3)

    def carry(i, state, d, inj, kept):
        r0 = pl.multiple_of(i * BLOCK, BLOCK)
        here = pl.ds(r0, BLOCK)
        grown = jnp.where(left, cums[here, 16 + 2 * d : 17 + 2 * d], cums[here, 17 + 2 * d : 18 + 2 * d])
        high = state.astype(BF16)
        rest = (state - high.astype(F32)).astype(BF16)
        read = reads[here, :]
        add = jnp.dot(read, high, preferred_element_type=F32) + jnp.dot(
            read, rest, preferred_element_type=F32
        )
        kept[here, :] = add * grown
        end = grown[BLOCK - 1 : BLOCK, :] if d == 0 else grown[0:1, :]
        return state * end + inj[i]

    def advance(i, states):
        return (
            carry(i, states[0], 0, injf, carf),
            carry(blocks - 1 - i, states[1], 1, injb, carb),
        )

    with jax.named_scope("carry"):
        zero = jnp.zeros((STATE, LANES), F32)
        lax.fori_loop(0, blocks, advance, (zero, zero), unroll=4)

    gain = gains[pl.ds(s, 1), :]

    def finish(i):
        r0 = pl.multiple_of(i * BLOCK, BLOCK)
        here = pl.ds(r0, BLOCK)
        g = (yy[here, :] + carf[here, :] + carb[here, :]) * silu(gate[here, :].astype(F32))
        sq = g * g
        m0 = jnp.sum(jnp.where(left, sq, 0.0), -1, keepdims=True) / HEAD_DIM
        m1 = jnp.sum(jnp.where(left, 0.0, sq), -1, keepdims=True) / HEAD_DIM
        scale = jnp.where(left, lax.rsqrt(m0 + EPSILON), lax.rsqrt(m1 + EPSILON))
        nh[here, :] = (g * scale * gain).astype(BF16)

    away = []
    for dz in range(1, q + 1):
        to = lax.rem(z + dz, q)

        with jax.named_scope("finish"):

            @pl.loop(0, q, unroll=4)
            def _(i):
                finish(to * q + i)

        if dz < q:
            away.append(
                push(nh.at[span(to, q * BLOCK)], full.at[:, mine], as_.at[0], ar.at[dz], (at(dz, 0), t))
            )
    near = {}
    keep = local(nh.at[span(z, q * BLOCK)], full.at[:, mine], 8)
    for i, to in enumerate("xy"):
        near[0, to] = push(
            nh.at[span(z, q * BLOCK)], full.at[:, mine], bs.at[0], br.at[0, i], side[to]
        )
    rest_rows = q * BLOCK // 2

    def near_relay(dz):
        with jax.named_scope("nearwait"):
            for i, (near_by, other) in enumerate(turns):
                near[dz, near_by].wait_recv()
                got = full.at[pl.ds(i * rest_rows, rest_rows), span(chip(dz, (px, py)[i]), LANES)]
                near[dz, other + "d"] = push(got, got, bs.at[0], bdr.at[0], side[other])

    for dz in range(1, q):
        with jax.named_scope("awaywait"):
            away[dz - 1].wait_recv()
        got = full.at[:, span(at(q - dz, 0), LANES)]
        for i, to in enumerate("xy"):
            near[dz, to] = push(got, got, bs.at[0], br.at[dz, i], side[to])
        near_relay(dz - 1)
        if dz == 2:
            with jax.named_scope("wout2"):
                wout_onward(3)
    near_relay(q - 1)
    with jax.named_scope("outswait"):
        for e in range(1, q):
            wout_arrive(e)
    with jax.named_scope("fullwait"):
        keep.wait()
        landed(full.at[pl.ds(0, BLOCK)], bdr.at[0])
    legs = []

    def leg(dp):
        to = lax.rem(p + dp, q)
        legs.append(push(part.at[to], both.at[t, p], es.at[0], er.at[dp], (at(0, dp), t)))

    with jax.named_scope("outdot"):
        for dp in range(1, q + 1):
            to = lax.rem(p + dp, q)
            part[to] = jnp.dot(full[span(to, BLOCK), :], wout[...], preferred_element_type=F32).astype(BF16)
            if dp >= 2:
                leg(dp - 1)
    across = [push(part.at[p], both.at[t, p], fs.at[0], fr.at[0], sibling)]
    keep = local(part.at[p], both.at[t, p], 9)
    with jax.named_scope("legswait"):
        for dp in range(1, q):
            legs[dp - 1].wait_recv()
            got = both.at[t, lax.rem(p + q - dp, q)]
            across.append(push(got, got, fs.at[0], fr.at[0], sibling))
    with jax.named_scope("acrosswait"):
        keep.wait()
        landed(part, fr.at[0])
    with jax.named_scope("sum"):
        for a in range(q):
            for b in range(q):
                here = slice(a * LANES, (a + 1) * LANES)
                total = both[0, b, :, here].astype(F32) + both[1, b, :, here].astype(F32)
                out[:, (a * q + b) * LANES : (a * q + b + 1) * LANES] = total.astype(BF16)
    with jax.named_scope("sends"):
        settle_chain(unit, tzs, tzr, tok_of)
        settle_chain(wo, os, orr, wout_of)
        left_here(tok.at[pl.ds(0, 3 * q), 0], tps.at[0])
        left_here(tok.at[pl.ds(0, n - 1), 0], tss.at[0])
        left_here(wgt.at[pl.ds(0, 2 * (q - 1) * depth)], kzs.at[0])
        left_here(wts.at[pl.ds(0, 6 * depth)], kps.at[0])
        left_here(wgt.at[pl.ds(0, (n - 1) * depth)], vs.at[0])
        left_here(wgt.at[pl.ds(0, (n - 1) * depth)], vs.at[1])
        left_here(ws.at[pl.ds(0, (n - 1) * slot)], ss.at[0])
        left_here(nh.at[pl.ds(0, (q - 1) * q * BLOCK)], as_.at[0])
        left_here(full.at[pl.ds(0, 3 * BLOCK)], bs.at[0])
        left_here(part.at[pl.ds(0, q - 1)], es.at[0])
        left_here(part, fs.at[0])


def whole(n, q, *args):
    dma = pltpu.SemaphoreType.DMA
    vm = pltpu.VMEM
    tokens, wo, wsf = args[0], args[8], args[6]
    depth, width = tokens.shape
    seq = n * depth
    slot = 16
    return pl.pallas_call(
        functools.partial(whole_kernel, n, q),
        out_shape=jax.ShapeDtypeStruct((BLOCK, n * LANES), BF16),
        in_specs=[HBM_SPEC] * len(args),
        out_specs=VMEM_SPEC,
        scratch_shapes=[
            *[vm(args[i].shape, args[i].dtype) for i in (0, 1, 6, 7, 9, 10, 11, 12, 13, 14)],
            vm((depth, width), BF16),
            vm((n * slot, depth), BF16),
            vm((8, 3 * LANES), F32),
            vm((n, LANES), F32),
            vm((n, 2, depth // 2, width), BF16),
            vm((width, 4 * LANES), BF16),
            vm((width, LANES), BF16),
            vm((LANES, width), BF16),
            vm((wo.shape[0], q * LANES), BF16),
            vm((seq + 16, 3 * LANES), F32),
            vm((seq, LANES), BF16),
            vm((8, seq), F32),
            vm((8, seq), F32),
            vm((seq, LANES), BF16),
            vm((seq, LANES), BF16),
            vm((seq, LANES), BF16),
            vm((seq, LANES), F32),
            vm((seq, LANES), F32),
            vm((seq // BLOCK, STATE, LANES), F32),
            vm((seq // BLOCK, STATE, LANES), F32),
            vm((seq, LANES), F32),
            vm((seq, LANES), F32),
            vm((seq, LANES), BF16),
            vm((q * BLOCK, n * LANES), BF16),
            vm((q, BLOCK, q * LANES), BF16),
            vm((2, q, BLOCK, q * LANES), BF16),
            dma((q + 1,)), dma((q,)), dma((1,)), dma((q, 3)), dma((1,)), dma((q,)),
            dma((1,)), dma((q,)), dma((1,)), dma((q, 2)), dma((1,)),
            dma((2,)), dma((2,)), dma((1,)), dma((1,)), dma((q + 1,)), dma((q,)),
            dma((1,)), dma((q,)), dma((1,)), dma((q, 2)), dma((1,)), dma((1,)), dma((q,)),
            dma((1,)), dma((1,)), dma((10,)), dma((10,)),
        ],
        compiler_params=pltpu.CompilerParams(
            collective_id=0, has_side_effects=True, vmem_limit_bytes=VMEM_LIMIT << 10
        ),
        name="whole",
    )(*args)


VMEM_LIMIT = 57344
HBM_SPEC = pl.BlockSpec(memory_space=pltpu.HBM)


def headwise(
    n,
    q,
    tokens,
    in_gain,
    w_value,
    w_gate,
    w_in_key,
    w_read,
    w_step_fwd,
    w_step_bwd,
    conv_value,
    conv_key,
    conv_read,
    step_bias,
    rate,
    norm_gain,
    w_out,
):
    return whole(
        n, q, tokens, in_gain, w_value, w_gate, w_in_key, w_read, w_step_fwd.T, w_step_bwd.T, w_out,
        conv_value, conv_key, conv_read, step_bias, rate, norm_gain,
    )


def whole_heads(mesh):
    n, q = mesh.shape["sp"], math.isqrt(mesh.shape["sp"])

    def run(*args):
        cols, keys = args[2].shape[1], args[4].shape[1]
        ready = (
            q * q == n
            and mesh.shape["tp"] == 2
            and cols == n * LANES
            and args[14].shape[1] == LANES
            and keys == q * LANES
            and q == 4
            and args[0].shape[1] == n * LANES
            and args[0].shape[0] == BLOCK
        )
        return headwise(n, q, *args) if ready else body(*args)

    return run


def solution(mesh):
    in_specs = (
        P("sp", None),
        P(),
        P("sp", "tp"),
        P("sp", "tp"),
        P("sp", "tp"),
        P("sp", "tp"),
        P("sp", "tp"),
        P("sp", "tp"),
        P(None, "tp"),
        P(None, "tp"),
        P(None, "tp"),
        P(None, "tp"),
        P(None, "tp"),
        P("tp"),
        P("tp", "sp"),
    )
    out_specs = P("sp", None)
    return jax.shard_map(whole_heads(mesh), mesh=mesh, in_specs=in_specs, out_specs=out_specs, check_vma=False)
```

```python
import functools
import math

import jax
import jax.numpy as jnp
from jax import lax
from jax.experimental import pallas as pl
from jax.experimental.pallas import tpu as pltpu
from jax.sharding import PartitionSpec as P

HEAD_DIM = 64
STATE = 128
KERNEL = 5
BLOCK = 128


EPSILON = 1e-05
FULL_PRECISION = lax.Precision.HIGHEST


def entering_2(x, axis, combine, identity, reverse):
    length, place = (lax.axis_size(axis), lax.axis_index(axis))
    everything = jax.tree.map(lambda part: lax.all_gather(part, axis), x)
    start = jax.tree.map(
        lambda part, zero: jnp.broadcast_to(jnp.asarray(zero, part.dtype), part.shape), x, identity
    )

    def step(k, before):
        at = length - 1 - k if reverse else k
        reached = at > place if reverse else at < place
        new = combine(before, jax.tree.map(lambda part: part[at], everything))
        return jax.tree.map(lambda a, b: jnp.where(reached, a, b), new, before)

    return lax.fori_loop(0, length, step, start)


def with_halo(cells, sides, width):
    for axis, dim in sides:
        count = lax.axis_size(axis)
        ends = count - 1
        head = lax.slice_in_dim(cells, 0, width, axis=dim)
        tail = lax.slice_in_dim(cells, cells.shape[dim] - width, cells.shape[dim], axis=dim)
        cells = jnp.concatenate(
            [
                lax.ppermute(tail, axis, [(i, (i + 1) % count) for i in range(ends)]),
                cells,
                lax.ppermute(head, axis, [((i + 1) % count, i) for i in range(ends)]),
            ],
            axis=dim,
        )
    return cells


def normalize(tensor, gain):
    return tensor * lax.rsqrt(jnp.mean(tensor * tensor, -1, keepdims=True) + EPSILON) * gain


def block_parts(values, step_size, log_decay, in_keys):
    per_group = values.shape[1] // in_keys.shape[1]
    cumulative = jnp.cumsum(log_decay, axis=0)
    log_total = cumulative[-1]
    weighting = jnp.exp(log_total[None, :] - cumulative) * step_size
    key_heads = jnp.repeat(in_keys, per_group, axis=1)
    scaled = (values.astype(jnp.float32) * weighting[:, :, None]).astype(jnp.bfloat16)
    injected = jnp.einsum("jhn,jhp->hpn", key_heads, scaled, preferred_element_type=jnp.float32)
    return (cumulative, jnp.exp(log_total), injected)


def block_step(memory, inputs):
    values, step_size, cumulative, damping, injected, in_keys, read_in = inputs
    per_group = values.shape[1] // in_keys.shape[1]
    scores = jnp.einsum("ign,jgn->ijg", read_in, in_keys, preferred_element_type=jnp.float32)
    scores = jnp.repeat(scores, per_group, axis=2)
    length = values.shape[0]
    below_mask = (jnp.arange(length)[:, None] >= jnp.arange(length)[None, :])[:, :, None]
    gaps = jnp.where(below_mask, cumulative[:, None, :] - cumulative[None, :, :], -jnp.inf)
    weights = (scores * jnp.exp(gaps) * step_size[None, :, :]).astype(jnp.bfloat16)
    within = jnp.einsum("ijh,jhp->ihp", weights, values, preferred_element_type=jnp.float32)
    read_heads = jnp.repeat(read_in.astype(jnp.float32), per_group, axis=1)
    carried = (
        jnp.einsum("ihn,hpn->ihp", read_heads, memory, precision=FULL_PRECISION)
        * jnp.exp(cumulative)[:, :, None]
    )
    memory = damping[:, None, None] * memory + injected
    return (memory, within + carried)


def blocked(tensor):
    blocks = tensor.shape[0] // BLOCK
    return tensor.reshape((blocks, BLOCK) + tensor.shape[1:])


def sweep(block_inputs, memory):
    memory, swept = lax.scan(block_step, memory, block_inputs)
    return (swept.reshape((swept.shape[0] * swept.shape[1],) + swept.shape[2:]), memory)


def settle(damping_blocks, injected_blocks, memory):

    def advance(memory, inputs):
        return (inputs[0][:, None, None] * memory + inputs[1], None)

    memory, unused = lax.scan(advance, memory, (damping_blocks, injected_blocks))
    return memory


def chain(before_pair, after_pair):
    return (
        before_pair[0] * after_pair[0],
        after_pair[0][:, None, None] * before_pair[1] + after_pair[1],
    )


def entering(damping, final_state, backward):
    identity_pair = (jnp.ones_like(damping), jnp.zeros_like(final_state))
    if backward:
        arrived = entering_2((damping, final_state), "sp", chain, identity_pair, True)
    else:
        arrived = entering_2((damping, final_state), "sp", chain, identity_pair, False)
    return arrived[1]


def body(
    tokens,
    in_gain,
    w_value,
    w_gate,
    w_in_key,
    w_read,
    w_step_fwd,
    w_step_bwd,
    conv_value,
    conv_key,
    conv_read,
    step_bias,
    rate,
    norm_gain,
    w_out,
):
    normed = normalize(tokens.astype(jnp.float32), in_gain.astype(jnp.float32)).astype(jnp.bfloat16)
    weights = (
        lax.all_gather(w_value, "sp", axis=0, tiled=True),
        lax.all_gather(w_gate, "sp", axis=0, tiled=True),
        lax.all_gather(w_in_key, "sp", axis=0, tiled=True),
        lax.all_gather(w_read, "sp", axis=0, tiled=True),
        lax.all_gather(w_step_fwd, "sp", axis=0, tiled=True),
        lax.all_gather(w_step_bwd, "sp", axis=0, tiled=True),
    )
    projected = [
        jnp.dot(normed, weight, preferred_element_type=jnp.float32).astype(jnp.bfloat16)
        for weight in weights
    ]
    value_raw, gate_raw, key_raw, read_raw, pre_fwd, pre_bwd = projected
    value_cols = value_raw.shape[1]
    key_cols = key_raw.shape[1]
    joined = jnp.concatenate([value_raw, key_raw, read_raw], axis=1)
    padded = with_halo(joined, (("sp", 0),), (KERNEL - 1) // 2)
    kernel_taps = jnp.concatenate([conv_value, conv_key, conv_read], axis=1).astype(jnp.float32)
    length = joined.shape[0]
    summed = jnp.zeros(joined.shape, jnp.float32)
    for offset in range(KERNEL):
        summed = summed + padded[offset : offset + length].astype(jnp.float32) * kernel_taps[offset]
    mixed_in = jax.nn.silu(summed).astype(jnp.bfloat16)
    head_count = value_cols // HEAD_DIM
    group_count = key_cols // STATE
    values = mixed_in[:, :value_cols].reshape(length, head_count, HEAD_DIM)
    in_keys = mixed_in[:, value_cols : value_cols + key_cols].reshape(length, group_count, STATE)
    read_in = mixed_in[:, value_cols + key_cols :].reshape(length, group_count, STATE)
    blank = jnp.zeros((head_count, HEAD_DIM, STATE), jnp.float32)
    summed_heads = jnp.zeros(values.shape, jnp.float32)
    for direction, step_pre in ((0, pre_fwd), (1, pre_bwd)):
        step_size = jax.nn.softplus(step_pre.astype(jnp.float32) + step_bias[direction])
        log_decay = -rate[direction] * step_size
        ordered = (values, step_size, log_decay, in_keys, read_in)
        if direction == 1:
            ordered = tuple((tensor[::-1] for tensor in ordered))
        value_blocks, step_blocks, decay_blocks, key_blocks, read_blocks = [
            blocked(tensor) for tensor in ordered
        ]
        cumulative_blocks, damping_blocks, injected_blocks = jax.vmap(block_parts)(
            value_blocks, step_blocks, decay_blocks, key_blocks
        )
        block_inputs = (
            value_blocks,
            step_blocks,
            cumulative_blocks,
            damping_blocks,
            injected_blocks,
            key_blocks,
            read_blocks,
        )
        damping = jnp.exp(jnp.sum(ordered[2], axis=0))
        final_state = settle(damping_blocks, injected_blocks, blank)
        arriving = entering(damping, final_state, direction == 1)
        swept, final_state = sweep(block_inputs, arriving)
        if direction == 1:
            swept = swept[::-1]
        summed_heads = summed_heads + swept
    gated_out = summed_heads * jax.nn.silu(gate_raw.astype(jnp.float32)).reshape(values.shape)
    head_gain = norm_gain.astype(jnp.float32).reshape(head_count, HEAD_DIM)
    normed_heads = normalize(gated_out, head_gain).astype(jnp.bfloat16).reshape(length, value_cols)
    out_whole = lax.all_gather(w_out, "sp", axis=1, tiled=True)
    own_rows = lax.psum_scatter(
        jnp.dot(normed_heads, out_whole, preferred_element_type=jnp.float32).astype(jnp.bfloat16),
        "tp",
        scatter_dimension=0,
        tiled=True,
    )
    return lax.all_gather(own_rows, "tp", axis=0, tiled=True)


F32 = jnp.float32
BF16 = jnp.bfloat16
LANES = 128
VMEM_SPEC = pl.BlockSpec(memory_space=pltpu.VMEM)


def push(src, dst, send, recv, peer):
    copy = pltpu.make_async_remote_copy(
        src_ref=src,
        dst_ref=dst,
        send_sem=send,
        recv_sem=recv,
        device_id=peer,
        device_id_type=pl.DeviceIdType.MESH,
    )
    copy.start()
    return copy


def silu(x):
    return x * jax.nn.sigmoid(x)


def whole_kernel(
    n, q, tin_h, ing_h, wv, wg, wk, wr, wsf_h, wsb_h, wo, cv_h, ck_h, cr_h, bias_h, rate_h, ngain_h, out,
    tin, ing, wsf, wsb, cv, ck, cr, bias, rate, ngain,
    nrm, ws, taps, gains, tok, wts, wgt, wst, wout, raw, gate, pre, sums, vals, keys, reads, cums, yy, injf, injb, entered,
    nh, full, part, other, summed_up, both,
    tzs, tzr, tps, tpr, tss, tsr, kzs, kzr, kps, kpr, kdr, vs, vr, ss, sr, os, orr,
    as_, ar, bs, br, bdr, xs, xr, es, er, fs, fr, ls, ins,
):
    s, t = lax.axis_index("sp"), lax.axis_index("tp")
    z, p = s // q, s % q
    sibling = (s, 1 - t)
    half = tok.shape[2]
    depth = wv.shape[0]
    blocks = tok.shape[0] * 2 * half // BLOCK

    def at(dz, dp):
        return lax.rem(z + dz, q) * q + lax.rem(p + dp, q)

    def span(i, size):
        return pl.ds(pl.multiple_of(i * size, size), size)

    px = p + 1 - 2 * lax.rem(p, 2)
    py = lax.rem(p + 2, q)
    pd = lax.rem(px + 2, q)
    side = {"x": (z * q + px, t), "y": (z * q + py, t)}
    turns = (("x", "y"), ("y", "x"))

    def chip(dz, where):
        return lax.rem(z + q - dz, q) * q + where

    with jax.named_scope("greet"):
        barrier = pltpu.get_barrier_semaphore()
        peers = [(lax.rem(s + k, n), t) for k in range(1, n)] + [sibling]
        for peer in peers:
            pl.semaphore_signal(barrier, inc=1, device_id=peer, device_id_type=pl.DeviceIdType.MESH)

    def local(src, dst, i):
        copy = pltpu.make_async_copy(src, dst, ls.at[i])
        copy.start()
        return copy

    mine = span(s, depth)
    rows = span(t, half)
    kcol, rcol = pl.ds(LANES, LANES), pl.ds(2 * LANES, LANES)
    krcol = pl.ds(LANES, 2 * LANES)

    with jax.named_scope("load"):
        held = (
            (tin_h, tin), (ing_h, ing), (wsf_h, wsf), (wsb_h, wsb), (cv_h, cv), (ck_h, ck), (cr_h, cr),
            (bias_h, bias), (rate_h, rate), (ngain_h, ngain),
        )
        loads = [pltpu.make_async_copy(src, dst, ins.at[i]) for i, (src, dst) in enumerate(held)]
        for copy in loads:
            copy.start()
        locals_ = [
            local(wk.at[:, span(z, LANES)], wts.at[mine, kcol], 2),
            local(wr.at[:, span(z, LANES)], wts.at[mine, rcol], 3),
            local(wv.at[:, mine], wts.at[mine, pl.ds(0, LANES)], 4),
            local(wg.at[:, mine], wgt.at[mine], 5),
        ]
        for copy in loads:
            copy.wait()
    with jax.named_scope("prep"):
        wide_in = tin[...].astype(F32)
        nrm[...] = normalize(wide_in, ing[...].astype(F32).reshape(1, ing.shape[0])).astype(BF16)
        heads = wsf.shape[0]
        slot = ws.shape[0] // n
        row_i = lax.broadcasted_iota(jnp.int32, (n * slot, heads), 0)
        col_i = lax.broadcasted_iota(jnp.int32, (n * slot, heads), 1)
        place = lax.rem(row_i, slot)
        head_of = 2 * (row_i // slot)
        pick_f = jnp.where((place < 2) & (col_i == head_of + place), 1.0, 0.0).astype(BF16)
        pick_b = jnp.where((place >= 2) & (col_i == head_of + place - 2), 1.0, 0.0).astype(BF16)
        ws[...] = (
            jnp.dot(pick_f, wsf[...], preferred_element_type=F32)
            + jnp.dot(pick_b, wsb[...], preferred_element_type=F32)
        ).astype(BF16)
        own = span(s, LANES)
        taps[0:KERNEL, 0:LANES] = cv[:, own].astype(F32)
        taps[0:KERNEL, LANES : 2 * LANES] = ck[:, span(z, LANES)].astype(F32)
        taps[0:KERNEL, 2 * LANES : 3 * LANES] = cr[:, span(z, LANES)].astype(F32)
        gains[...] = ngain[...].astype(F32).reshape(n, LANES)
        lanes_of = lax.broadcasted_iota(jnp.int32, (8, heads), 1)
        rows_of = lax.broadcasted_iota(jnp.int32, (8, heads), 0)
        spread = jnp.where((rows_of < 4) & (lanes_of == 2 * s + lax.rem(rows_of, 2)), 1.0, 0.0).astype(F32)
        first_two = lax.broadcasted_iota(jnp.int32, (8, 1), 0) < 2
        across_lanes = (((1,), (1,)), ((), ()))

        def own_rows(both_dirs):
            got = lax.dot_general(
                spread, both_dirs, across_lanes, precision=FULL_PRECISION, preferred_element_type=F32
            )
            return jnp.where(first_two, got[:, 0:1], got[:, 1:2])

        offsets = own_rows(bias[...])
        rates = own_rows(rate[...])
        wst[slot:, :] = jnp.zeros((LANES - slot, wst.shape[1]), BF16)
        seq = blocks * BLOCK
        wide = 3 * LANES
        raw[0:8, :] = jnp.zeros((8, wide), F32)
        raw[seq + 8 : seq + 16, :] = jnp.zeros((8, wide), F32)
        for copy in locals_:
            copy.wait()
    with jax.named_scope("greeted"):
        pl.semaphore_wait(barrier, len(peers))

    one, last = q - 1, q
    rising, sinking = z < q - 1, z > 0
    unit = nrm.at[rows]

    def arrival(e):
        later = [[1, 2, 3], [0, 2, 3], [3, 1, 0], [2, 1, 0]]
        picked = later[q - 1][e]
        for k in range(q - 1):
            picked = jnp.where(z == k, later[k][e], picked)
        return picked

    sources = [z] + [arrival(e) for e in range(q - 1)]

    def chain(src_ref, dst_ref, sends, recvs):
        @pl.when(rising)
        def _():
            push(src_ref, dst_ref, sends.at[z], recvs.at[z], (s + q, t))

        @pl.when(sinking)
        def _():
            push(src_ref, dst_ref, sends.at[q], recvs.at[z], (s - q, t))

    def remote(src, dst, send, recv, peer):
        return pltpu.make_async_remote_copy(
            src_ref=src, dst_ref=dst, send_sem=send, recv_sem=recv,
            device_id=peer, device_id_type=pl.DeviceIdType.MESH,
        )

    def landed(ref, sem):
        remote(ref, ref, sem, sem, sibling).wait_recv()

    def left_here(ref, sem):
        remote(ref, ref, sem, sem, sibling).wait_send()

    def onward(zs):
        to = z + jnp.where(zs < z, 1, -1)
        return to, (to >= 0) & (to < q)

    def settle_chain(src_ref, sends, recvs, ref_of):
        @pl.when(rising)
        def _():
            remote(src_ref, ref_of(z), sends.at[z], recvs.at[z], (s + q, t)).wait_send()

        @pl.when(sinking)
        def _():
            remote(src_ref, ref_of(z), sends.at[q], recvs.at[z], (s - q, t)).wait_send()

        for zs in sources[1:]:
            to, ok = onward(zs)

            @pl.when(ok)
            def _():
                ref = ref_of(zs)
                remote(ref, ref, sends.at[zs], recvs.at[zs], (to * q + p, t)).wait_send()

    def tok_of(zs):
        return tok.at[zs * q + p, t]

    def wout_of(zs):
        return wout.at[:, span(zs, LANES)]

    plane, keyz, keyp, weights, swaps = {}, [], {}, [], {}
    with jax.named_scope("issue"):
        chain(unit, tok_of(z), tzs, tzr)
        for i, to in enumerate("xy"):
            plane[0, to] = push(unit, tok.at[s, t], tps.at[0], tpr.at[0, i], side[to])
        for dz in range(1, q):
            grp = span(lax.rem(z + dz, q), LANES)
            keyz.append(
                [
                    push(w.at[:, grp], wts.at[mine, col], kzs.at[0], kzr.at[dz], (at(dz, 0), t))
                    for i, (w, col) in enumerate(((wk, kcol), (wr, rcol)))
                ]
            )
        got = wts.at[mine, krcol]
        for i, to in enumerate("xy"):
            keyp[0, to] = push(got, got, kps.at[0], kpr.at[0, i], side[to])
        for k in range(1, n):
            j = lax.rem(s + k, n)
            weights.append(
                push(wv.at[:, span(j, LANES)], wts.at[mine, pl.ds(0, LANES)], vs.at[0], vr.at[0], (j, t))
            )
            weights.append(
                push(ws.at[span(j, slot)], wst.at[pl.ds(0, slot), mine], ss.at[0], sr.at[0], (j, t))
            )
        locals_ = [
            local(nrm.at[pl.ds(0, half)], tok.at[s, 0], 0),
            local(nrm.at[pl.ds(half, half)], tok.at[s, 1], 1),
            local(ws.at[span(s, slot)], wst.at[pl.ds(0, slot), mine], 6),
            local(wo, wout_of(z), 7),
        ]

    gates = []

    def send_gates():
        for k in range(1, n):
            j = lax.rem(s + k, n)
            gates.append(push(wg.at[:, span(j, LANES)], wgt.at[mine], vs.at[1], vr.at[1], (j, t)))

    def swap(e, i):
        src = sources[e] * q + (p, px, py, pd)[i]
        swaps[e, i] = push(tok.at[src, t], tok.at[src, t], tss.at[0], tsr.at[e], sibling)

    def arrive(e):
        with jax.named_scope("arrive"):
            zs = sources[e]
            ref = tok_of(zs)
            remote(ref, ref, tzs.at[zs], tzr.at[zs], sibling).wait_recv()
            to, ok = onward(zs)

            @pl.when(ok)
            def _():
                push(ref, ref, tzs.at[zs], tzr.at[zs], (to * q + p, t))

    def spread_plane(e):
        ref = tok_of(sources[e])
        for i, way in enumerate("xy"):
            plane[e, way] = push(ref, ref, tps.at[0], tpr.at[e, i], side[way])
        swap(e, 0)

    def arrive_last(forwards):
        zs = sources[q - 1]
        ok = onward(zs)[1]

        @pl.when(ok if forwards else jnp.logical_not(ok))
        def _():
            arrive(q - 1)
            spread_plane(q - 1)

    quarter = half // 2

    def relay(e):
        with jax.named_scope("relay"):
            for i, (near_by, other) in enumerate(turns):
                landed(tok.at[0, 0], tpr.at[e, i])
                ref = tok.at[sources[e] * q + (px, py)[i], t, pl.ds(i * quarter, quarter)]
                plane[e, other + "d"] = push(ref, ref, tps.at[0], tpr.at[e, 2], side[other])
                swap(e, 1 + i)

    def key_arrive(dz):
        with jax.named_scope("key_arrive"):
            landed(wgt.at[pl.ds(0, 2 * depth)], kzr.at[dz])
            ref = wts.at[span(at(q - dz, 0), depth), krcol]
            for i, to in enumerate("xy"):
                keyp[dz, to] = push(ref, ref, kps.at[0], kpr.at[dz, i], side[to])

    def key_relay(dz):
        with jax.named_scope("key_relay"):
            for i, (near_by, other) in enumerate(turns):
                keyp[dz, near_by].wait_recv()
                ref = wts.at[span(chip(dz, (px, py)[i]), depth), (kcol, rcol)[i]]
                keyp[dz, other + "d"] = push(ref, ref, kps.at[0], kdr.at[0], side[other])

    ri = lax.broadcasted_iota(jnp.int32, (BLOCK, BLOCK), 0)
    ci = lax.broadcasted_iota(jnp.int32, (BLOCK, BLOCK), 1)
    low = ri >= ci
    diag = ri == ci
    left = ci < HEAD_DIM
    until = jnp.where(ri <= ci, 1.0, 0.0).astype(BF16)
    since = jnp.where(low, 1.0, 0.0).astype(BF16)
    sums_of = jnp.concatenate([until, since], axis=1)
    pick = jnp.where(ri[0:8] == ci[0:8], 1.0, 0.0).astype(BF16)

    def project(zs):
        r0 = pl.multiple_of(zs * q * BLOCK, q * BLOCK)
        whole_plane = pl.ds(r0, q * BLOCK)
        x = tok[pl.ds(zs * q, q)].reshape(q * BLOCK, tok.shape[3])
        got = jnp.dot(x, wts[...], preferred_element_type=F32).astype(BF16)
        raw[pl.ds(r0 + 8, q * BLOCK), :] = got[:, 0 : 3 * LANES].astype(F32)
        u = lax.dot_general(pick, got[:, 3 * LANES :], across_lanes, preferred_element_type=F32) + offsets
        steps = jnp.maximum(u, 0.0) + jnp.log1p(jnp.exp(-jnp.abs(u)))
        pre[:, whole_plane] = steps
        decay = -rates * steps
        parts = []
        for b in range(q):
            rest = decay[:, b * BLOCK : (b + 1) * BLOCK]
            for _ in range(3):
                piece = rest.astype(BF16).astype(F32)
                parts.append(piece)
                rest = rest - piece
        summed = jnp.dot(jnp.concatenate(parts, axis=0).astype(BF16), sums_of, preferred_element_type=F32)
        for b in range(q):
            at_b = pl.ds(pl.multiple_of((zs * q + b) * BLOCK, BLOCK), BLOCK)
            got = [summed[24 * b + 8 * k : 24 * b + 8 * k + 8] for k in range(3)]
            both_sums = got[0] + (got[1] + got[2])
            c = jnp.where(first_two, both_sums[:, 0:BLOCK], both_sums[:, BLOCK:])
            c_end = jnp.where(first_two, c[:, BLOCK - 1 : BLOCK], c[:, 0:1])
            sums[:, at_b] = c
            weighting = jnp.exp(c_end - c) * steps[:, b * BLOCK : (b + 1) * BLOCK]
            stacked = jnp.concatenate([c, weighting, jnp.exp(c), jnp.zeros((LANES - 24, BLOCK), F32)], axis=0)
            cums[at_b, :] = stacked.T

    def open_gate(zs):
        with jax.named_scope("gate"):
            x = tok[pl.ds(zs * q, q)].reshape(q * BLOCK, tok.shape[3])
            here = pl.ds(pl.multiple_of(zs * q * BLOCK, q * BLOCK), q * BLOCK)
            gate[here, :] = jnp.dot(x, wgt[...], preferred_element_type=F32).astype(BF16)

    def convolve(i):
        r0 = pl.multiple_of(i * BLOCK, BLOCK)
        for b, dst in enumerate((vals, keys, reads)):
            window = raw[pl.ds(r0, BLOCK + 16), b * LANES : (b + 1) * LANES]
            total = jnp.zeros((BLOCK, LANES), F32)
            for k in range(KERNEL):
                lo = 8 - (KERNEL - 1) // 2 + k
                total = total + window[lo : lo + BLOCK] * taps[k : k + 1, b * LANES : (b + 1) * LANES]
            dst[pl.ds(r0, BLOCK), :] = silu(total).astype(BF16)

    def within(i):
        r0 = pl.multiple_of(i * BLOCK, BLOCK)
        here = pl.ds(r0, BLOCK)
        c, ct, stt = cums[here, :], sums[:, here], pre[:, here]
        key, read, val = keys[here, :], reads[here, :], vals[here, :]
        val32 = val.astype(F32)
        score = lax.dot_general(read, key, across_lanes, preferred_element_type=F32)
        total = jnp.zeros((BLOCK, LANES), F32)
        for h in range(2):
            gap = jnp.where(low, c[:, h : h + 1] - ct[h : h + 1, :], c[:, h + 2 : h + 3] - ct[h + 2 : h + 3, :])
            sb = stt[h + 2 : h + 3, :]
            e = jnp.exp(gap) * jnp.where(low, stt[h : h + 1, :], sb) + jnp.where(diag, sb, 0.0)
            mask = left if h == 0 else jnp.logical_not(left)
            own_val = jnp.where(mask, val32, 0.0).astype(BF16)
            total = total + jnp.dot((score * e).astype(BF16), own_val, preferred_element_type=F32)
        yy[here, :] = total
        key_t = key.astype(F32).T.astype(BF16)
        for d, dst in ((0, injf), (1, injb)):
            w = jnp.where(left, c[:, 8 + 2 * d : 9 + 2 * d], c[:, 9 + 2 * d : 10 + 2 * d])
            scaled = (val32 * w).astype(BF16)
            dst[i] = jnp.dot(key_t, scaled, preferred_element_type=F32)

    def meet(e):
        with jax.named_scope("meet"):
            landed(tok.at[0, 0], tpr.at[e, 2])
            swap(e, 3)

    def use(e):
        zs = sources[e]
        with jax.named_scope("usewait"):
            landed(tok.at[pl.ds(0, q if e else q - 1), 0], tsr.at[e])
        with jax.named_scope("project"):
            project(zs)
        edge = jnp.where(zs == 0, 0, blocks - 1)
        if e == 0:
            start, count = zs * q + 1, q - 2
        else:
            start, count = zs * q + jnp.where(zs > z, -1, 1), q
        if e == q - 1:
            count = count + 1

        def which(i):
            return start + i if e < q - 1 else jnp.where(i < q, start + i, edge)

        if e == q - 1:
            open_gate(zs)
        with jax.named_scope("conv"):

            @pl.loop(0, count, unroll=count)
            def _(i):
                convolve(which(i))

        with jax.named_scope("intra"):

            @pl.loop(0, count, unroll=count)
            def _(i):
                within(which(i))

        if e < q - 1:

            @pl.when((zs == 0) | (zs == q - 1))
            def _():
                convolve(edge)
                within(edge)

    def wout_onward(e):
        zs = sources[e]
        to, ok = onward(zs)

        @pl.when(ok)
        def _():
            ref = wout_of(zs)
            remote(ref, ref, os.at[zs], orr.at[zs], sibling).wait_recv()
            push(ref, ref, os.at[zs], orr.at[zs], (to * q + p, t))

    def wout_arrive(e):
        zs = sources[e]
        to, ok = onward(zs)

        @pl.when(jnp.logical_not(ok))
        def _():
            ref = wout_of(zs)
            remote(ref, ref, os.at[zs], orr.at[zs], sibling).wait_recv()

    arrive(1)
    relay(0)
    for dz in range(1, q):
        key_arrive(dz)
    key_relay(0)
    spread_plane(1)
    for dz in range(1, q):
        key_relay(dz)
    arrive(2)
    spread_plane(2)
    relay(1)
    send_gates()
    meet(0)
    arrive_last(True)
    chain(wo, wout_of(z), os, orr)
    with jax.named_scope("weights"):
        for copy in locals_:
            copy.wait()
        landed(wgt.at[pl.ds(0, (n - 1) * depth)], vr.at[0])
        landed(ws.at[pl.ds(0, (n - 1) * slot)], sr.at[0])
        landed(wgt.at[pl.ds(0, 2 * q * depth)], kdr.at[0])
    with jax.named_scope("turn"):
        for k in range(wst.shape[1] // LANES):
            chunk = slice(k * LANES, (k + 1) * LANES)
            wts[chunk, 3 * LANES :] = wst[:, chunk].astype(F32).T.astype(BF16)
    use(0)
    meet(1)
    relay(2)
    arrive_last(False)
    use(1)
    meet(2)
    relay(3)
    use(2)
    meet(3)
    with jax.named_scope("wout1"):
        wout_onward(1)
        wout_onward(2)
    with jax.named_scope("gates"):
        landed(wgt.at[pl.ds(0, (n - 1) * depth)], vr.at[1])
    for e in range(q - 1):
        open_gate(sources[e])
    use(3)

    def climb(i, states):
        after = []
        for d, inj in ((0, injf), (1, injb)):
            j = i if d == 0 else blocks - 1 - i
            edge_row = cums[pl.ds(pl.multiple_of(j * BLOCK + (1 - d) * (BLOCK - 8), 8), 8), :]
            edge_row = edge_row[7:8] if d == 0 else edge_row[0:1]
            end = jnp.where(left[0:1], edge_row[:, 16 + 2 * d : 17 + 2 * d], edge_row[:, 17 + 2 * d : 18 + 2 * d])
            high = states[d].astype(BF16)
            entered[j, :, 2 * d * LANES : (2 * d + 1) * LANES] = high
            entered[j, :, (2 * d + 1) * LANES : (2 * d + 2) * LANES] = (states[d] - high.astype(F32)).astype(BF16)
            after.append(states[d] * end + inj[j])
        return tuple(after)

    with jax.named_scope("carry"):
        zero = jnp.zeros((STATE, LANES), F32)
        lax.fori_loop(0, blocks, climb, (zero, zero), unroll=4)

    gain = gains[pl.ds(s, 1), :]

    def finish(i):
        r0 = pl.multiple_of(i * BLOCK, BLOCK)
        here = pl.ds(r0, BLOCK)
        got = jnp.dot(reads[here, :], entered[i], preferred_element_type=F32)
        y = yy[here, :]
        for d in range(2):
            grown = jnp.where(left, cums[here, 16 + 2 * d : 17 + 2 * d], cums[here, 17 + 2 * d : 18 + 2 * d])
            y = y + (
                got[:, 2 * d * LANES : (2 * d + 1) * LANES] + got[:, (2 * d + 1) * LANES : (2 * d + 2) * LANES]
            ) * grown
        g = y * silu(gate[here, :].astype(F32))
        sq = g * g
        m0 = jnp.sum(jnp.where(left, sq, 0.0), -1, keepdims=True) / HEAD_DIM
        m1 = jnp.sum(jnp.where(left, 0.0, sq), -1, keepdims=True) / HEAD_DIM
        scale = jnp.where(left, lax.rsqrt(m0 + EPSILON), lax.rsqrt(m1 + EPSILON))
        nh[here, :] = (g * scale * gain).astype(BF16)

    def finish_plane(zs):
        with jax.named_scope("finish"):

            @pl.loop(0, q, unroll=4)
            def _(i):
                finish(zs * q + i)

    near = {}

    def spread_near(e):
        ref = full.at[:, span(sources[e] * q + p, LANES)] if e else nh.at[span(z, q * BLOCK)]
        dst = full.at[:, span(sources[e] * q + p, LANES)]
        for i, to in enumerate("xy"):
            near[e, to] = push(ref, dst, bs.at[0], br.at[e, i], side[to])

    def near_relay(e):
        with jax.named_scope("nearwait"):
            for i, (near_by, other) in enumerate(turns):
                near[e, near_by].wait_recv()
                got = full.at[pl.ds(i * rest_rows, rest_rows), span(sources[e] * q + (px, py)[i], LANES)]
                push(got, got, bs.at[0], bdr.at[0], side[other])

    rest_rows = q * BLOCK // 2
    for e in range(1, q):
        zs = sources[e]
        finish_plane(zs)
        push(nh.at[span(zs, q * BLOCK)], full.at[:, mine], as_.at[0], ar.at[z], (zs * q + p, t))
    finish_plane(z)
    keep = local(nh.at[span(z, q * BLOCK)], full.at[:, mine], 8)
    spread_near(0)
    for e in range(1, q):
        with jax.named_scope("awaywait"):
            landed(nh.at[pl.ds(0, q * BLOCK)], ar.at[sources[e]])
        spread_near(e)
        near_relay(e - 1)
        if e == 2:
            with jax.named_scope("wout2"):
                wout_onward(3)
    near_relay(q - 1)
    with jax.named_scope("outswait"):
        for e in range(1, q):
            wout_arrive(e)
    with jax.named_scope("fullwait"):
        keep.wait()
        landed(full.at[pl.ds(0, BLOCK)], bdr.at[0])
    legs = []
    part_rows = BLOCK // 2
    kept, given = span(t, part_rows), span(1 - t, part_rows)

    def toward(dp):
        return lax.rem(p + dp, q)

    def multiply(dp):
        to = toward(dp)
        part[to] = jnp.dot(full[span(to, BLOCK), :], wout[...], preferred_element_type=F32).astype(BF16)

    def give(dp):
        to = toward(dp)
        push(part.at[to, given], other.at[to], xs.at[0], xr.at[dp - 1], sibling)

    def add_up(dp):
        to = toward(dp)
        landed(other.at[to], xr.at[dp - 1])
        total = (part[to, kept, :].astype(F32) + other[to].astype(F32)).astype(BF16)
        if dp < q:
            summed_up[to] = total
            legs.append(push(summed_up.at[to], both.at[t, p], es.at[0], er.at[dp], (at(0, dp), t)))
        else:
            both[t, p] = total
            push(both.at[t, p], both.at[t, p], fs.at[0], fr.at[0], sibling)

    with jax.named_scope("outdot"):
        multiply(1)
        for dp in range(2, q + 1):
            multiply(dp)
            give(dp - 1)
        give(q)
        for dp in range(1, q + 1):
            add_up(dp)
    with jax.named_scope("legswait"):
        for dp in range(1, q):
            legs[dp - 1].wait_recv()
            got = both.at[t, lax.rem(p + q - dp, q)]
            push(got, got, fs.at[0], fr.at[0], sibling)
    with jax.named_scope("acrosswait"):
        landed(both.at[0], fr.at[0])
    with jax.named_scope("sum"):
        for h in range(2):
            for a in range(q):
                for b in range(q):
                    out[h * part_rows : (h + 1) * part_rows, (a * q + b) * LANES : (a * q + b + 1) * LANES] = both[
                        h, b, :, a * LANES : (a + 1) * LANES
                    ]
    with jax.named_scope("sends"):
        settle_chain(unit, tzs, tzr, tok_of)
        settle_chain(wo, os, orr, wout_of)
        left_here(tok.at[pl.ds(0, 3 * q), 0], tps.at[0])
        left_here(tok.at[pl.ds(0, n - 1), 0], tss.at[0])
        left_here(wgt.at[pl.ds(0, 2 * (q - 1) * depth)], kzs.at[0])
        left_here(wts.at[pl.ds(0, 6 * depth)], kps.at[0])
        left_here(wgt.at[pl.ds(0, (n - 1) * depth)], vs.at[0])
        left_here(wgt.at[pl.ds(0, (n - 1) * depth)], vs.at[1])
        left_here(ws.at[pl.ds(0, (n - 1) * slot)], ss.at[0])
        left_here(nh.at[pl.ds(0, (q - 1) * q * BLOCK)], as_.at[0])
        left_here(full.at[pl.ds(0, 3 * BLOCK)], bs.at[0])
        left_here(other, xs.at[0])
        left_here(summed_up.at[pl.ds(0, q - 1)], es.at[0])
        left_here(both.at[0], fs.at[0])


def whole(n, q, *args):
    dma = pltpu.SemaphoreType.DMA
    vm = pltpu.VMEM
    tokens, wo, wsf = args[0], args[8], args[6]
    depth, width = tokens.shape
    seq = n * depth
    slot = 16
    return pl.pallas_call(
        functools.partial(whole_kernel, n, q),
        out_shape=jax.ShapeDtypeStruct((BLOCK, n * LANES), BF16),
        in_specs=[HBM_SPEC] * len(args),
        out_specs=VMEM_SPEC,
        scratch_shapes=[
            *[vm(args[i].shape, args[i].dtype) for i in (0, 1, 6, 7, 9, 10, 11, 12, 13, 14)],
            vm((depth, width), BF16),
            vm((n * slot, depth), BF16),
            vm((8, 3 * LANES), F32),
            vm((n, LANES), F32),
            vm((n, 2, depth // 2, width), BF16),
            vm((width, 4 * LANES), BF16),
            vm((width, LANES), BF16),
            vm((LANES, width), BF16),
            vm((wo.shape[0], q * LANES), BF16),
            vm((seq + 16, 3 * LANES), F32),
            vm((seq, LANES), BF16),
            vm((8, seq), F32),
            vm((8, seq), F32),
            vm((seq, LANES), BF16),
            vm((seq, LANES), BF16),
            vm((seq, LANES), BF16),
            vm((seq, LANES), F32),
            vm((seq, LANES), F32),
            vm((seq // BLOCK, STATE, LANES), F32),
            vm((seq // BLOCK, STATE, LANES), F32),
            vm((seq // BLOCK, STATE, 4 * LANES), BF16),
            vm((seq, LANES), BF16),
            vm((q * BLOCK, n * LANES), BF16),
            vm((q, BLOCK, q * LANES), BF16),
            vm((q, BLOCK // 2, q * LANES), BF16),
            vm((q, BLOCK // 2, q * LANES), BF16),
            vm((2, q, BLOCK // 2, q * LANES), BF16),
            dma((q + 1,)), dma((q,)), dma((1,)), dma((q, 3)), dma((1,)), dma((q,)),
            dma((1,)), dma((q,)), dma((1,)), dma((q, 2)), dma((1,)),
            dma((2,)), dma((2,)), dma((1,)), dma((1,)), dma((q + 1,)), dma((q,)),
            dma((1,)), dma((q,)), dma((1,)), dma((q, 2)), dma((1,)), dma((1,)), dma((q,)), dma((1,)), dma((q,)),
            dma((1,)), dma((1,)), dma((10,)), dma((10,)),
        ],
        compiler_params=pltpu.CompilerParams(
            collective_id=0, has_side_effects=True, vmem_limit_bytes=VMEM_LIMIT << 10
        ),
        name="whole",
    )(*args)


VMEM_LIMIT = 57344
HBM_SPEC = pl.BlockSpec(memory_space=pltpu.HBM)


def headwise(
    n,
    q,
    tokens,
    in_gain,
    w_value,
    w_gate,
    w_in_key,
    w_read,
    w_step_fwd,
    w_step_bwd,
    conv_value,
    conv_key,
    conv_read,
    step_bias,
    rate,
    norm_gain,
    w_out,
):
    return whole(
        n, q, tokens, in_gain, w_value, w_gate, w_in_key, w_read, w_step_fwd.T, w_step_bwd.T, w_out,
        conv_value, conv_key, conv_read, step_bias, rate, norm_gain,
    )


def whole_heads(mesh):
    n, q = mesh.shape["sp"], math.isqrt(mesh.shape["sp"])

    def run(*args):
        cols, keys = args[2].shape[1], args[4].shape[1]
        ready = (
            q * q == n
            and mesh.shape["tp"] == 2
            and cols == n * LANES
            and args[14].shape[1] == LANES
            and keys == q * LANES
            and q == 4
            and args[0].shape[1] == n * LANES
            and args[0].shape[0] == BLOCK
        )
        return headwise(n, q, *args) if ready else body(*args)

    return run


def solution(mesh):
    in_specs = (
        P("sp", None),
        P(),
        P("sp", "tp"),
        P("sp", "tp"),
        P("sp", "tp"),
        P("sp", "tp"),
        P("sp", "tp"),
        P("sp", "tp"),
        P(None, "tp"),
        P(None, "tp"),
        P(None, "tp"),
        P(None, "tp"),
        P(None, "tp"),
        P("tp"),
        P("tp", "sp"),
    )
    out_specs = P("sp", None)
    return jax.shard_map(whole_heads(mesh), mesh=mesh, in_specs=in_specs, out_specs=out_specs, check_vma=False)
```

```python
import functools
import math

import jax
import jax.numpy as jnp
from jax import lax
from jax.experimental import pallas as pl
from jax.experimental.pallas import tpu as pltpu
from jax.sharding import PartitionSpec as P

HEAD_DIM = 64
STATE = 128
KERNEL = 5
BLOCK = 128


EPSILON = 1e-05
FULL_PRECISION = lax.Precision.HIGHEST


def entering_2(x, axis, combine, identity, reverse):
    length, place = (lax.axis_size(axis), lax.axis_index(axis))
    everything = jax.tree.map(lambda part: lax.all_gather(part, axis), x)
    start = jax.tree.map(
        lambda part, zero: jnp.broadcast_to(jnp.asarray(zero, part.dtype), part.shape), x, identity
    )

    def step(k, before):
        at = length - 1 - k if reverse else k
        reached = at > place if reverse else at < place
        new = combine(before, jax.tree.map(lambda part: part[at], everything))
        return jax.tree.map(lambda a, b: jnp.where(reached, a, b), new, before)

    return lax.fori_loop(0, length, step, start)


def with_halo(cells, sides, width):
    for axis, dim in sides:
        count = lax.axis_size(axis)
        ends = count - 1
        head = lax.slice_in_dim(cells, 0, width, axis=dim)
        tail = lax.slice_in_dim(cells, cells.shape[dim] - width, cells.shape[dim], axis=dim)
        cells = jnp.concatenate(
            [
                lax.ppermute(tail, axis, [(i, (i + 1) % count) for i in range(ends)]),
                cells,
                lax.ppermute(head, axis, [((i + 1) % count, i) for i in range(ends)]),
            ],
            axis=dim,
        )
    return cells


def normalize(tensor, gain):
    return tensor * lax.rsqrt(jnp.mean(tensor * tensor, -1, keepdims=True) + EPSILON) * gain


def block_parts(values, step_size, log_decay, in_keys):
    per_group = values.shape[1] // in_keys.shape[1]
    cumulative = jnp.cumsum(log_decay, axis=0)
    log_total = cumulative[-1]
    weighting = jnp.exp(log_total[None, :] - cumulative) * step_size
    key_heads = jnp.repeat(in_keys, per_group, axis=1)
    scaled = (values.astype(jnp.float32) * weighting[:, :, None]).astype(jnp.bfloat16)
    injected = jnp.einsum("jhn,jhp->hpn", key_heads, scaled, preferred_element_type=jnp.float32)
    return (cumulative, jnp.exp(log_total), injected)


def block_step(memory, inputs):
    values, step_size, cumulative, damping, injected, in_keys, read_in = inputs
    per_group = values.shape[1] // in_keys.shape[1]
    scores = jnp.einsum("ign,jgn->ijg", read_in, in_keys, preferred_element_type=jnp.float32)
    scores = jnp.repeat(scores, per_group, axis=2)
    length = values.shape[0]
    below_mask = (jnp.arange(length)[:, None] >= jnp.arange(length)[None, :])[:, :, None]
    gaps = jnp.where(below_mask, cumulative[:, None, :] - cumulative[None, :, :], -jnp.inf)
    weights = (scores * jnp.exp(gaps) * step_size[None, :, :]).astype(jnp.bfloat16)
    within = jnp.einsum("ijh,jhp->ihp", weights, values, preferred_element_type=jnp.float32)
    read_heads = jnp.repeat(read_in.astype(jnp.float32), per_group, axis=1)
    carried = (
        jnp.einsum("ihn,hpn->ihp", read_heads, memory, precision=FULL_PRECISION)
        * jnp.exp(cumulative)[:, :, None]
    )
    memory = damping[:, None, None] * memory + injected
    return (memory, within + carried)


def blocked(tensor):
    blocks = tensor.shape[0] // BLOCK
    return tensor.reshape((blocks, BLOCK) + tensor.shape[1:])


def sweep(block_inputs, memory):
    memory, swept = lax.scan(block_step, memory, block_inputs)
    return (swept.reshape((swept.shape[0] * swept.shape[1],) + swept.shape[2:]), memory)


def settle(damping_blocks, injected_blocks, memory):

    def advance(memory, inputs):
        return (inputs[0][:, None, None] * memory + inputs[1], None)

    memory, unused = lax.scan(advance, memory, (damping_blocks, injected_blocks))
    return memory


def chain(before_pair, after_pair):
    return (
        before_pair[0] * after_pair[0],
        after_pair[0][:, None, None] * before_pair[1] + after_pair[1],
    )


def entering(damping, final_state, backward):
    identity_pair = (jnp.ones_like(damping), jnp.zeros_like(final_state))
    if backward:
        arrived = entering_2((damping, final_state), "sp", chain, identity_pair, True)
    else:
        arrived = entering_2((damping, final_state), "sp", chain, identity_pair, False)
    return arrived[1]


def body(
    tokens,
    in_gain,
    w_value,
    w_gate,
    w_in_key,
    w_read,
    w_step_fwd,
    w_step_bwd,
    conv_value,
    conv_key,
    conv_read,
    step_bias,
    rate,
    norm_gain,
    w_out,
):
    normed = normalize(tokens.astype(jnp.float32), in_gain.astype(jnp.float32)).astype(jnp.bfloat16)
    weights = (
        lax.all_gather(w_value, "sp", axis=0, tiled=True),
        lax.all_gather(w_gate, "sp", axis=0, tiled=True),
        lax.all_gather(w_in_key, "sp", axis=0, tiled=True),
        lax.all_gather(w_read, "sp", axis=0, tiled=True),
        lax.all_gather(w_step_fwd, "sp", axis=0, tiled=True),
        lax.all_gather(w_step_bwd, "sp", axis=0, tiled=True),
    )
    projected = [
        jnp.dot(normed, weight, preferred_element_type=jnp.float32).astype(jnp.bfloat16)
        for weight in weights
    ]
    value_raw, gate_raw, key_raw, read_raw, pre_fwd, pre_bwd = projected
    value_cols = value_raw.shape[1]
    key_cols = key_raw.shape[1]
    joined = jnp.concatenate([value_raw, key_raw, read_raw], axis=1)
    padded = with_halo(joined, (("sp", 0),), (KERNEL - 1) // 2)
    kernel_taps = jnp.concatenate([conv_value, conv_key, conv_read], axis=1).astype(jnp.float32)
    length = joined.shape[0]
    summed = jnp.zeros(joined.shape, jnp.float32)
    for offset in range(KERNEL):
        summed = summed + padded[offset : offset + length].astype(jnp.float32) * kernel_taps[offset]
    mixed_in = jax.nn.silu(summed).astype(jnp.bfloat16)
    head_count = value_cols // HEAD_DIM
    group_count = key_cols // STATE
    values = mixed_in[:, :value_cols].reshape(length, head_count, HEAD_DIM)
    in_keys = mixed_in[:, value_cols : value_cols + key_cols].reshape(length, group_count, STATE)
    read_in = mixed_in[:, value_cols + key_cols :].reshape(length, group_count, STATE)
    blank = jnp.zeros((head_count, HEAD_DIM, STATE), jnp.float32)
    summed_heads = jnp.zeros(values.shape, jnp.float32)
    for direction, step_pre in ((0, pre_fwd), (1, pre_bwd)):
        step_size = jax.nn.softplus(step_pre.astype(jnp.float32) + step_bias[direction])
        log_decay = -rate[direction] * step_size
        ordered = (values, step_size, log_decay, in_keys, read_in)
        if direction == 1:
            ordered = tuple((tensor[::-1] for tensor in ordered))
        value_blocks, step_blocks, decay_blocks, key_blocks, read_blocks = [
            blocked(tensor) for tensor in ordered
        ]
        cumulative_blocks, damping_blocks, injected_blocks = jax.vmap(block_parts)(
            value_blocks, step_blocks, decay_blocks, key_blocks
        )
        block_inputs = (
            value_blocks,
            step_blocks,
            cumulative_blocks,
            damping_blocks,
            injected_blocks,
            key_blocks,
            read_blocks,
        )
        damping = jnp.exp(jnp.sum(ordered[2], axis=0))
        final_state = settle(damping_blocks, injected_blocks, blank)
        arriving = entering(damping, final_state, direction == 1)
        swept, final_state = sweep(block_inputs, arriving)
        if direction == 1:
            swept = swept[::-1]
        summed_heads = summed_heads + swept
    gated_out = summed_heads * jax.nn.silu(gate_raw.astype(jnp.float32)).reshape(values.shape)
    head_gain = norm_gain.astype(jnp.float32).reshape(head_count, HEAD_DIM)
    normed_heads = normalize(gated_out, head_gain).astype(jnp.bfloat16).reshape(length, value_cols)
    out_whole = lax.all_gather(w_out, "sp", axis=1, tiled=True)
    own_rows = lax.psum_scatter(
        jnp.dot(normed_heads, out_whole, preferred_element_type=jnp.float32).astype(jnp.bfloat16),
        "tp",
        scatter_dimension=0,
        tiled=True,
    )
    return lax.all_gather(own_rows, "tp", axis=0, tiled=True)


F32 = jnp.float32
BF16 = jnp.bfloat16
LANES = 128
VMEM_SPEC = pl.BlockSpec(memory_space=pltpu.VMEM)


def push(src, dst, send, recv, peer):
    copy = pltpu.make_async_remote_copy(
        src_ref=src,
        dst_ref=dst,
        send_sem=send,
        recv_sem=recv,
        device_id=peer,
        device_id_type=pl.DeviceIdType.MESH,
    )
    copy.start()
    return copy


def silu(x):
    return x * jax.nn.sigmoid(x)


def whole_kernel(
    n, q, tin_h, ing_h, wv, wg, wk, wr, wsf_h, wsb_h, wo, cv_h, ck_h, cr_h, bias_h, rate_h, ngain_h, out,
    tin, ing, wsf, wsb, cv, ck, cr, bias, rate, ngain,
    nrm, ws, taps, gains, tok, wts, wgt, wst, wout, raw, gate, pre, sums, vals, keys, reads, cums, yy, injf, injb, entered,
    nh, full, part, other, summed_up, both,
    tzs, tzr, tps, tpr, tss, tsr, kzs, kzr, kps, kpr, kdr, vs, vr, ss, sr, os, orr,
    as_, ar, bs, br, bdr, xs, xr, es, er, fs, fr, ls, ins,
):
    s, t = lax.axis_index("sp"), lax.axis_index("tp")
    z, p = s // q, s % q
    sibling = (s, 1 - t)
    half = tok.shape[2]
    depth = wv.shape[0]
    blocks = tok.shape[0] * 2 * half // BLOCK

    def at(dz, dp):
        return lax.rem(z + dz, q) * q + lax.rem(p + dp, q)

    def span(i, size):
        return pl.ds(pl.multiple_of(i * size, size), size)

    px = p + 1 - 2 * lax.rem(p, 2)
    py = lax.rem(p + 2, q)
    pd = lax.rem(px + 2, q)
    side = {"x": (z * q + px, t), "y": (z * q + py, t)}
    turns = (("x", "y"), ("y", "x"))

    def chip(dz, where):
        return lax.rem(z + q - dz, q) * q + where

    with jax.named_scope("greet"):
        barrier = pltpu.get_barrier_semaphore()
        peers = [(lax.rem(s + k, n), t) for k in range(1, n)] + [sibling]
        for peer in peers:
            pl.semaphore_signal(barrier, inc=1, device_id=peer, device_id_type=pl.DeviceIdType.MESH)

    def local(src, dst, i):
        copy = pltpu.make_async_copy(src, dst, ls.at[i])
        copy.start()
        return copy

    mine = span(s, depth)
    rows = span(t, half)
    kcol, rcol = pl.ds(LANES, LANES), pl.ds(2 * LANES, LANES)
    krcol = pl.ds(LANES, 2 * LANES)

    with jax.named_scope("load"):
        held = (
            (tin_h, tin), (ing_h, ing), (wsf_h, wsf), (wsb_h, wsb), (cv_h, cv), (ck_h, ck), (cr_h, cr),
            (bias_h, bias), (rate_h, rate), (ngain_h, ngain),
        )
        loads = [pltpu.make_async_copy(src, dst, ins.at[i]) for i, (src, dst) in enumerate(held)]
        for copy in loads:
            copy.start()
        locals_ = [
            local(wk.at[:, span(z, LANES)], wts.at[mine, kcol], 2),
            local(wr.at[:, span(z, LANES)], wts.at[mine, rcol], 3),
            local(wv.at[:, mine], wts.at[mine, pl.ds(0, LANES)], 4),
            local(wg.at[:, mine], wgt.at[mine], 5),
        ]
        for copy in loads:
            copy.wait()
    with jax.named_scope("prep"):
        wide_in = tin[...].astype(F32)
        nrm[...] = normalize(wide_in, ing[...].astype(F32).reshape(1, ing.shape[0])).astype(BF16)
        heads = wsf.shape[0]
        slot = ws.shape[0] // n
        row_i = lax.broadcasted_iota(jnp.int32, (n * slot, heads), 0)
        col_i = lax.broadcasted_iota(jnp.int32, (n * slot, heads), 1)
        place = lax.rem(row_i, slot)
        head_of = 2 * (row_i // slot)
        pick_f = jnp.where((place < 2) & (col_i == head_of + place), 1.0, 0.0).astype(BF16)
        pick_b = jnp.where((place >= 2) & (col_i == head_of + place - 2), 1.0, 0.0).astype(BF16)
        ws[...] = (
            jnp.dot(pick_f, wsf[...], preferred_element_type=F32)
            + jnp.dot(pick_b, wsb[...], preferred_element_type=F32)
        ).astype(BF16)
        own = span(s, LANES)
        taps[0:KERNEL, 0:LANES] = cv[:, own].astype(F32)
        taps[0:KERNEL, LANES : 2 * LANES] = ck[:, span(z, LANES)].astype(F32)
        taps[0:KERNEL, 2 * LANES : 3 * LANES] = cr[:, span(z, LANES)].astype(F32)
        gains[...] = ngain[...].astype(F32).reshape(n, LANES)
        lanes_of = lax.broadcasted_iota(jnp.int32, (8, heads), 1)
        rows_of = lax.broadcasted_iota(jnp.int32, (8, heads), 0)
        spread = jnp.where((rows_of < 4) & (lanes_of == 2 * s + lax.rem(rows_of, 2)), 1.0, 0.0).astype(F32)
        first_two = lax.broadcasted_iota(jnp.int32, (8, 1), 0) < 2
        across_lanes = (((1,), (1,)), ((), ()))

        def own_rows(both_dirs):
            got = lax.dot_general(
                spread, both_dirs, across_lanes, precision=FULL_PRECISION, preferred_element_type=F32
            )
            return jnp.where(first_two, got[:, 0:1], got[:, 1:2])

        offsets = own_rows(bias[...])
        rates = own_rows(rate[...])
        wst[slot:, :] = jnp.zeros((LANES - slot, wst.shape[1]), BF16)
        seq = blocks * BLOCK
        wide = 3 * LANES
        raw[0:8, :] = jnp.zeros((8, wide), F32)
        raw[seq + 8 : seq + 16, :] = jnp.zeros((8, wide), F32)
        for copy in locals_:
            copy.wait()
    with jax.named_scope("greeted"):
        pl.semaphore_wait(barrier, len(peers))

    one, last = q - 1, q
    rising, sinking = z < q - 1, z > 0
    unit = nrm.at[rows]

    def arrival(e):
        later = [[1, 2, 3], [0, 2, 3], [3, 1, 0], [2, 1, 0]]
        picked = later[q - 1][e]
        for k in range(q - 1):
            picked = jnp.where(z == k, later[k][e], picked)
        return picked

    sources = [z] + [arrival(e) for e in range(q - 1)]

    def chain(src_ref, dst_ref, sends, recvs):
        @pl.when(rising)
        def _():
            push(src_ref, dst_ref, sends.at[z], recvs.at[z], (s + q, t))

        @pl.when(sinking)
        def _():
            push(src_ref, dst_ref, sends.at[q], recvs.at[z], (s - q, t))

    def remote(src, dst, send, recv, peer):
        return pltpu.make_async_remote_copy(
            src_ref=src, dst_ref=dst, send_sem=send, recv_sem=recv,
            device_id=peer, device_id_type=pl.DeviceIdType.MESH,
        )

    def landed(ref, sem):
        remote(ref, ref, sem, sem, sibling).wait_recv()

    def left_here(ref, sem):
        remote(ref, ref, sem, sem, sibling).wait_send()

    def onward(zs):
        to = z + jnp.where(zs < z, 1, -1)
        return to, (to >= 0) & (to < q)

    def settle_chain(src_ref, sends, recvs, ref_of):
        @pl.when(rising)
        def _():
            remote(src_ref, ref_of(z), sends.at[z], recvs.at[z], (s + q, t)).wait_send()

        @pl.when(sinking)
        def _():
            remote(src_ref, ref_of(z), sends.at[q], recvs.at[z], (s - q, t)).wait_send()

        for zs in sources[1:]:
            to, ok = onward(zs)

            @pl.when(ok)
            def _():
                ref = ref_of(zs)
                remote(ref, ref, sends.at[zs], recvs.at[zs], (to * q + p, t)).wait_send()

    def tok_of(zs):
        return tok.at[zs * q + p, t]

    def wout_of(zs):
        return wout.at[:, span(zs, LANES)]

    plane, keyz, keyp, weights, swaps = {}, [], {}, [], {}
    with jax.named_scope("issue"):
        chain(unit, tok_of(z), tzs, tzr)
        for i, to in enumerate("xy"):
            plane[0, to] = push(unit, tok.at[s, t], tps.at[0], tpr.at[0, i], side[to])
        for dz in range(1, q):
            grp = span(lax.rem(z + dz, q), LANES)
            keyz.append(
                [
                    push(w.at[:, grp], wts.at[mine, col], kzs.at[0], kzr.at[dz], (at(dz, 0), t))
                    for i, (w, col) in enumerate(((wk, kcol), (wr, rcol)))
                ]
            )
        got = wts.at[mine, krcol]
        for i, to in enumerate("xy"):
            keyp[0, to] = push(got, got, kps.at[0], kpr.at[0, i], side[to])
        for k in range(1, n):
            j = lax.rem(s + k, n)
            weights.append(
                push(wv.at[:, span(j, LANES)], wts.at[mine, pl.ds(0, LANES)], vs.at[0], vr.at[0], (j, t))
            )
            weights.append(
                push(ws.at[span(j, slot)], wst.at[pl.ds(0, slot), mine], ss.at[0], sr.at[0], (j, t))
            )
        locals_ = [
            local(nrm.at[pl.ds(0, half)], tok.at[s, 0], 0),
            local(nrm.at[pl.ds(half, half)], tok.at[s, 1], 1),
            local(ws.at[span(s, slot)], wst.at[pl.ds(0, slot), mine], 6),
            local(wo, wout_of(z), 7),
        ]

    gates = []

    def send_gates():
        for k in range(1, n):
            j = lax.rem(s + k, n)
            gates.append(push(wg.at[:, span(j, LANES)], wgt.at[mine], vs.at[1], vr.at[1], (j, t)))

    def swap(e, i):
        src = sources[e] * q + (p, px, py, pd)[i]
        swaps[e, i] = push(tok.at[src, t], tok.at[src, t], tss.at[0], tsr.at[e], sibling)

    def arrive(e):
        with jax.named_scope("arrive"):
            zs = sources[e]
            ref = tok_of(zs)
            remote(ref, ref, tzs.at[zs], tzr.at[zs], sibling).wait_recv()
            to, ok = onward(zs)

            @pl.when(ok)
            def _():
                push(ref, ref, tzs.at[zs], tzr.at[zs], (to * q + p, t))

    def spread_plane(e):
        ref = tok_of(sources[e])
        for i, way in enumerate("xy"):
            plane[e, way] = push(ref, ref, tps.at[0], tpr.at[e, i], side[way])
        swap(e, 0)

    def arrive_last(forwards):
        zs = sources[q - 1]
        ok = onward(zs)[1]

        @pl.when(ok if forwards else jnp.logical_not(ok))
        def _():
            arrive(q - 1)
            spread_plane(q - 1)

    quarter = half // 2

    def relay(e):
        with jax.named_scope("relay"):
            for i, (near_by, other) in enumerate(turns):
                landed(tok.at[0, 0], tpr.at[e, i])
                ref = tok.at[sources[e] * q + (px, py)[i], t, pl.ds(i * quarter, quarter)]
                plane[e, other + "d"] = push(ref, ref, tps.at[0], tpr.at[e, 2], side[other])
                swap(e, 1 + i)

    def key_arrive(dz):
        with jax.named_scope("key_arrive"):
            landed(wgt.at[pl.ds(0, 2 * depth)], kzr.at[dz])
            ref = wts.at[span(at(q - dz, 0), depth), krcol]
            for i, to in enumerate("xy"):
                keyp[dz, to] = push(ref, ref, kps.at[0], kpr.at[dz, i], side[to])

    def key_relay(dz):
        with jax.named_scope("key_relay"):
            for i, (near_by, other) in enumerate(turns):
                keyp[dz, near_by].wait_recv()
                ref = wts.at[span(chip(dz, (px, py)[i]), depth), (kcol, rcol)[i]]
                keyp[dz, other + "d"] = push(ref, ref, kps.at[0], kdr.at[0], side[other])

    ri = lax.broadcasted_iota(jnp.int32, (BLOCK, BLOCK), 0)
    ci = lax.broadcasted_iota(jnp.int32, (BLOCK, BLOCK), 1)
    low = ri >= ci
    diag = ri == ci
    left = ci < HEAD_DIM
    until = jnp.where(ri <= ci, 1.0, 0.0).astype(BF16)
    since = jnp.where(low, 1.0, 0.0).astype(BF16)
    sums_of = jnp.concatenate([until, since], axis=1)
    pick = jnp.where(ri[0:8] == ci[0:8], 1.0, 0.0).astype(BF16)

    def project(zs):
        r0 = pl.multiple_of(zs * q * BLOCK, q * BLOCK)
        whole_plane = pl.ds(r0, q * BLOCK)
        x = tok[pl.ds(zs * q, q)].reshape(q * BLOCK, tok.shape[3])
        got = jnp.dot(x, wts[...], preferred_element_type=F32).astype(BF16)
        raw[pl.ds(r0 + 8, q * BLOCK), :] = got[:, 0 : 3 * LANES].astype(F32)
        u = lax.dot_general(pick, got[:, 3 * LANES :], across_lanes, preferred_element_type=F32) + offsets
        steps = jnp.maximum(u, 0.0) + jnp.log1p(jnp.exp(-jnp.abs(u)))
        pre[:, whole_plane] = steps
        decay = -rates * steps
        parts = []
        for b in range(q):
            rest = decay[:, b * BLOCK : (b + 1) * BLOCK]
            for _ in range(3):
                piece = rest.astype(BF16).astype(F32)
                parts.append(piece)
                rest = rest - piece
        summed = jnp.dot(jnp.concatenate(parts, axis=0).astype(BF16), sums_of, preferred_element_type=F32)
        for b in range(q):
            at_b = pl.ds(pl.multiple_of((zs * q + b) * BLOCK, BLOCK), BLOCK)
            got = [summed[24 * b + 8 * k : 24 * b + 8 * k + 8] for k in range(3)]
            both_sums = got[0] + (got[1] + got[2])
            c = jnp.where(first_two, both_sums[:, 0:BLOCK], both_sums[:, BLOCK:])
            c_end = jnp.where(first_two, c[:, BLOCK - 1 : BLOCK], c[:, 0:1])
            sums[:, at_b] = c
            weighting = jnp.exp(c_end - c) * steps[:, b * BLOCK : (b + 1) * BLOCK]
            stacked = jnp.concatenate([c, weighting, jnp.exp(c), jnp.zeros((LANES - 24, BLOCK), F32)], axis=0)
            cums[at_b, :] = stacked.T

    def open_gate(zs):
        with jax.named_scope("gate"):
            x = tok[pl.ds(zs * q, q)].reshape(q * BLOCK, tok.shape[3])
            here = pl.ds(pl.multiple_of(zs * q * BLOCK, q * BLOCK), q * BLOCK)
            gate[here, :] = jnp.dot(x, wgt[...], preferred_element_type=F32).astype(BF16)

    def open_block(i):
        here = pl.ds(pl.multiple_of(i * BLOCK, BLOCK), BLOCK)
        x = tok[i].reshape(BLOCK, tok.shape[3])
        gate[here, :] = jnp.dot(x, wgt[...], preferred_element_type=F32).astype(BF16)

    def convolve(i):
        r0 = pl.multiple_of(i * BLOCK, BLOCK)
        for b, dst in enumerate((vals, keys, reads)):
            window = raw[pl.ds(r0, BLOCK + 16), b * LANES : (b + 1) * LANES]
            total = jnp.zeros((BLOCK, LANES), F32)
            for k in range(KERNEL):
                lo = 8 - (KERNEL - 1) // 2 + k
                total = total + window[lo : lo + BLOCK] * taps[k : k + 1, b * LANES : (b + 1) * LANES]
            dst[pl.ds(r0, BLOCK), :] = silu(total).astype(BF16)

    def within(i):
        r0 = pl.multiple_of(i * BLOCK, BLOCK)
        here = pl.ds(r0, BLOCK)
        c, ct, stt = cums[here, :], sums[:, here], pre[:, here]
        key, read, val = keys[here, :], reads[here, :], vals[here, :]
        val32 = val.astype(F32)
        score = lax.dot_general(read, key, across_lanes, preferred_element_type=F32)
        total = jnp.zeros((BLOCK, LANES), F32)
        for h in range(2):
            gap = jnp.where(low, c[:, h : h + 1] - ct[h : h + 1, :], c[:, h + 2 : h + 3] - ct[h + 2 : h + 3, :])
            sb = stt[h + 2 : h + 3, :]
            e = jnp.exp(gap) * jnp.where(low, stt[h : h + 1, :], sb) + jnp.where(diag, sb, 0.0)
            mask = left if h == 0 else jnp.logical_not(left)
            own_val = jnp.where(mask, val32, 0.0).astype(BF16)
            total = total + jnp.dot((score * e).astype(BF16), own_val, preferred_element_type=F32)
        yy[here, :] = total
        key_t = key.astype(F32).T.astype(BF16)
        for d, dst in ((0, injf), (1, injb)):
            w = jnp.where(left, c[:, 8 + 2 * d : 9 + 2 * d], c[:, 9 + 2 * d : 10 + 2 * d])
            scaled = (val32 * w).astype(BF16)
            dst[i] = jnp.dot(key_t, scaled, preferred_element_type=F32)

    def meet(e):
        with jax.named_scope("meet"):
            landed(tok.at[0, 0], tpr.at[e, 2])
            swap(e, 3)

    def use(e):
        zs = sources[e]
        with jax.named_scope("usewait"):
            landed(tok.at[pl.ds(0, q if e else q - 1), 0], tsr.at[e])
        with jax.named_scope("project"):
            project(zs)
        edge = jnp.where(zs == 0, 0, blocks - 1)
        if e == 0:
            start, count = zs * q + 1, q - 2
        else:
            start, count = zs * q + jnp.where(zs > z, -1, 1), q
        if e == q - 1:
            count = count + 1

        def which(i):
            return start + i if e < q - 1 else jnp.where(i < q, start + i, edge)

        with jax.named_scope("conv"):

            @pl.loop(0, count, unroll=count)
            def _(i):
                convolve(which(i))

        with jax.named_scope("intra"):

            @pl.loop(0, count, unroll=count)
            def _(i):
                if e == q - 1:
                    open_block(zs * q + jnp.minimum(i, q - 1))
                within(which(i))

        if e < q - 1:

            @pl.when((zs == 0) | (zs == q - 1))
            def _():
                convolve(edge)
                within(edge)

    def wout_onward(e):
        zs = sources[e]
        to, ok = onward(zs)

        @pl.when(ok)
        def _():
            ref = wout_of(zs)
            remote(ref, ref, os.at[zs], orr.at[zs], sibling).wait_recv()
            push(ref, ref, os.at[zs], orr.at[zs], (to * q + p, t))

    def wout_arrive(e):
        zs = sources[e]
        to, ok = onward(zs)

        @pl.when(jnp.logical_not(ok))
        def _():
            ref = wout_of(zs)
            remote(ref, ref, os.at[zs], orr.at[zs], sibling).wait_recv()

    arrive(1)
    relay(0)
    for dz in range(1, q):
        key_arrive(dz)
    key_relay(0)
    spread_plane(1)
    for dz in range(1, q):
        key_relay(dz)
    arrive(2)
    spread_plane(2)
    relay(1)
    send_gates()
    meet(0)
    arrive_last(True)
    chain(wo, wout_of(z), os, orr)
    with jax.named_scope("weights"):
        for copy in locals_:
            copy.wait()
        landed(wgt.at[pl.ds(0, (n - 1) * depth)], vr.at[0])
        landed(ws.at[pl.ds(0, (n - 1) * slot)], sr.at[0])
        landed(wgt.at[pl.ds(0, 2 * q * depth)], kdr.at[0])
    with jax.named_scope("turn"):
        for k in range(wst.shape[1] // LANES):
            chunk = slice(k * LANES, (k + 1) * LANES)
            wts[chunk, 3 * LANES :] = wst[:, chunk].astype(F32).T.astype(BF16)
    use(0)
    meet(1)
    relay(2)
    arrive_last(False)
    use(1)
    meet(2)
    relay(3)
    with jax.named_scope("wout1"):
        wout_onward(1)
        wout_onward(2)
    use(2)
    meet(3)
    with jax.named_scope("gates"):
        landed(wgt.at[pl.ds(0, (n - 1) * depth)], vr.at[1])
    for e in range(q - 1):
        open_gate(sources[e])
    use(3)

    def climb(i, states):
        after = []
        for d, inj in ((0, injf), (1, injb)):
            j = i if d == 0 else blocks - 1 - i
            edge_row = cums[pl.ds(pl.multiple_of(j * BLOCK + (1 - d) * (BLOCK - 8), 8), 8), :]
            edge_row = edge_row[7:8] if d == 0 else edge_row[0:1]
            end = jnp.where(left[0:1], edge_row[:, 16 + 2 * d : 17 + 2 * d], edge_row[:, 17 + 2 * d : 18 + 2 * d])
            high = states[d].astype(BF16)
            entered[j, :, 2 * d * LANES : (2 * d + 1) * LANES] = high
            entered[j, :, (2 * d + 1) * LANES : (2 * d + 2) * LANES] = (states[d] - high.astype(F32)).astype(BF16)
            after.append(states[d] * end + inj[j])
        return tuple(after)

    with jax.named_scope("carry"):
        zero = jnp.zeros((STATE, LANES), F32)
        lax.fori_loop(0, blocks, climb, (zero, zero), unroll=4)

    gain = gains[pl.ds(s, 1), :]

    def finish(i):
        r0 = pl.multiple_of(i * BLOCK, BLOCK)
        here = pl.ds(r0, BLOCK)
        got = jnp.dot(reads[here, :], entered[i], preferred_element_type=F32)
        y = yy[here, :]
        for d in range(2):
            grown = jnp.where(left, cums[here, 16 + 2 * d : 17 + 2 * d], cums[here, 17 + 2 * d : 18 + 2 * d])
            y = y + (
                got[:, 2 * d * LANES : (2 * d + 1) * LANES] + got[:, (2 * d + 1) * LANES : (2 * d + 2) * LANES]
            ) * grown
        g = y * silu(gate[here, :].astype(F32))
        sq = g * g
        m0 = jnp.sum(jnp.where(left, sq, 0.0), -1, keepdims=True) / HEAD_DIM
        m1 = jnp.sum(jnp.where(left, 0.0, sq), -1, keepdims=True) / HEAD_DIM
        scale = jnp.where(left, lax.rsqrt(m0 + EPSILON), lax.rsqrt(m1 + EPSILON))
        nh[here, :] = (g * scale * gain).astype(BF16)

    def finish_plane(zs):
        with jax.named_scope("finish"):

            @pl.loop(0, q, unroll=4)
            def _(i):
                finish(zs * q + i)

    near = {}

    def spread_near(e):
        ref = full.at[:, span(sources[e] * q + p, LANES)] if e else nh.at[span(z, q * BLOCK)]
        dst = full.at[:, span(sources[e] * q + p, LANES)]
        for i, to in enumerate("xy"):
            near[e, to] = push(ref, dst, bs.at[0], br.at[e, i], side[to])

    def near_relay(e):
        with jax.named_scope("nearwait"):
            for i, (near_by, other) in enumerate(turns):
                near[e, near_by].wait_recv()
                got = full.at[pl.ds(i * rest_rows, rest_rows), span(sources[e] * q + (px, py)[i], LANES)]
                push(got, got, bs.at[0], bdr.at[0], side[other])

    rest_rows = q * BLOCK // 2
    for e in range(1, q):
        zs = sources[e]
        finish_plane(zs)
        push(nh.at[span(zs, q * BLOCK)], full.at[:, mine], as_.at[0], ar.at[z], (zs * q + p, t))
    finish_plane(z)
    keep = local(nh.at[span(z, q * BLOCK)], full.at[:, mine], 8)
    spread_near(0)
    for e in range(1, q):
        with jax.named_scope("awaywait"):
            landed(nh.at[pl.ds(0, q * BLOCK)], ar.at[sources[e]])
        spread_near(e)
        near_relay(e - 1)
        if e == 2:
            with jax.named_scope("wout2"):
                wout_onward(3)
    near_relay(q - 1)
    with jax.named_scope("outswait"):
        for e in range(1, q):
            wout_arrive(e)
    with jax.named_scope("fullwait"):
        keep.wait()
        landed(full.at[pl.ds(0, BLOCK)], bdr.at[0])
    legs = []
    part_rows = BLOCK // 2
    kept, given = span(t, part_rows), span(1 - t, part_rows)

    def toward(dp):
        return lax.rem(p + dp, q)

    def multiply(dp):
        to = toward(dp)
        part[to] = jnp.dot(full[span(to, BLOCK), :], wout[...], preferred_element_type=F32).astype(BF16)

    def give(dp):
        to = toward(dp)
        push(part.at[to, given], other.at[to], xs.at[0], xr.at[dp - 1], sibling)

    def add_up(dp):
        to = toward(dp)
        landed(other.at[to], xr.at[dp - 1])
        total = (part[to, kept, :].astype(F32) + other[to].astype(F32)).astype(BF16)
        if dp < q:
            summed_up[to] = total
            legs.append(push(summed_up.at[to], both.at[t, p], es.at[0], er.at[dp], (at(0, dp), t)))
        else:
            both[t, p] = total
            push(both.at[t, p], both.at[t, p], fs.at[0], fr.at[0], sibling)

    with jax.named_scope("outdot"):
        multiply(1)
        for dp in range(2, q + 1):
            multiply(dp)
            give(dp - 1)
        give(q)
        for dp in range(1, q + 1):
            add_up(dp)
    with jax.named_scope("legswait"):
        for dp in range(1, q):
            legs[dp - 1].wait_recv()
            got = both.at[t, lax.rem(p + q - dp, q)]
            push(got, got, fs.at[0], fr.at[0], sibling)
    with jax.named_scope("acrosswait"):
        landed(both.at[0], fr.at[0])
    with jax.named_scope("sum"):
        for h in range(2):
            for a in range(q):
                for b in range(q):
                    out[h * part_rows : (h + 1) * part_rows, (a * q + b) * LANES : (a * q + b + 1) * LANES] = both[
                        h, b, :, a * LANES : (a + 1) * LANES
                    ]
    with jax.named_scope("sends"):
        settle_chain(unit, tzs, tzr, tok_of)
        settle_chain(wo, os, orr, wout_of)
        left_here(tok.at[pl.ds(0, 3 * q), 0], tps.at[0])
        left_here(tok.at[pl.ds(0, n - 1), 0], tss.at[0])
        left_here(wgt.at[pl.ds(0, 2 * (q - 1) * depth)], kzs.at[0])
        left_here(wts.at[pl.ds(0, 6 * depth)], kps.at[0])
        left_here(wgt.at[pl.ds(0, (n - 1) * depth)], vs.at[0])
        left_here(wgt.at[pl.ds(0, (n - 1) * depth)], vs.at[1])
        left_here(ws.at[pl.ds(0, (n - 1) * slot)], ss.at[0])
        left_here(nh.at[pl.ds(0, (q - 1) * q * BLOCK)], as_.at[0])
        left_here(full.at[pl.ds(0, 3 * BLOCK)], bs.at[0])
        left_here(other, xs.at[0])
        left_here(summed_up.at[pl.ds(0, q - 1)], es.at[0])
        left_here(both.at[0], fs.at[0])


def whole(n, q, *args):
    dma = pltpu.SemaphoreType.DMA
    vm = pltpu.VMEM
    tokens, wo, wsf = args[0], args[8], args[6]
    depth, width = tokens.shape
    seq = n * depth
    slot = 16
    return pl.pallas_call(
        functools.partial(whole_kernel, n, q),
        out_shape=jax.ShapeDtypeStruct((BLOCK, n * LANES), BF16),
        in_specs=[HBM_SPEC] * len(args),
        out_specs=VMEM_SPEC,
        scratch_shapes=[
            *[vm(args[i].shape, args[i].dtype) for i in (0, 1, 6, 7, 9, 10, 11, 12, 13, 14)],
            vm((depth, width), BF16),
            vm((n * slot, depth), BF16),
            vm((8, 3 * LANES), F32),
            vm((n, LANES), F32),
            vm((n, 2, depth // 2, width), BF16),
            vm((width, 4 * LANES), BF16),
            vm((width, LANES), BF16),
            vm((LANES, width), BF16),
            vm((wo.shape[0], q * LANES), BF16),
            vm((seq + 16, 3 * LANES), F32),
            vm((seq, LANES), BF16),
            vm((8, seq), F32),
            vm((8, seq), F32),
            vm((seq, LANES), BF16),
            vm((seq, LANES), BF16),
            vm((seq, LANES), BF16),
            vm((seq, LANES), F32),
            vm((seq, LANES), F32),
            vm((seq // BLOCK, STATE, LANES), F32),
            vm((seq // BLOCK, STATE, LANES), F32),
            vm((seq // BLOCK, STATE, 4 * LANES), BF16),
            vm((seq, LANES), BF16),
            vm((q * BLOCK, n * LANES), BF16),
            vm((q, BLOCK, q * LANES), BF16),
            vm((q, BLOCK // 2, q * LANES), BF16),
            vm((q, BLOCK // 2, q * LANES), BF16),
            vm((2, q, BLOCK // 2, q * LANES), BF16),
            dma((q + 1,)), dma((q,)), dma((1,)), dma((q, 3)), dma((1,)), dma((q,)),
            dma((1,)), dma((q,)), dma((1,)), dma((q, 2)), dma((1,)),
            dma((2,)), dma((2,)), dma((1,)), dma((1,)), dma((q + 1,)), dma((q,)),
            dma((1,)), dma((q,)), dma((1,)), dma((q, 2)), dma((1,)), dma((1,)), dma((q,)), dma((1,)), dma((q,)),
            dma((1,)), dma((1,)), dma((10,)), dma((10,)),
        ],
        compiler_params=pltpu.CompilerParams(
            collective_id=0, has_side_effects=True, vmem_limit_bytes=VMEM_LIMIT << 10
        ),
        name="whole",
    )(*args)


VMEM_LIMIT = 57344
HBM_SPEC = pl.BlockSpec(memory_space=pltpu.HBM)


def headwise(
    n,
    q,
    tokens,
    in_gain,
    w_value,
    w_gate,
    w_in_key,
    w_read,
    w_step_fwd,
    w_step_bwd,
    conv_value,
    conv_key,
    conv_read,
    step_bias,
    rate,
    norm_gain,
    w_out,
):
    return whole(
        n, q, tokens, in_gain, w_value, w_gate, w_in_key, w_read, w_step_fwd.T, w_step_bwd.T, w_out,
        conv_value, conv_key, conv_read, step_bias, rate, norm_gain,
    )


def whole_heads(mesh):
    n, q = mesh.shape["sp"], math.isqrt(mesh.shape["sp"])

    def run(*args):
        cols, keys = args[2].shape[1], args[4].shape[1]
        ready = (
            q * q == n
            and mesh.shape["tp"] == 2
            and cols == n * LANES
            and args[14].shape[1] == LANES
            and keys == q * LANES
            and q == 4
            and args[0].shape[1] == n * LANES
            and args[0].shape[0] == BLOCK
        )
        return headwise(n, q, *args) if ready else body(*args)

    return run


def solution(mesh):
    in_specs = (
        P("sp", None),
        P(),
        P("sp", "tp"),
        P("sp", "tp"),
        P("sp", "tp"),
        P("sp", "tp"),
        P("sp", "tp"),
        P("sp", "tp"),
        P(None, "tp"),
        P(None, "tp"),
        P(None, "tp"),
        P(None, "tp"),
        P(None, "tp"),
        P("tp"),
        P("tp", "sp"),
    )
    out_specs = P("sp", None)
    return jax.shard_map(whole_heads(mesh), mesh=mesh, in_specs=in_specs, out_specs=out_specs, check_vma=False)
```

```python
import functools
import math

import jax
import jax.numpy as jnp
from jax import lax
from jax.experimental import pallas as pl
from jax.experimental.pallas import tpu as pltpu
from jax.sharding import PartitionSpec as P

HEAD_DIM = 64
STATE = 128
KERNEL = 5
BLOCK = 128


EPSILON = 1e-05
FULL_PRECISION = lax.Precision.HIGHEST


def entering_2(x, axis, combine, identity, reverse):
    length, place = (lax.axis_size(axis), lax.axis_index(axis))
    everything = jax.tree.map(lambda part: lax.all_gather(part, axis), x)
    start = jax.tree.map(
        lambda part, zero: jnp.broadcast_to(jnp.asarray(zero, part.dtype), part.shape), x, identity
    )

    def step(k, before):
        at = length - 1 - k if reverse else k
        reached = at > place if reverse else at < place
        new = combine(before, jax.tree.map(lambda part: part[at], everything))
        return jax.tree.map(lambda a, b: jnp.where(reached, a, b), new, before)

    return lax.fori_loop(0, length, step, start)


def with_halo(cells, sides, width):
    for axis, dim in sides:
        count = lax.axis_size(axis)
        ends = count - 1
        head = lax.slice_in_dim(cells, 0, width, axis=dim)
        tail = lax.slice_in_dim(cells, cells.shape[dim] - width, cells.shape[dim], axis=dim)
        cells = jnp.concatenate(
            [
                lax.ppermute(tail, axis, [(i, (i + 1) % count) for i in range(ends)]),
                cells,
                lax.ppermute(head, axis, [((i + 1) % count, i) for i in range(ends)]),
            ],
            axis=dim,
        )
    return cells


def normalize(tensor, gain):
    return tensor * lax.rsqrt(jnp.mean(tensor * tensor, -1, keepdims=True) + EPSILON) * gain


def block_parts(values, step_size, log_decay, in_keys):
    per_group = values.shape[1] // in_keys.shape[1]
    cumulative = jnp.cumsum(log_decay, axis=0)
    log_total = cumulative[-1]
    weighting = jnp.exp(log_total[None, :] - cumulative) * step_size
    key_heads = jnp.repeat(in_keys, per_group, axis=1)
    scaled = (values.astype(jnp.float32) * weighting[:, :, None]).astype(jnp.bfloat16)
    injected = jnp.einsum("jhn,jhp->hpn", key_heads, scaled, preferred_element_type=jnp.float32)
    return (cumulative, jnp.exp(log_total), injected)


def block_step(memory, inputs):
    values, step_size, cumulative, damping, injected, in_keys, read_in = inputs
    per_group = values.shape[1] // in_keys.shape[1]
    scores = jnp.einsum("ign,jgn->ijg", read_in, in_keys, preferred_element_type=jnp.float32)
    scores = jnp.repeat(scores, per_group, axis=2)
    length = values.shape[0]
    below_mask = (jnp.arange(length)[:, None] >= jnp.arange(length)[None, :])[:, :, None]
    gaps = jnp.where(below_mask, cumulative[:, None, :] - cumulative[None, :, :], -jnp.inf)
    weights = (scores * jnp.exp(gaps) * step_size[None, :, :]).astype(jnp.bfloat16)
    within = jnp.einsum("ijh,jhp->ihp", weights, values, preferred_element_type=jnp.float32)
    read_heads = jnp.repeat(read_in.astype(jnp.float32), per_group, axis=1)
    carried = (
        jnp.einsum("ihn,hpn->ihp", read_heads, memory, precision=FULL_PRECISION)
        * jnp.exp(cumulative)[:, :, None]
    )
    memory = damping[:, None, None] * memory + injected
    return (memory, within + carried)


def blocked(tensor):
    blocks = tensor.shape[0] // BLOCK
    return tensor.reshape((blocks, BLOCK) + tensor.shape[1:])


def sweep(block_inputs, memory):
    memory, swept = lax.scan(block_step, memory, block_inputs)
    return (swept.reshape((swept.shape[0] * swept.shape[1],) + swept.shape[2:]), memory)


def settle(damping_blocks, injected_blocks, memory):

    def advance(memory, inputs):
        return (inputs[0][:, None, None] * memory + inputs[1], None)

    memory, unused = lax.scan(advance, memory, (damping_blocks, injected_blocks))
    return memory


def chain(before_pair, after_pair):
    return (
        before_pair[0] * after_pair[0],
        after_pair[0][:, None, None] * before_pair[1] + after_pair[1],
    )


def entering(damping, final_state, backward):
    identity_pair = (jnp.ones_like(damping), jnp.zeros_like(final_state))
    if backward:
        arrived = entering_2((damping, final_state), "sp", chain, identity_pair, True)
    else:
        arrived = entering_2((damping, final_state), "sp", chain, identity_pair, False)
    return arrived[1]


def body(
    tokens,
    in_gain,
    w_value,
    w_gate,
    w_in_key,
    w_read,
    w_step_fwd,
    w_step_bwd,
    conv_value,
    conv_key,
    conv_read,
    step_bias,
    rate,
    norm_gain,
    w_out,
):
    normed = normalize(tokens.astype(jnp.float32), in_gain.astype(jnp.float32)).astype(jnp.bfloat16)
    weights = (
        lax.all_gather(w_value, "sp", axis=0, tiled=True),
        lax.all_gather(w_gate, "sp", axis=0, tiled=True),
        lax.all_gather(w_in_key, "sp", axis=0, tiled=True),
        lax.all_gather(w_read, "sp", axis=0, tiled=True),
        lax.all_gather(w_step_fwd, "sp", axis=0, tiled=True),
        lax.all_gather(w_step_bwd, "sp", axis=0, tiled=True),
    )
    projected = [
        jnp.dot(normed, weight, preferred_element_type=jnp.float32).astype(jnp.bfloat16)
        for weight in weights
    ]
    value_raw, gate_raw, key_raw, read_raw, pre_fwd, pre_bwd = projected
    value_cols = value_raw.shape[1]
    key_cols = key_raw.shape[1]
    joined = jnp.concatenate([value_raw, key_raw, read_raw], axis=1)
    padded = with_halo(joined, (("sp", 0),), (KERNEL - 1) // 2)
    kernel_taps = jnp.concatenate([conv_value, conv_key, conv_read], axis=1).astype(jnp.float32)
    length = joined.shape[0]
    summed = jnp.zeros(joined.shape, jnp.float32)
    for offset in range(KERNEL):
        summed = summed + padded[offset : offset + length].astype(jnp.float32) * kernel_taps[offset]
    mixed_in = jax.nn.silu(summed).astype(jnp.bfloat16)
    head_count = value_cols // HEAD_DIM
    group_count = key_cols // STATE
    values = mixed_in[:, :value_cols].reshape(length, head_count, HEAD_DIM)
    in_keys = mixed_in[:, value_cols : value_cols + key_cols].reshape(length, group_count, STATE)
    read_in = mixed_in[:, value_cols + key_cols :].reshape(length, group_count, STATE)
    blank = jnp.zeros((head_count, HEAD_DIM, STATE), jnp.float32)
    summed_heads = jnp.zeros(values.shape, jnp.float32)
    for direction, step_pre in ((0, pre_fwd), (1, pre_bwd)):
        step_size = jax.nn.softplus(step_pre.astype(jnp.float32) + step_bias[direction])
        log_decay = -rate[direction] * step_size
        ordered = (values, step_size, log_decay, in_keys, read_in)
        if direction == 1:
            ordered = tuple((tensor[::-1] for tensor in ordered))
        value_blocks, step_blocks, decay_blocks, key_blocks, read_blocks = [
            blocked(tensor) for tensor in ordered
        ]
        cumulative_blocks, damping_blocks, injected_blocks = jax.vmap(block_parts)(
            value_blocks, step_blocks, decay_blocks, key_blocks
        )
        block_inputs = (
            value_blocks,
            step_blocks,
            cumulative_blocks,
            damping_blocks,
            injected_blocks,
            key_blocks,
            read_blocks,
        )
        damping = jnp.exp(jnp.sum(ordered[2], axis=0))
        final_state = settle(damping_blocks, injected_blocks, blank)
        arriving = entering(damping, final_state, direction == 1)
        swept, final_state = sweep(block_inputs, arriving)
        if direction == 1:
            swept = swept[::-1]
        summed_heads = summed_heads + swept
    gated_out = summed_heads * jax.nn.silu(gate_raw.astype(jnp.float32)).reshape(values.shape)
    head_gain = norm_gain.astype(jnp.float32).reshape(head_count, HEAD_DIM)
    normed_heads = normalize(gated_out, head_gain).astype(jnp.bfloat16).reshape(length, value_cols)
    out_whole = lax.all_gather(w_out, "sp", axis=1, tiled=True)
    own_rows = lax.psum_scatter(
        jnp.dot(normed_heads, out_whole, preferred_element_type=jnp.float32).astype(jnp.bfloat16),
        "tp",
        scatter_dimension=0,
        tiled=True,
    )
    return lax.all_gather(own_rows, "tp", axis=0, tiled=True)


F32 = jnp.float32
BF16 = jnp.bfloat16
LANES = 128
VMEM_SPEC = pl.BlockSpec(memory_space=pltpu.VMEM)


def push(src, dst, send, recv, peer):
    copy = pltpu.make_async_remote_copy(
        src_ref=src,
        dst_ref=dst,
        send_sem=send,
        recv_sem=recv,
        device_id=peer,
        device_id_type=pl.DeviceIdType.MESH,
    )
    copy.start()
    return copy


def silu(x):
    return x * jax.nn.sigmoid(x)


def whole_kernel(
    n, q, tin_h, ing_h, wv, wg, wk, wr, wsf_h, wsb_h, wo, cv_h, ck_h, cr_h, bias_h, rate_h, ngain_h, out,
    tin, ing, wsf, wsb, cv, ck, cr, bias, rate, ngain,
    nrm, ws, taps, gains, tok, wts, wgt, wst, wout, raw, gate, pre, sums, vals, keys, reads, cums, yy, injf, injb, entered,
    nh, full, part, other, summed_up, both,
    tzs, tzr, tps, tpr, tss, tsr, kzs, kzr, kps, kpr, kdr, vs, vr, ss, sr, os, orr,
    as_, ar, bs, br, bdr, xs, xr, es, er, fs, fr, ls, ins,
):
    s, t = lax.axis_index("sp"), lax.axis_index("tp")
    z, p = s // q, s % q
    sibling = (s, 1 - t)
    half = tok.shape[2]
    depth = wv.shape[0]
    blocks = tok.shape[0] * 2 * half // BLOCK

    def at(dz, dp):
        return lax.rem(z + dz, q) * q + lax.rem(p + dp, q)

    def span(i, size):
        return pl.ds(pl.multiple_of(i * size, size), size)

    px = p + 1 - 2 * lax.rem(p, 2)
    py = lax.rem(p + 2, q)
    pd = lax.rem(px + 2, q)
    side = {"x": (z * q + px, t), "y": (z * q + py, t)}
    turns = (("x", "y"), ("y", "x"))

    def chip(dz, where):
        return lax.rem(z + q - dz, q) * q + where

    with jax.named_scope("greet"):
        barrier = pltpu.get_barrier_semaphore()
        peers = [(lax.rem(s + k, n), t) for k in range(1, n)] + [sibling]
        for peer in peers:
            pl.semaphore_signal(barrier, inc=1, device_id=peer, device_id_type=pl.DeviceIdType.MESH)

    def local(src, dst, i):
        copy = pltpu.make_async_copy(src, dst, ls.at[i])
        copy.start()
        return copy

    mine = span(s, depth)
    rows = span(t, half)
    kcol, rcol = pl.ds(LANES, LANES), pl.ds(2 * LANES, LANES)
    krcol = pl.ds(LANES, 2 * LANES)

    with jax.named_scope("load"):
        held = (
            (tin_h, tin), (ing_h, ing), (wsf_h, wsf), (wsb_h, wsb), (cv_h, cv), (ck_h, ck), (cr_h, cr),
            (bias_h, bias), (rate_h, rate), (ngain_h, ngain),
        )
        loads = [pltpu.make_async_copy(src, dst, ins.at[i]) for i, (src, dst) in enumerate(held)]
        for copy in loads:
            copy.start()
        locals_ = [
            local(wk.at[:, span(z, LANES)], wts.at[mine, kcol], 2),
            local(wr.at[:, span(z, LANES)], wts.at[mine, rcol], 3),
            local(wv.at[:, mine], wts.at[mine, pl.ds(0, LANES)], 4),
            local(wg.at[:, mine], wgt.at[mine], 5),
        ]
        for copy in loads:
            copy.wait()
    with jax.named_scope("prep"):
        wide_in = tin[...].astype(F32)
        nrm[...] = normalize(wide_in, ing[...].astype(F32).reshape(1, ing.shape[0])).astype(BF16)
        heads = wsf.shape[0]
        slot = ws.shape[0] // n
        row_i = lax.broadcasted_iota(jnp.int32, (n * slot, heads), 0)
        col_i = lax.broadcasted_iota(jnp.int32, (n * slot, heads), 1)
        place = lax.rem(row_i, slot)
        head_of = 2 * (row_i // slot)
        pick_f = jnp.where((place < 2) & (col_i == head_of + place), 1.0, 0.0).astype(BF16)
        pick_b = jnp.where((place >= 2) & (col_i == head_of + place - 2), 1.0, 0.0).astype(BF16)
        ws[...] = (
            jnp.dot(pick_f, wsf[...], preferred_element_type=F32)
            + jnp.dot(pick_b, wsb[...], preferred_element_type=F32)
        ).astype(BF16)
        own = span(s, LANES)
        taps[0:KERNEL, 0:LANES] = cv[:, own].astype(F32)
        taps[0:KERNEL, LANES : 2 * LANES] = ck[:, span(z, LANES)].astype(F32)
        taps[0:KERNEL, 2 * LANES : 3 * LANES] = cr[:, span(z, LANES)].astype(F32)
        gains[...] = ngain[...].astype(F32).reshape(n, LANES)
        lanes_of = lax.broadcasted_iota(jnp.int32, (8, heads), 1)
        rows_of = lax.broadcasted_iota(jnp.int32, (8, heads), 0)
        spread = jnp.where((rows_of < 4) & (lanes_of == 2 * s + lax.rem(rows_of, 2)), 1.0, 0.0).astype(F32)
        first_two = lax.broadcasted_iota(jnp.int32, (8, 1), 0) < 2
        across_lanes = (((1,), (1,)), ((), ()))

        def own_rows(both_dirs):
            got = lax.dot_general(
                spread, both_dirs, across_lanes, precision=FULL_PRECISION, preferred_element_type=F32
            )
            return jnp.where(first_two, got[:, 0:1], got[:, 1:2])

        offsets = own_rows(bias[...])
        rates = own_rows(rate[...])
        wst[slot:, :] = jnp.zeros((LANES - slot, wst.shape[1]), BF16)
        seq = blocks * BLOCK
        wide = 3 * LANES
        raw[0:8, :] = jnp.zeros((8, wide), F32)
        raw[seq + 8 : seq + 16, :] = jnp.zeros((8, wide), F32)
        for copy in locals_:
            copy.wait()
    with jax.named_scope("greeted"):
        pl.semaphore_wait(barrier, len(peers))

    one, last = q - 1, q
    rising, sinking = z < q - 1, z > 0
    unit = nrm.at[rows]

    def arrival(e):
        later = [[1, 2, 3], [0, 2, 3], [3, 1, 0], [2, 1, 0]]
        picked = later[q - 1][e]
        for k in range(q - 1):
            picked = jnp.where(z == k, later[k][e], picked)
        return picked

    sources = [z] + [arrival(e) for e in range(q - 1)]

    def chain(src_ref, dst_ref, sends, recvs):
        @pl.when(rising)
        def _():
            push(src_ref, dst_ref, sends.at[z], recvs.at[z], (s + q, t))

        @pl.when(sinking)
        def _():
            push(src_ref, dst_ref, sends.at[q], recvs.at[z], (s - q, t))

    def remote(src, dst, send, recv, peer):
        return pltpu.make_async_remote_copy(
            src_ref=src, dst_ref=dst, send_sem=send, recv_sem=recv,
            device_id=peer, device_id_type=pl.DeviceIdType.MESH,
        )

    def landed(ref, sem):
        remote(ref, ref, sem, sem, sibling).wait_recv()

    def left_here(ref, sem):
        remote(ref, ref, sem, sem, sibling).wait_send()

    def onward(zs):
        to = z + jnp.where(zs < z, 1, -1)
        return to, (to >= 0) & (to < q)

    def settle_chain(src_ref, sends, recvs, ref_of):
        @pl.when(rising)
        def _():
            remote(src_ref, ref_of(z), sends.at[z], recvs.at[z], (s + q, t)).wait_send()

        @pl.when(sinking)
        def _():
            remote(src_ref, ref_of(z), sends.at[q], recvs.at[z], (s - q, t)).wait_send()

        for zs in sources[1:]:
            to, ok = onward(zs)

            @pl.when(ok)
            def _():
                ref = ref_of(zs)
                remote(ref, ref, sends.at[zs], recvs.at[zs], (to * q + p, t)).wait_send()

    def tok_of(zs):
        return tok.at[zs * q + p, t]

    def wout_of(zs):
        return wout.at[:, span(zs, LANES)]

    plane, keyz, keyp, weights, swaps = {}, [], {}, [], {}
    with jax.named_scope("issue"):
        chain(unit, tok_of(z), tzs, tzr)
        for i, to in enumerate("xy"):
            plane[0, to] = push(unit, tok.at[s, t], tps.at[0], tpr.at[0, i], side[to])
        for dz in range(1, q):
            grp = span(lax.rem(z + dz, q), LANES)
            keyz.append(
                [
                    push(w.at[:, grp], wts.at[mine, col], kzs.at[0], kzr.at[dz], (at(dz, 0), t))
                    for i, (w, col) in enumerate(((wk, kcol), (wr, rcol)))
                ]
            )
        got = wts.at[mine, krcol]
        for i, to in enumerate("xy"):
            keyp[0, to] = push(got, got, kps.at[0], kpr.at[0, i], side[to])
        for k in range(1, n):
            j = lax.rem(s + k, n)
            weights.append(
                push(wv.at[:, span(j, LANES)], wts.at[mine, pl.ds(0, LANES)], vs.at[0], vr.at[0], (j, t))
            )
            weights.append(
                push(ws.at[span(j, slot)], wst.at[pl.ds(0, slot), mine], ss.at[0], sr.at[0], (j, t))
            )
        locals_ = [
            local(nrm.at[pl.ds(0, half)], tok.at[s, 0], 0),
            local(nrm.at[pl.ds(half, half)], tok.at[s, 1], 1),
            local(ws.at[span(s, slot)], wst.at[pl.ds(0, slot), mine], 6),
            local(wo, wout_of(z), 7),
        ]

    gates = []

    def send_gates():
        for k in range(1, n):
            j = lax.rem(s + k, n)
            gates.append(push(wg.at[:, span(j, LANES)], wgt.at[mine], vs.at[1], vr.at[1], (j, t)))

    def swap(e, i):
        src = sources[e] * q + (p, px, py, pd)[i]
        swaps[e, i] = push(tok.at[src, t], tok.at[src, t], tss.at[0], tsr.at[e], sibling)

    def arrive(e):
        with jax.named_scope("arrive"):
            zs = sources[e]
            ref = tok_of(zs)
            remote(ref, ref, tzs.at[zs], tzr.at[zs], sibling).wait_recv()
            to, ok = onward(zs)

            @pl.when(ok)
            def _():
                push(ref, ref, tzs.at[zs], tzr.at[zs], (to * q + p, t))

    def spread_plane(e):
        ref = tok_of(sources[e])
        for i, way in enumerate("xy"):
            plane[e, way] = push(ref, ref, tps.at[0], tpr.at[e, i], side[way])
        swap(e, 0)

    def arrive_last(forwards):
        zs = sources[q - 1]
        ok = onward(zs)[1]

        @pl.when(ok if forwards else jnp.logical_not(ok))
        def _():
            arrive(q - 1)
            spread_plane(q - 1)

    quarter = half // 2

    def relay(e):
        with jax.named_scope("relay"):
            for i, (near_by, other) in enumerate(turns):
                landed(tok.at[0, 0], tpr.at[e, i])
                ref = tok.at[sources[e] * q + (px, py)[i], t, pl.ds(i * quarter, quarter)]
                plane[e, other + "d"] = push(ref, ref, tps.at[0], tpr.at[e, 2], side[other])
                swap(e, 1 + i)

    def key_arrive(dz):
        with jax.named_scope("key_arrive"):
            landed(wgt.at[pl.ds(0, 2 * depth)], kzr.at[dz])
            ref = wts.at[span(at(q - dz, 0), depth), krcol]
            for i, to in enumerate("xy"):
                keyp[dz, to] = push(ref, ref, kps.at[0], kpr.at[dz, i], side[to])

    def key_relay(dz):
        with jax.named_scope("key_relay"):
            for i, (near_by, other) in enumerate(turns):
                keyp[dz, near_by].wait_recv()
                ref = wts.at[span(chip(dz, (px, py)[i]), depth), (kcol, rcol)[i]]
                keyp[dz, other + "d"] = push(ref, ref, kps.at[0], kdr.at[0], side[other])

    ri = lax.broadcasted_iota(jnp.int32, (BLOCK, BLOCK), 0)
    ci = lax.broadcasted_iota(jnp.int32, (BLOCK, BLOCK), 1)
    low = ri >= ci
    diag = ri == ci
    left = ci < HEAD_DIM
    until = jnp.where(ri <= ci, 1.0, 0.0).astype(BF16)
    since = jnp.where(low, 1.0, 0.0).astype(BF16)
    sums_of = jnp.concatenate([until, since], axis=1)
    pick = jnp.where(ri[0:8] == ci[0:8], 1.0, 0.0).astype(BF16)

    def project(zs):
        r0 = pl.multiple_of(zs * q * BLOCK, q * BLOCK)
        whole_plane = pl.ds(r0, q * BLOCK)
        x = tok[pl.ds(zs * q, q)].reshape(q * BLOCK, tok.shape[3])
        got = jnp.dot(x, wts[...], preferred_element_type=F32).astype(BF16)
        raw[pl.ds(r0 + 8, q * BLOCK), :] = got[:, 0 : 3 * LANES].astype(F32)
        u = lax.dot_general(pick, got[:, 3 * LANES :], across_lanes, preferred_element_type=F32) + offsets
        steps = jnp.maximum(u, 0.0) + jnp.log1p(jnp.exp(-jnp.abs(u)))
        pre[:, whole_plane] = steps
        decay = -rates * steps
        parts = []
        for b in range(q):
            rest = decay[:, b * BLOCK : (b + 1) * BLOCK]
            for _ in range(3):
                piece = rest.astype(BF16).astype(F32)
                parts.append(piece)
                rest = rest - piece
        summed = jnp.dot(jnp.concatenate(parts, axis=0).astype(BF16), sums_of, preferred_element_type=F32)
        for b in range(q):
            at_b = pl.ds(pl.multiple_of((zs * q + b) * BLOCK, BLOCK), BLOCK)
            got = [summed[24 * b + 8 * k : 24 * b + 8 * k + 8] for k in range(3)]
            both_sums = got[0] + (got[1] + got[2])
            c = jnp.where(first_two, both_sums[:, 0:BLOCK], both_sums[:, BLOCK:])
            c_end = jnp.where(first_two, c[:, BLOCK - 1 : BLOCK], c[:, 0:1])
            sums[:, at_b] = c
            weighting = jnp.exp(c_end - c) * steps[:, b * BLOCK : (b + 1) * BLOCK]
            stacked = jnp.concatenate([c, weighting, jnp.exp(c), jnp.zeros((LANES - 24, BLOCK), F32)], axis=0)
            cums[at_b, :] = stacked.T

    def open_gate(zs):
        with jax.named_scope("gate"):
            x = tok[pl.ds(zs * q, q)].reshape(q * BLOCK, tok.shape[3])
            here = pl.ds(pl.multiple_of(zs * q * BLOCK, q * BLOCK), q * BLOCK)
            gate[here, :] = jnp.dot(x, wgt[...], preferred_element_type=F32).astype(BF16)

    def open_block(i):
        here = pl.ds(pl.multiple_of(i * BLOCK, BLOCK), BLOCK)
        x = tok[i].reshape(BLOCK, tok.shape[3])
        gate[here, :] = jnp.dot(x, wgt[...], preferred_element_type=F32).astype(BF16)

    def convolve(i):
        r0 = pl.multiple_of(i * BLOCK, BLOCK)
        for b, dst in enumerate((vals, keys, reads)):
            window = raw[pl.ds(r0, BLOCK + 16), b * LANES : (b + 1) * LANES]
            total = jnp.zeros((BLOCK, LANES), F32)
            for k in range(KERNEL):
                lo = 8 - (KERNEL - 1) // 2 + k
                total = total + window[lo : lo + BLOCK] * taps[k : k + 1, b * LANES : (b + 1) * LANES]
            dst[pl.ds(r0, BLOCK), :] = silu(total).astype(BF16)

    def within(i):
        r0 = pl.multiple_of(i * BLOCK, BLOCK)
        here = pl.ds(r0, BLOCK)
        c, ct, stt = cums[here, :], sums[:, here], pre[:, here]
        key, read, val = keys[here, :], reads[here, :], vals[here, :]
        val32 = val.astype(F32)
        score = lax.dot_general(read, key, across_lanes, preferred_element_type=F32)
        total = jnp.zeros((BLOCK, LANES), F32)
        for h in range(2):
            gap = jnp.where(low, c[:, h : h + 1] - ct[h : h + 1, :], c[:, h + 2 : h + 3] - ct[h + 2 : h + 3, :])
            sb = stt[h + 2 : h + 3, :]
            e = jnp.exp(gap) * jnp.where(low, stt[h : h + 1, :], sb) + jnp.where(diag, sb, 0.0)
            mask = left if h == 0 else jnp.logical_not(left)
            own_val = jnp.where(mask, val32, 0.0).astype(BF16)
            total = total + jnp.dot((score * e).astype(BF16), own_val, preferred_element_type=F32)
        yy[here, :] = total
        key_t = key.astype(F32).T.astype(BF16)
        for d, dst in ((0, injf), (1, injb)):
            w = jnp.where(left, c[:, 8 + 2 * d : 9 + 2 * d], c[:, 9 + 2 * d : 10 + 2 * d])
            scaled = (val32 * w).astype(BF16)
            dst[i] = jnp.dot(key_t, scaled, preferred_element_type=F32)

    def meet(e):
        with jax.named_scope("meet"):
            landed(tok.at[0, 0], tpr.at[e, 2])
            swap(e, 3)

    def use(e):
        zs = sources[e]
        with jax.named_scope("usewait"):
            landed(tok.at[pl.ds(0, q if e else q - 1), 0], tsr.at[e])
        with jax.named_scope("project"):
            project(zs)
        edge = jnp.where(zs == 0, 0, blocks - 1)
        if e == 0:
            start, count = zs * q + 1, q - 2
        else:
            start, count = zs * q + jnp.where(zs > z, -1, 1), q
        if e == q - 1:
            count = count + 1

        def which(i):
            return start + i if e < q - 1 else jnp.where(i < q, start + i, edge)

        with jax.named_scope("conv"):

            @pl.loop(0, count, unroll=count)
            def _(i):
                convolve(which(i))

        with jax.named_scope("intra"):

            @pl.loop(0, count, unroll=count)
            def _(i):
                if e == q - 1:
                    open_block(zs * q + jnp.minimum(i, q - 1))
                within(which(i))

        if e < q - 1:

            @pl.when((zs == 0) | (zs == q - 1))
            def _():
                convolve(edge)
                within(edge)

    def wout_onward(e):
        zs = sources[e]
        to, ok = onward(zs)

        @pl.when(ok)
        def _():
            ref = wout_of(zs)
            remote(ref, ref, os.at[zs], orr.at[zs], sibling).wait_recv()
            push(ref, ref, os.at[zs], orr.at[zs], (to * q + p, t))

    def wout_arrive(e):
        zs = sources[e]
        to, ok = onward(zs)

        @pl.when(jnp.logical_not(ok))
        def _():
            ref = wout_of(zs)
            remote(ref, ref, os.at[zs], orr.at[zs], sibling).wait_recv()

    arrive(1)
    relay(0)
    for dz in range(1, q):
        key_arrive(dz)
    key_relay(0)
    spread_plane(1)
    for dz in range(1, q):
        key_relay(dz)
    arrive(2)
    spread_plane(2)
    relay(1)
    send_gates()
    meet(0)
    arrive_last(True)
    chain(wo, wout_of(z), os, orr)
    with jax.named_scope("weights"):
        for copy in locals_:
            copy.wait()
        landed(wgt.at[pl.ds(0, (n - 1) * depth)], vr.at[0])
        landed(ws.at[pl.ds(0, (n - 1) * slot)], sr.at[0])
        landed(wgt.at[pl.ds(0, 2 * q * depth)], kdr.at[0])
    with jax.named_scope("turn"):
        for k in range(wst.shape[1] // LANES):
            chunk = slice(k * LANES, (k + 1) * LANES)
            wts[chunk, 3 * LANES :] = wst[:, chunk].astype(F32).T.astype(BF16)
    use(0)
    meet(1)
    relay(2)
    arrive_last(False)
    use(1)
    meet(2)
    with jax.named_scope("wout1"):
        wout_onward(1)
        wout_onward(2)
    relay(3)
    use(2)
    meet(3)
    with jax.named_scope("gates"):
        landed(wgt.at[pl.ds(0, (n - 1) * depth)], vr.at[1])
    for e in range(q - 1):
        open_gate(sources[e])
    use(3)

    def climb(i, states):
        after = []
        for d, inj in ((0, injf), (1, injb)):
            j = i if d == 0 else blocks - 1 - i
            edge_row = cums[pl.ds(pl.multiple_of(j * BLOCK + (1 - d) * (BLOCK - 8), 8), 8), :]
            edge_row = edge_row[7:8] if d == 0 else edge_row[0:1]
            end = jnp.where(left[0:1], edge_row[:, 16 + 2 * d : 17 + 2 * d], edge_row[:, 17 + 2 * d : 18 + 2 * d])
            high = states[d].astype(BF16)
            entered[j, :, 2 * d * LANES : (2 * d + 1) * LANES] = high
            entered[j, :, (2 * d + 1) * LANES : (2 * d + 2) * LANES] = (states[d] - high.astype(F32)).astype(BF16)
            after.append(states[d] * end + inj[j])
        return tuple(after)

    with jax.named_scope("carry"):
        zero = jnp.zeros((STATE, LANES), F32)
        lax.fori_loop(0, blocks, climb, (zero, zero), unroll=4)

    gain = gains[pl.ds(s, 1), :]

    def finish(i):
        r0 = pl.multiple_of(i * BLOCK, BLOCK)
        here = pl.ds(r0, BLOCK)
        got = jnp.dot(reads[here, :], entered[i], preferred_element_type=F32)
        y = yy[here, :]
        for d in range(2):
            grown = jnp.where(left, cums[here, 16 + 2 * d : 17 + 2 * d], cums[here, 17 + 2 * d : 18 + 2 * d])
            y = y + (
                got[:, 2 * d * LANES : (2 * d + 1) * LANES] + got[:, (2 * d + 1) * LANES : (2 * d + 2) * LANES]
            ) * grown
        g = y * silu(gate[here, :].astype(F32))
        sq = g * g
        m0 = jnp.sum(jnp.where(left, sq, 0.0), -1, keepdims=True) / HEAD_DIM
        m1 = jnp.sum(jnp.where(left, 0.0, sq), -1, keepdims=True) / HEAD_DIM
        scale = jnp.where(left, lax.rsqrt(m0 + EPSILON), lax.rsqrt(m1 + EPSILON))
        nh[here, :] = (g * scale * gain).astype(BF16)

    def finish_plane(zs):
        with jax.named_scope("finish"):

            @pl.loop(0, q, unroll=4)
            def _(i):
                finish(zs * q + i)

    near = {}

    def spread_near(e):
        ref = full.at[:, span(sources[e] * q + p, LANES)] if e else nh.at[span(z, q * BLOCK)]
        dst = full.at[:, span(sources[e] * q + p, LANES)]
        for i, to in enumerate("xy"):
            near[e, to] = push(ref, dst, bs.at[0], br.at[e, i], side[to])

    def near_relay(e):
        with jax.named_scope("nearwait"):
            for i, (near_by, other) in enumerate(turns):
                near[e, near_by].wait_recv()
                got = full.at[pl.ds(i * rest_rows, rest_rows), span(sources[e] * q + (px, py)[i], LANES)]
                push(got, got, bs.at[0], bdr.at[0], side[other])

    rest_rows = q * BLOCK // 2
    for e in range(1, q):
        zs = sources[e]
        finish_plane(zs)
        push(nh.at[span(zs, q * BLOCK)], full.at[:, mine], as_.at[0], ar.at[z], (zs * q + p, t))
    finish_plane(z)
    keep = local(nh.at[span(z, q * BLOCK)], full.at[:, mine], 8)
    spread_near(0)
    for e in range(1, q):
        with jax.named_scope("awaywait"):
            landed(nh.at[pl.ds(0, q * BLOCK)], ar.at[sources[e]])
        spread_near(e)
        near_relay(e - 1)
        if e == 2:
            with jax.named_scope("wout2"):
                wout_onward(3)
    near_relay(q - 1)
    with jax.named_scope("outswait"):
        for e in range(1, q):
            wout_arrive(e)
    with jax.named_scope("fullwait"):
        keep.wait()
        landed(full.at[pl.ds(0, BLOCK)], bdr.at[0])
    legs = []
    part_rows = BLOCK // 2
    kept, given = span(t, part_rows), span(1 - t, part_rows)

    def toward(dp):
        return lax.rem(p + dp, q)

    def multiply(dp):
        to = toward(dp)
        part[to] = jnp.dot(full[span(to, BLOCK), :], wout[...], preferred_element_type=F32).astype(BF16)

    def give(dp):
        to = toward(dp)
        push(part.at[to, given], other.at[to], xs.at[0], xr.at[dp - 1], sibling)

    def add_up(dp):
        to = toward(dp)
        landed(other.at[to], xr.at[dp - 1])
        total = (part[to, kept, :].astype(F32) + other[to].astype(F32)).astype(BF16)
        if dp < q:
            summed_up[to] = total
            legs.append(push(summed_up.at[to], both.at[t, p], es.at[0], er.at[dp], (at(0, dp), t)))
        else:
            both[t, p] = total
            push(both.at[t, p], both.at[t, p], fs.at[0], fr.at[0], sibling)

    with jax.named_scope("outdot"):
        multiply(1)
        for dp in range(2, q + 1):
            multiply(dp)
            give(dp - 1)
        give(q)
        for dp in range(1, q + 1):
            add_up(dp)
    with jax.named_scope("legswait"):
        for dp in range(1, q):
            legs[dp - 1].wait_recv()
            got = both.at[t, lax.rem(p + q - dp, q)]
            push(got, got, fs.at[0], fr.at[0], sibling)
    with jax.named_scope("acrosswait"):
        landed(both.at[0], fr.at[0])
    with jax.named_scope("sum"):
        for h in range(2):
            for a in range(q):
                for b in range(q):
                    out[h * part_rows : (h + 1) * part_rows, (a * q + b) * LANES : (a * q + b + 1) * LANES] = both[
                        h, b, :, a * LANES : (a + 1) * LANES
                    ]
    with jax.named_scope("sends"):
        settle_chain(unit, tzs, tzr, tok_of)
        settle_chain(wo, os, orr, wout_of)
        left_here(tok.at[pl.ds(0, 3 * q), 0], tps.at[0])
        left_here(tok.at[pl.ds(0, n - 1), 0], tss.at[0])
        left_here(wgt.at[pl.ds(0, 2 * (q - 1) * depth)], kzs.at[0])
        left_here(wts.at[pl.ds(0, 6 * depth)], kps.at[0])
        left_here(wgt.at[pl.ds(0, (n - 1) * depth)], vs.at[0])
        left_here(wgt.at[pl.ds(0, (n - 1) * depth)], vs.at[1])
        left_here(ws.at[pl.ds(0, (n - 1) * slot)], ss.at[0])
        left_here(nh.at[pl.ds(0, (q - 1) * q * BLOCK)], as_.at[0])
        left_here(full.at[pl.ds(0, 3 * BLOCK)], bs.at[0])
        left_here(other, xs.at[0])
        left_here(summed_up.at[pl.ds(0, q - 1)], es.at[0])
        left_here(both.at[0], fs.at[0])


def whole(n, q, *args):
    dma = pltpu.SemaphoreType.DMA
    vm = pltpu.VMEM
    tokens, wo, wsf = args[0], args[8], args[6]
    depth, width = tokens.shape
    seq = n * depth
    slot = 16
    return pl.pallas_call(
        functools.partial(whole_kernel, n, q),
        out_shape=jax.ShapeDtypeStruct((BLOCK, n * LANES), BF16),
        in_specs=[HBM_SPEC] * len(args),
        out_specs=VMEM_SPEC,
        scratch_shapes=[
            *[vm(args[i].shape, args[i].dtype) for i in (0, 1, 6, 7, 9, 10, 11, 12, 13, 14)],
            vm((depth, width), BF16),
            vm((n * slot, depth), BF16),
            vm((8, 3 * LANES), F32),
            vm((n, LANES), F32),
            vm((n, 2, depth // 2, width), BF16),
            vm((width, 4 * LANES), BF16),
            vm((width, LANES), BF16),
            vm((LANES, width), BF16),
            vm((wo.shape[0], q * LANES), BF16),
            vm((seq + 16, 3 * LANES), F32),
            vm((seq, LANES), BF16),
            vm((8, seq), F32),
            vm((8, seq), F32),
            vm((seq, LANES), BF16),
            vm((seq, LANES), BF16),
            vm((seq, LANES), BF16),
            vm((seq, LANES), F32),
            vm((seq, LANES), F32),
            vm((seq // BLOCK, STATE, LANES), F32),
            vm((seq // BLOCK, STATE, LANES), F32),
            vm((seq // BLOCK, STATE, 4 * LANES), BF16),
            vm((seq, LANES), BF16),
            vm((q * BLOCK, n * LANES), BF16),
            vm((q, BLOCK, q * LANES), BF16),
            vm((q, BLOCK // 2, q * LANES), BF16),
            vm((q, BLOCK // 2, q * LANES), BF16),
            vm((2, q, BLOCK // 2, q * LANES), BF16),
            dma((q + 1,)), dma((q,)), dma((1,)), dma((q, 3)), dma((1,)), dma((q,)),
            dma((1,)), dma((q,)), dma((1,)), dma((q, 2)), dma((1,)),
            dma((2,)), dma((2,)), dma((1,)), dma((1,)), dma((q + 1,)), dma((q,)),
            dma((1,)), dma((q,)), dma((1,)), dma((q, 2)), dma((1,)), dma((1,)), dma((q,)), dma((1,)), dma((q,)),
            dma((1,)), dma((1,)), dma((10,)), dma((10,)),
        ],
        compiler_params=pltpu.CompilerParams(
            collective_id=0, has_side_effects=True, vmem_limit_bytes=VMEM_LIMIT << 10
        ),
        name="whole",
    )(*args)


VMEM_LIMIT = 57344
HBM_SPEC = pl.BlockSpec(memory_space=pltpu.HBM)


def headwise(
    n,
    q,
    tokens,
    in_gain,
    w_value,
    w_gate,
    w_in_key,
    w_read,
    w_step_fwd,
    w_step_bwd,
    conv_value,
    conv_key,
    conv_read,
    step_bias,
    rate,
    norm_gain,
    w_out,
):
    return whole(
        n, q, tokens, in_gain, w_value, w_gate, w_in_key, w_read, w_step_fwd.T, w_step_bwd.T, w_out,
        conv_value, conv_key, conv_read, step_bias, rate, norm_gain,
    )


def whole_heads(mesh):
    n, q = mesh.shape["sp"], math.isqrt(mesh.shape["sp"])

    def run(*args):
        cols, keys = args[2].shape[1], args[4].shape[1]
        ready = (
            q * q == n
            and mesh.shape["tp"] == 2
            and cols == n * LANES
            and args[14].shape[1] == LANES
            and keys == q * LANES
            and q == 4
            and args[0].shape[1] == n * LANES
            and args[0].shape[0] == BLOCK
        )
        return headwise(n, q, *args) if ready else body(*args)

    return run


def solution(mesh):
    in_specs = (
        P("sp", None),
        P(),
        P("sp", "tp"),
        P("sp", "tp"),
        P("sp", "tp"),
        P("sp", "tp"),
        P("sp", "tp"),
        P("sp", "tp"),
        P(None, "tp"),
        P(None, "tp"),
        P(None, "tp"),
        P(None, "tp"),
        P(None, "tp"),
        P("tp"),
        P("tp", "sp"),
    )
    out_specs = P("sp", None)
    return jax.shard_map(whole_heads(mesh), mesh=mesh, in_specs=in_specs, out_specs=out_specs, check_vma=False)
```
